32 devices in a mesh: ep: 8 (over z, y), tp: 4 (over x, core).
Axes of the slice: x: 2, y: 2, z: 4, core: 2. Of those that a mesh axis runs over, the one named last changes fastest.
Arguments:
- sequence_entry_features: bfloat16 [12288, 4096], P('ep', 'tp'), may hold values from -6 to 6
- sequence_exit_gating: bfloat16 [12288, 4096], P('ep', 'tp'), may hold values from -6 to 6
- memory_insert_clusters: bfloat16 [12288, 1024], P('ep', 'tp'), may hold values from -6 to 6
- memory_query_clusters: bfloat16 [12288, 1024], P('ep', 'tp'), may hold values from -6 to 6
- interval_presoftplus: bfloat16 [12288, 64], P('ep', 'tp'), may hold values from -4 to 4
- entry_filter_taps: bfloat16 [4, 4096], P(None, 'tp'), may hold values from -3 to 3
- insert_filter_taps: bfloat16 [4, 1024], P(None, 'tp'), may hold values from -3 to 3
- query_filter_taps: bfloat16 [4, 1024], P(None, 'tp'), may hold values from -3 to 3
- interval_offset: float32 [64], P('tp'), may hold values from -6 to -1
- head_fading_exponent: float32 [64], P('tp'), may hold values from -8 to -1
- skip_connection_factor: float32 [64], P('tp'), may hold values from 0.1 to 1.9
- spike_fading_exponent: float32 [12288, 64], P('ep', 'tp'), may hold values from -1 to 0
- cluster_scaling_vector: float32 [4096], P('tp'), may hold values from 0.1 to 1.9
- sequence_exit_projection: bfloat16 [4096, 2048], P('tp'), may hold values from -0.09375 to 0.09375
- specialist_sample_slice: bfloat16 [4096, 2048], P(('ep', 'tp')), may hold values from -6 to 6
- specialist_scaling_vector: float32 [2048], replicated, may hold values from 0.1 to 1.9
- chosen_specialists: int32 [4096, 4], P(('ep', 'tp')), may hold values from 0 to 7, all different within a row; in each aligned block of 128 rows (0 to 127, 128 to 255, ...) at most 80 rows name the same one
- dispatcher_affinity_matrix: float32 [4096, 4], P(('ep', 'tp')), may hold values from -4 to 4
- gating_projection: bfloat16 [8, 2048, 2048], P('ep', None, 'tp'), may hold values from -0.5 to 0.5
- expand_projection: bfloat16 [8, 2048, 2048], P('ep', None, 'tp'), may hold values from -0.5 to 0.5
- shrink_projection: bfloat16 [8, 2048, 2048], P('ep', 'tp'), may hold values from -0.03125 to 0.03125
Outputs:
- mixed: bfloat16 [12288, 2048], P(('ep', 'tp'))
- moe_out: bfloat16 [4096, 2048], P(('ep', 'tp'))
The draws below stay inside these ranges and needn't reach their ends.
Inputs may be any that keep to these rules, and one draw needn't show every extreme that they name: `chosen_specialists`: in each aligned block of 128 rows (the rows of one device) no expert is named by more than 80 rows, a bound that some block reaches; the 4 experts of a row differ.
All inputs are finite; a program needn't handle non-finite values.
Results may differ from the reference program's by a relative error of at most 0.015.
Values may be sent and summed in bfloat16 or wider, within the bound.
A program may use at most 192 MiB of HBM per device.

```python
import math
import jax
import jax.numpy as jnp
import numpy as np
from jax import lax

D = 2048
HEADS = 64
HEAD = 64
GROUPS = 8
STATE = 128
TAPS = 4
SPAN = 128
FF = 2048
TOPK = 4
TOKA = 1536
TOK_B = 128
INNER = 4096
EXPERTS = 8
CAP = 80
SEQUENCE_LENGTH = 12288
TOKENS_B = 4096
N_TP = 4


def head_speed(key):
    share = 0.5
    return jax.random.bernoulli(jax.random.fold_in(key, 101), share, (HEADS,))


def draw_head_fading_exponent(key, part):
    quick = head_speed(key)
    fast_rate = jax.random.uniform(jax.random.fold_in(key, 102), (HEADS,), jnp.float32, 0.1, 0.25)
    slow_rate = jax.random.uniform(jax.random.fold_in(key, 103), (HEADS,), jnp.float32, 30.0, 77.0) / SEQUENCE_LENGTH
    return jnp.log(jnp.where(quick, fast_rate, slow_rate)).astype(jnp.float32)


def draw_interval_offset(key, part):
    quick = head_speed(key)
    fast_step = jnp.exp(jax.random.uniform(jax.random.fold_in(key, 104), (HEADS,), jnp.float32, -2.302585, -1.386294))
    slow_step = jnp.exp(jax.random.uniform(jax.random.fold_in(key, 105), (HEADS,), jnp.float32, -5.521461, -4.60517))
    chosen = jnp.where(quick, fast_step, slow_step)
    return (chosen + jnp.log(-jnp.expm1(-chosen))).astype(jnp.float32)


def draw_interval_presoftplus(key, part):
    noise = jnp.clip(0.5 * jax.random.normal(jax.random.fold_in(key, 106), (SEQUENCE_LENGTH, HEADS), jnp.float32), -2.5, 2.5)
    shifts = jax.random.uniform(jax.random.fold_in(key, 107), (SEQUENCE_LENGTH // TOKA, HEADS), jnp.float32, -0.8, 0.8)
    return (noise + jnp.repeat(shifts, TOKA, axis=0)).astype(jnp.bfloat16)


def draw_spike_fading_exponent(key, part):
    spike_positions = jax.random.randint(jax.random.fold_in(key, 108), (3,), 0, SEQUENCE_LENGTH)
    spike_mask = jnp.any(jnp.arange(SEQUENCE_LENGTH)[:, None] == spike_positions[None, :], axis=1)
    objective_values = jnp.log(jax.random.uniform(jax.random.fold_in(key, 109), (SEQUENCE_LENGTH, HEADS), jnp.float32, 0.65, 0.8))
    return jnp.where(spike_mask[:, None], objective_values, 0.0).astype(jnp.float32)


def levels(stream_key, dims, split, smallest, high):
    level, own = 1.0, jax.random.fold_in(stream_key, 6)
    for axis_at, shards_of in split:
        steps = jnp.exp(jax.random.uniform(jax.random.fold_in(own, axis_at), (shards_of,), jnp.float32, smallest / len(split), high / len(split)))
        level = level * jnp.repeat(steps, dims[axis_at] // shards_of).reshape([-1 if axis == axis_at else 1 for axis in range(len(dims))])
    return level


def shared_out(stream_key, own, number, rows, count, top, reach, skew):
    order = jax.random.permutation(stream_key, count)
    packed, usual = shares(count, rows * top, reach, skew, True), shares(count, rows * top, reach, skew, False)
    places = jnp.arange(count)

    def named(lengths, rotation):
        used = int((lengths > 0).sum())
        fixed = max(1, used // 4)
        passed = fixed + (places - fixed + rotation * (used - fixed)) % max(1, count - fixed)
        return jnp.zeros((count,), jnp.int32).at[order[jnp.where(places < fixed, places, passed)]].set(jnp.asarray(lengths, jnp.int32))

    lengths = jnp.where(number % 4 == 0, named(packed, number // 4), named(usual, number - number // 4 - 1))
    mixed = jax.random.permutation(jax.random.fold_in(own, 3), count)
    giver, taker = mixed[0:count // 2 * 2:2], mixed[1:count // 2 * 2:2]
    margin = jnp.minimum(lengths[giver] - 1, reach - lengths[taker]) // 2
    margin = jnp.where((giver == order[0]) | (taker == order[0]) | (lengths[taker] == 0), 0, jnp.maximum(margin, 0))
    passed = jax.random.randint(jax.random.fold_in(own, 4), (count // 2,), 0, 1 << 20) % (margin + 1)
    lengths = lengths.at[giver].add(-passed).at[taker].add(passed)
    labels = jnp.searchsorted(jnp.cumsum(lengths), jnp.arange(rows * top), side="right").astype(jnp.int32)
    listing = labels.reshape(top, rows).T
    listing = listing[jax.random.permutation(jax.random.fold_in(own, 1), rows)]
    rotation = jax.random.randint(jax.random.fold_in(own, 2), (rows, 1), 0, top)
    return jnp.take_along_axis(listing, (jnp.arange(top)[None, :] + rotation) % top, axis=1)


def shares(amount, total, reach, slope, full):
    portions = [(1 << 20) // math.isqrt(rank ** slope) + 1 for rank in range(1, amount + 1)]
    largest = reach if full else min(reach, max(-(-total // amount), total * portions[0] // sum(portions)))
    least = 1 if total - largest >= amount - 1 else 0
    given, rest = [largest] + [least] * (amount - 1), total - largest - least * (amount - 1)
    while rest > 0:
        free = [i for i in range(1, amount) if given[i] < largest] or [i for i in range(1, amount) if given[i] < reach]
        mass, remaining = sum([portions[i] for i in free]), rest
        for i in free:
            more = min(reach - given[i], max(1, remaining * portions[i] // mass), rest)
            given[i] = given[i] + more
            rest = rest - more
    return np.array(given)


def scatter_about(rng, shape, spread, reach, cuts=(), kind=jnp.bfloat16):
    array = spread * jax.random.normal(rng, shape, jnp.float32)
    if cuts:
        array = array * levels(rng, shape, cuts, -0.22, 0.18)
    return jnp.clip(array, -reach, reach).astype(kind)


def setup_inputs(seed: int = 0) -> dict:
    key_list = jax.random.split(jax.random.key(seed), 22)
    sequence_entry_features = scatter_about(key_list[0], (SEQUENCE_LENGTH, INNER), 1.0, 6.0, ((0, 8), (1, 4)))
    sequence_exit_gating = scatter_about(key_list[1], (SEQUENCE_LENGTH, INNER), 1.0, 6.0, ((0, 8), (1, 4)))
    memory_insert_clusters = scatter_about(key_list[2], (SEQUENCE_LENGTH, GROUPS * STATE), 1.0, 6.0, ((0, 8), (1, 4)))
    memory_query_clusters = scatter_about(key_list[3], (SEQUENCE_LENGTH, GROUPS * STATE), 1.0, 6.0, ((0, 8), (1, 4)))
    interval_presoftplus = draw_interval_presoftplus(jax.random.fold_in(key_list[21], 71), 0)
    entry_filter_taps = scatter_about(key_list[5], (TAPS, INNER), 0.5, 3.0, ((1, 4),))
    insert_filter_taps = scatter_about(key_list[6], (TAPS, GROUPS * STATE), 0.5, 3.0, ((1, 4),))
    query_filter_taps = scatter_about(key_list[7], (TAPS, GROUPS * STATE), 0.5, 3.0, ((1, 4),))
    interval_offset = draw_interval_offset(jax.random.fold_in(key_list[21], 71), 0)
    head_fading_exponent = draw_head_fading_exponent(jax.random.fold_in(key_list[21], 71), 0)
    skip_connection_factor = jnp.clip(1.0 + 0.18 * jax.random.normal(key_list[10], (HEADS,), jnp.float32), 0.1, 1.9)
    spike_fading_exponent = draw_spike_fading_exponent(jax.random.fold_in(key_list[21], 71), 0)
    cluster_scaling_vector = jnp.clip(1.0 + 0.18 * jax.random.normal(key_list[12], (INNER,), jnp.float32), 0.1, 1.9)
    sequence_exit_projection = scatter_about(key_list[13], (INNER, D), INNER ** -0.5, 0.09375, ((0, 4),))
    specialist_sample_slice = scatter_about(key_list[14], (TOKENS_B, D), 1.0, 6.0, ((0, 32),))
    specialist_scaling_vector = jnp.clip(1.0 + 0.18 * jax.random.normal(key_list[15], (D,), jnp.float32), 0.1, 1.9)
    chosen_specialists_keys = jax.random.split(jax.random.fold_in(key_list[16], 1), TOKENS_B // TOK_B)
    chosen_specialists_turns = jax.random.permutation(jax.random.fold_in(key_list[16], 3), TOKENS_B // TOK_B)
    chosen_specialists = jax.vmap(lambda own, number: shared_out(jax.random.fold_in(key_list[16], 2), own, number, TOK_B, EXPERTS, TOPK, CAP, 1))(chosen_specialists_keys, chosen_specialists_turns).reshape((TOKENS_B, TOPK))
    dispatcher_affinity_matrix = scatter_about(key_list[17], (TOKENS_B, TOPK), 1.0, 4.0, ((0, 32),), jnp.float32)
    gating_projection = scatter_about(key_list[18], (EXPERTS, D, FF), (D // 16) ** -0.5, 0.5, ((0, 8), (2, 4)))
    expand_projection = scatter_about(key_list[19], (EXPERTS, D, FF), (D // 16) ** -0.5, 0.5, ((0, 8), (2, 4)))
    shrink_projection = scatter_about(key_list[20], (EXPERTS, FF, D), (16 * FF) ** -0.5, 0.03125, ((0, 8), (1, 4)))
    return dict(sequence_entry_features=sequence_entry_features, sequence_exit_gating=sequence_exit_gating, memory_insert_clusters=memory_insert_clusters, memory_query_clusters=memory_query_clusters, interval_presoftplus=interval_presoftplus, entry_filter_taps=entry_filter_taps, insert_filter_taps=insert_filter_taps, query_filter_taps=query_filter_taps, interval_offset=interval_offset, head_fading_exponent=head_fading_exponent, skip_connection_factor=skip_connection_factor, spike_fading_exponent=spike_fading_exponent, cluster_scaling_vector=cluster_scaling_vector, sequence_exit_projection=sequence_exit_projection, specialist_sample_slice=specialist_sample_slice, specialist_scaling_vector=specialist_scaling_vector, chosen_specialists=chosen_specialists, dispatcher_affinity_matrix=dispatcher_affinity_matrix, gating_projection=gating_projection, expand_projection=expand_projection, shrink_projection=shrink_projection)


norm_eps = 1e-05
clamp_top = 7.0
sigmoid_sharp = 1.702
highest = lax.Precision.HIGHEST

def causal_conv(values, kernel):
    length = values.shape[0]
    joined = jnp.pad(values.astype(jnp.float32), ((kernel.shape[0] - 1, 0), (0, 0)))
    summed = jnp.zeros(values.shape, jnp.float32)
    for offset in range(kernel.shape[0]):
        summed = summed + joined[offset:offset + length] * kernel[offset].astype(jnp.float32)
    return jax.nn.silu(summed)

def sequence_reference_result(sequence_entry_features, sequence_exit_gating, memory_insert_clusters, memory_query_clusters, interval_presoftplus, entry_filter_taps, insert_filter_taps, query_filter_taps, interval_offset, head_fading_exponent, skip_connection_factor, spike_fading_exponent, cluster_scaling_vector, sequence_exit_projection):
    per_group = HEADS // GROUPS
    blocks = SEQUENCE_LENGTH // SPAN
    group_cols = HEADS * HEAD // GROUPS
    seq_x = causal_conv(sequence_entry_features, entry_filter_taps)
    seq_b = causal_conv(memory_insert_clusters, insert_filter_taps)
    seq_c = causal_conv(memory_query_clusters, query_filter_taps)
    discretization_interval = jax.nn.softplus(interval_presoftplus.astype(jnp.float32) + interval_offset)
    fading_exponent = spike_fading_exponent - jnp.exp(head_fading_exponent) * discretization_interval
    scaled = (seq_x.reshape(SEQUENCE_LENGTH, HEADS, HEAD) * discretization_interval[:, :, None]).reshape(blocks, SPAN, GROUPS, per_group, HEAD)
    direct = seq_x.reshape(blocks, SPAN, GROUPS, per_group, HEAD)
    gate_z = sequence_exit_gating.reshape(blocks, SPAN, GROUPS, group_cols)
    keys_b = seq_b.reshape(blocks, SPAN, GROUPS, STATE)
    query_c = seq_c.reshape(blocks, SPAN, GROUPS, STATE)
    decays = fading_exponent.reshape(blocks, SPAN, GROUPS, per_group)
    causal = jnp.tril(jnp.ones((SPAN, SPAN), bool))[:, :, None, None]
    skip_heads = skip_connection_factor.reshape(GROUPS, per_group)[:, :, None]
    gain_groups = cluster_scaling_vector.reshape(GROUPS, group_cols)

    def block_step(running, pieces):
        block_x, block_direct, block_z, block_b, block_c, block_decay = pieces
        cumulative = jnp.cumsum(block_decay, axis=0)
        weight = jnp.exp(jnp.where(causal, cumulative[:, None] - cumulative[None, :], -jnp.inf))
        scores = jnp.einsum('tgn,sgn->tsg', block_c, block_b, precision=highest)
        within = jnp.einsum('tsge,sgep->tgep', scores[..., None] * weight, block_x, precision=highest)
        carried = jnp.einsum('tgn,gepn->tgep', block_c, running, precision=highest) * jnp.exp(cumulative)[..., None]
        block_end = cumulative[-1]
        added = jnp.einsum('sgn,sgep->gepn', block_b, block_x * jnp.exp(block_end[None] - cumulative)[..., None], precision=highest)
        mixer_y = within + carried + block_direct * skip_heads
        gated_y = mixer_y.reshape(SPAN, GROUPS, group_cols) * jax.nn.silu(block_z.astype(jnp.float32))
        normed = gated_y * lax.rsqrt(lax.optimization_barrier(jnp.mean(gated_y * gated_y, axis=2, keepdims=True)) + norm_eps) * gain_groups
        return (running * jnp.exp(block_end)[:, :, None, None] + added, normed.astype(jnp.bfloat16))
    initial = jnp.zeros((GROUPS, per_group, HEAD, STATE), jnp.float32)
    normed_all = lax.scan(block_step, initial, (scaled, direct, gate_z, keys_b, query_c, decays))[1]
    normed_all = normed_all.reshape(SEQUENCE_LENGTH, HEADS * HEAD)
    part_cols = HEADS * HEAD // N_TP
    summed = jnp.zeros((SEQUENCE_LENGTH, D), jnp.float32)
    for member in range(N_TP):
        part_sum = jnp.dot(normed_all[:, member * part_cols:(member + 1) * part_cols], sequence_exit_projection[member * part_cols:(member + 1) * part_cols], preferred_element_type=jnp.float32)
        summed = summed + lax.optimization_barrier(part_sum.astype(jnp.bfloat16)).astype(jnp.float32)
    return summed.astype(jnp.bfloat16)

def specialist_reference_result(specialist_sample_slice, specialist_scaling_vector, chosen_specialists, dispatcher_affinity_matrix, gating_projection, expand_projection, shrink_projection):
    as_float = specialist_sample_slice.astype(jnp.float32)
    centred = as_float - lax.optimization_barrier(jnp.mean(as_float, axis=1, keepdims=True))
    normed = (centred * lax.rsqrt(lax.optimization_barrier(jnp.mean(centred * centred, axis=1, keepdims=True)) + norm_eps) * specialist_scaling_vector).astype(jnp.bfloat16)
    route_weight = jnp.exp(dispatcher_affinity_matrix) / lax.optimization_barrier(jnp.sum(jnp.exp(dispatcher_affinity_matrix), axis=1, keepdims=True))
    blocks_b = TOKENS_B // TOK_B
    slots_each = blocks_b * CAP
    flat_routes = chosen_specialists.reshape(blocks_b, TOK_B * TOPK)
    onehot = (flat_routes[:, :, None] == jnp.arange(EXPERTS, dtype=jnp.int32)[None, None, :]).astype(jnp.int32)
    position = lax.optimization_barrier(jnp.sum(onehot * (jnp.cumsum(onehot, axis=1) - 1), axis=2))
    target = (flat_routes * slots_each + jnp.arange(blocks_b, dtype=jnp.int32)[:, None] * CAP + position).reshape(-1)
    token_ids = jnp.arange(TOKENS_B * TOPK, dtype=jnp.int32) // TOPK
    source_table = jnp.full((EXPERTS * slots_each,), TOKENS_B, jnp.int32).at[target].set(token_ids)
    slot_weight = jnp.zeros((EXPERTS * slots_each,), jnp.float32).at[target].set(route_weight.reshape(-1))
    padded = jnp.concatenate([normed, jnp.zeros((1, D), jnp.bfloat16)], axis=0)
    part_cols = FF // N_TP

    def expert_step(running, pieces):
        gate_one, up_one, down_one, rows_index, rows_weight = pieces
        rows_in = padded[rows_index]
        gate_h = jnp.dot(rows_in, gate_one, preferred_element_type=jnp.float32)
        up_h = jnp.dot(rows_in, up_one, preferred_element_type=jnp.float32)
        clipped = jnp.minimum(gate_h, clamp_top)
        hidden_act = (clipped * jax.nn.sigmoid(sigmoid_sharp * clipped) * (jnp.clip(up_h, -clamp_top, clamp_top) + 1.0)).astype(jnp.bfloat16)
        result = jnp.zeros((slots_each, D), jnp.float32)
        for member in range(N_TP):
            part_sum = jnp.dot(hidden_act[:, member * part_cols:(member + 1) * part_cols], down_one[member * part_cols:(member + 1) * part_cols], preferred_element_type=jnp.float32)
            result = result + lax.optimization_barrier(part_sum.astype(jnp.bfloat16)).astype(jnp.float32)
        result = lax.optimization_barrier(result.astype(jnp.bfloat16)).astype(jnp.float32)
        return (running.at[rows_index].add(rows_weight[:, None] * result), None)
    initial = jnp.zeros((TOKENS_B + 1, D), jnp.float32)
    summed = lax.scan(expert_step, initial, (gating_projection, expand_projection, shrink_projection, source_table.reshape(EXPERTS, slots_each), slot_weight.reshape(EXPERTS, slots_each)))[0]
    return summed[:TOKENS_B].astype(jnp.bfloat16)

def reference(sequence_entry_features, sequence_exit_gating, memory_insert_clusters, memory_query_clusters, interval_presoftplus, entry_filter_taps, insert_filter_taps, query_filter_taps, interval_offset, head_fading_exponent, skip_connection_factor, spike_fading_exponent, cluster_scaling_vector, sequence_exit_projection, specialist_sample_slice, specialist_scaling_vector, chosen_specialists, dispatcher_affinity_matrix, gating_projection, expand_projection, shrink_projection):
    return (sequence_reference_result(sequence_entry_features, sequence_exit_gating, memory_insert_clusters, memory_query_clusters, interval_presoftplus, entry_filter_taps, insert_filter_taps, query_filter_taps, interval_offset, head_fading_exponent, skip_connection_factor, spike_fading_exponent, cluster_scaling_vector, sequence_exit_projection), specialist_reference_result(specialist_sample_slice, specialist_scaling_vector, chosen_specialists, dispatcher_affinity_matrix, gating_projection, expand_projection, shrink_projection))
```

```python
import functools
import jax
import jax.numpy as jnp
from jax import lax
from jax.experimental import pallas as pl
from jax.experimental.pallas import tpu as pltpu
from jax.sharding import PartitionSpec as P

HEAD = 64
STATE = 128
SPAN = 128
RIM = 8
LANES = 128

norm_eps = 1e-05
clamp_top = 7.0
sigmoid_sharp = 1.702
highest = lax.Precision.HIGHEST


def passed_along(block, axis, distance):
    devices = range(lax.axis_size(axis))
    route = [(i - distance, i) for i in devices if i - distance in devices]
    return lax.ppermute(block, axis, route)


def conv_block(buf, first, value_ref, rim_ref, taps_ref):
    @pl.when(first)
    def _():
        buf[0:RIM, :] = rim_ref[...].astype(jnp.float32)

    @pl.when(jnp.logical_not(first))
    def _():
        buf[0:RIM, :] = buf[SPAN : SPAN + RIM, :]

    buf[RIM : RIM + SPAN, :] = value_ref[...].astype(jnp.float32)
    taps = taps_ref[...].astype(jnp.float32)
    count = taps.shape[0]
    total = buf[RIM : RIM + SPAN, :] * taps[count - 1 : count]
    for j in range(count - 1):
        start = RIM - (count - 1) + j
        total = total + buf[start : start + SPAN, :] * taps[j : j + 1]
    return total * jax.nn.sigmoid(total)


def spread(cols, h, width):
    return jnp.broadcast_to(cols[:, h : h + 1], (SPAN, width))


def state_kernel(per_group, groups, x_ref, xr_ref, xt_ref, b_ref, br_ref, bt_ref, lw_ref, end_ref,
                 state_ref, xbuf, bbuf):
    first = pl.program_id(0) == 0
    x = conv_block(xbuf, first, x_ref, xr_ref, xt_ref)
    b = conv_block(bbuf, first, b_ref, br_ref, bt_ref)

    @pl.when(first)
    def _():
        state_ref[...] = jnp.zeros_like(state_ref)

    lw = lw_ref[...]
    low = lax.broadcasted_iota(jnp.int32, (SPAN, 2 * HEAD), 1) < HEAD
    for g in range(groups):
        bt = b[:, g * STATE : (g + 1) * STATE].T.astype(jnp.bfloat16)
        for pair in range(per_group // 2):
            h = g * per_group + 2 * pair
            cols = slice(h * HEAD, (h + 2) * HEAD)
            factor = jnp.exp(jnp.where(low, spread(lw, h, 2 * HEAD), spread(lw, h + 1, 2 * HEAD)))
            xw = (x[:, cols] * factor).astype(jnp.bfloat16)
            added = jnp.dot(bt, xw, preferred_element_type=jnp.float32)
            state_ref[:, cols] = state_ref[:, cols] * end_ref[0, :, cols] + added


def output_kernel(per_group, groups, x_ref, xr_ref, xt_ref, b_ref, br_ref, bt_ref, c_ref, cr_ref,
                  ct_ref, z_ref, lw_ref, cum_ref, row_ref, end_ref, enter_ref, skip_ref, scale_ref,
                  out_ref, xbuf, bbuf, cbuf, state, ybuf):
    first = pl.program_id(0) == 0
    x = conv_block(xbuf, first, x_ref, xr_ref, xt_ref)
    b = conv_block(bbuf, first, b_ref, br_ref, bt_ref)
    c = conv_block(cbuf, first, c_ref, cr_ref, ct_ref)

    @pl.when(first)
    def _():
        state[...] = enter_ref[...]

    lw = lw_ref[...]
    cum = cum_ref[...]
    low = lax.broadcasted_iota(jnp.int32, (SPAN, 2 * HEAD), 1) < HEAD
    causal = lax.broadcasted_iota(jnp.int32, (SPAN, SPAN), 0) >= lax.broadcasted_iota(
        jnp.int32, (SPAN, SPAN), 1
    )
    group_cols = per_group * HEAD
    for g in range(groups):
        bg = b[:, g * STATE : (g + 1) * STATE]
        bt = bg.T.astype(jnp.bfloat16)
        cg = c[:, g * STATE : (g + 1) * STATE].astype(jnp.bfloat16)
        scores = jnp.dot(cg, bt, preferred_element_type=jnp.float32)
        squares = jnp.zeros((SPAN, 2 * HEAD), jnp.float32)
        for pair in range(per_group // 2):
            h = g * per_group + 2 * pair
            cols = slice(h * HEAD, (h + 2) * HEAD)
            xp = x[:, cols]
            cum_0, cum_1 = spread(cum, h, SPAN), spread(cum, h + 1, SPAN)
            m_0 = scores * jnp.exp(jnp.where(causal, cum_0 + row_ref[0, h : h + 1, :], -jnp.inf))
            m_1 = scores * jnp.exp(jnp.where(causal, cum_1 + row_ref[0, h + 1 : h + 2, :], -jnp.inf))
            mixing = jnp.concatenate([m_0.astype(jnp.bfloat16), m_1.astype(jnp.bfloat16)], axis=1)
            x_0 = jnp.where(low, xp, 0.0).astype(jnp.bfloat16)
            x_1 = jnp.where(low, 0.0, xp).astype(jnp.bfloat16)
            y = jnp.dot(
                mixing, jnp.concatenate([x_0, x_1], axis=0), preferred_element_type=jnp.float32
            )
            before = state[:, cols]
            carried = jnp.dot(cg, before.astype(jnp.bfloat16), preferred_element_type=jnp.float32)
            y = y + carried * jnp.exp(jnp.where(low, cum_0, cum_1)) + xp * skip_ref[:, cols]
            factor = jnp.exp(jnp.where(low, spread(lw, h, 2 * HEAD), spread(lw, h + 1, 2 * HEAD)))
            xw = (xp * factor).astype(jnp.bfloat16)
            added = jnp.dot(bt, xw, preferred_element_type=jnp.float32)
            state[:, cols] = before * end_ref[0, :, cols] + added
            gate = z_ref[:, cols].astype(jnp.float32)
            gated = y * (gate * jax.nn.sigmoid(gate))
            squares = squares + gated * gated
            ybuf[:, cols] = gated
        mean = jnp.sum(squares, axis=1, keepdims=True) / group_cols
        inverse = lax.rsqrt(mean + norm_eps)
        cols = slice(g * group_cols, (g + 1) * group_cols)
        out_ref[:, cols] = (ybuf[:, cols] * inverse * scale_ref[:, cols]).astype(jnp.bfloat16)


def entering_state(own_state, own_decay):
    size, mine = (lax.axis_size("ep"), lax.axis_index("ep"))
    rows = own_state.shape[0]
    total = own_state
    decay = own_decay

    def joined():
        return jnp.concatenate(
            [total, jnp.broadcast_to(decay, (RIM, decay.shape[1]))], axis=0
        ).astype(jnp.bfloat16)

    distance = 1
    while distance < size:
        came = passed_along(joined(), "ep", distance)
        there = mine >= distance
        earlier = came[:rows].astype(jnp.float32)
        earlier_decay = jnp.where(there, came[rows : rows + 1].astype(jnp.float32), 1.0)
        total = earlier * decay + total
        decay = earlier_decay * decay
        distance *= 2
    return passed_along(total.astype(jnp.bfloat16), "ep", 1).astype(jnp.float32)


def mixer_half(
    sequence_entry_features,
    sequence_exit_gating,
    memory_insert_clusters,
    memory_query_clusters,
    interval_presoftplus,
    entry_filter_taps,
    insert_filter_taps,
    query_filter_taps,
    interval_offset,
    head_fading_exponent,
    skip_connection_factor,
    spike_fading_exponent,
    cluster_scaling_vector,
    sequence_exit_projection,
):
    tok_rows = sequence_entry_features.shape[0]
    local_heads = interval_offset.shape[0]
    local_groups = memory_insert_clusters.shape[1] // STATE
    per_group = local_heads // local_groups
    inner_cols = sequence_entry_features.shape[1]
    state_cols = memory_insert_clusters.shape[1]
    last_rows = jnp.concatenate(
        [
            sequence_entry_features[tok_rows - RIM :],
            memory_insert_clusters[tok_rows - RIM :],
            memory_query_clusters[tok_rows - RIM :],
        ],
        axis=1,
    )
    rims = passed_along(last_rows, "ep", 1)
    rim_x = rims[:, :inner_cols]
    rim_b = rims[:, inner_cols : inner_cols + state_cols]
    rim_c = rims[:, inner_cols + state_cols :]
    blocks = tok_rows // SPAN
    interval = jax.nn.softplus(interval_presoftplus.astype(jnp.float32) + interval_offset)
    fading = spike_fading_exponent - jnp.exp(head_fading_exponent) * interval
    lower = jnp.tril(jnp.ones((SPAN, SPAN), jnp.float32))
    cumulative = jnp.einsum(
        "ts,csh->cth", lower, fading.reshape(blocks, SPAN, local_heads), precision=highest
    )
    log_step = jnp.log(interval).reshape(blocks, SPAN, local_heads)
    block_end = cumulative[:, -1:]
    key_log = (log_step - cumulative + block_end).reshape(tok_rows, local_heads)
    row_log = jnp.swapaxes(log_step - cumulative, 1, 2)
    end_factor = jnp.repeat(jnp.exp(block_end), HEAD, axis=2)
    own_decay = jnp.repeat(jnp.exp(jnp.sum(block_end, axis=0)), HEAD, axis=1)
    cumulative = cumulative.reshape(tok_rows, local_heads)

    def rows_of(width):
        return pl.BlockSpec((SPAN, width), lambda i: (i, 0))

    def fixed(shape):
        return pl.BlockSpec(shape, lambda i: (0, 0))

    def block_of(rows, width):
        return pl.BlockSpec((1, rows, width), lambda i: (i, 0, 0))

    def cost(dots):
        return pl.CostEstimate(
            flops=dots * tok_rows * inner_cols * STATE * 8,
            bytes_accessed=dots * tok_rows * inner_cols * 8,
            transcendentals=0,
        )

    taps = entry_filter_taps.shape[0]
    x_specs = [rows_of(inner_cols), fixed((RIM, inner_cols)), fixed((taps, inner_cols))]
    s_specs = [rows_of(state_cols), fixed((RIM, state_cols)), fixed((taps, state_cols))]
    x_args = (sequence_entry_features, rim_x, entry_filter_taps)
    b_args = (memory_insert_clusters, rim_b, insert_filter_taps)
    c_args = (memory_query_clusters, rim_c, query_filter_taps)
    own_state = pl.pallas_call(
        functools.partial(state_kernel, per_group, local_groups),
        grid=(blocks,),
        in_specs=x_specs + s_specs + [rows_of(local_heads), block_of(1, inner_cols)],
        out_specs=fixed((STATE, inner_cols)),
        out_shape=jax.ShapeDtypeStruct((STATE, inner_cols), jnp.float32),
        scratch_shapes=[
            pltpu.VMEM((SPAN + RIM, inner_cols), jnp.float32),
            pltpu.VMEM((SPAN + RIM, state_cols), jnp.float32),
        ],
        cost_estimate=cost(1),
        name="own_state",
    )(*x_args, *b_args, key_log, end_factor)
    entering = entering_state(own_state, own_decay)
    normed = pl.pallas_call(
        functools.partial(output_kernel, per_group, local_groups),
        grid=(blocks,),
        in_specs=x_specs + s_specs + s_specs + [
            rows_of(inner_cols),
            rows_of(local_heads),
            rows_of(local_heads),
            block_of(local_heads, SPAN),
            block_of(1, inner_cols),
            fixed((STATE, inner_cols)),
            fixed((1, inner_cols)),
            fixed((1, inner_cols)),
        ],
        out_specs=rows_of(inner_cols),
        out_shape=jax.ShapeDtypeStruct((tok_rows, inner_cols), jnp.bfloat16),
        scratch_shapes=[
            pltpu.VMEM((SPAN + RIM, inner_cols), jnp.float32),
            pltpu.VMEM((SPAN + RIM, state_cols), jnp.float32),
            pltpu.VMEM((SPAN + RIM, state_cols), jnp.float32),
            pltpu.VMEM((STATE, inner_cols), jnp.float32),
            pltpu.VMEM((SPAN, inner_cols), jnp.float32),
        ],
        cost_estimate=cost(3),
        name="mixer_output",
    )(
        *x_args, *b_args, *c_args, sequence_exit_gating, key_log, cumulative, row_log, end_factor,
        entering, jnp.repeat(skip_connection_factor, HEAD)[None], cluster_scaling_vector[None],
    )
    return lax.psum_scatter(
        jnp.dot(normed, sequence_exit_projection, preferred_element_type=jnp.float32).astype(
            jnp.bfloat16
        ),
        "tp",
        scatter_dimension=0,
        tiled=True,
    )


def experts_half(
    specialist_sample_slice,
    specialist_scaling_vector,
    chosen_specialists,
    dispatcher_affinity_matrix,
    gating_projection,
    expand_projection,
    shrink_projection,
):
    tok_rows = specialist_sample_slice.shape[0]
    feature_count = specialist_sample_slice.shape[1]
    top_count = chosen_specialists.shape[1]
    experts = lax.axis_size("ep")
    groups_tp = lax.axis_size("tp")
    capacity = tok_rows * top_count * 5 // (4 * experts)
    as_float = specialist_sample_slice.astype(jnp.float32)
    centred = as_float - jnp.mean(as_float, axis=1, keepdims=True)
    normed = (
        centred
        * lax.rsqrt(jnp.mean(centred * centred, axis=1, keepdims=True) + norm_eps)
        * specialist_scaling_vector
    ).astype(jnp.bfloat16)
    route_weight = jnp.exp(dispatcher_affinity_matrix) / jnp.sum(
        jnp.exp(dispatcher_affinity_matrix), axis=1, keepdims=True
    )
    flat_routes = chosen_specialists.reshape(-1)
    onehot = (flat_routes[:, None] == jnp.arange(experts, dtype=jnp.int32)[None, :]).astype(
        jnp.int32
    )
    position = jnp.sum(onehot * (jnp.cumsum(onehot, axis=0) - 1), axis=1)
    target = flat_routes * capacity + position
    token_ids = jnp.arange(tok_rows * top_count, dtype=jnp.int32) // top_count
    source_table = jnp.full((experts * capacity,), tok_rows, jnp.int32).at[target].set(token_ids)
    padded = jnp.concatenate([normed, jnp.zeros((1, feature_count), jnp.bfloat16)], axis=0)
    outgoing = padded[source_table].reshape(experts, capacity, feature_count)
    arrived = lax.all_to_all(outgoing, "ep", split_axis=0, concat_axis=0, tiled=True)
    shard_rows = lax.all_gather(arrived, "tp", axis=0, tiled=True)
    rows_in = shard_rows.reshape(-1, feature_count)
    gate_h = jnp.dot(rows_in, gating_projection[0], preferred_element_type=jnp.float32)
    up_h = jnp.dot(rows_in, expand_projection[0], preferred_element_type=jnp.float32)
    clipped = jnp.minimum(gate_h, clamp_top)
    hidden_act = (
        (
            clipped
            * jax.nn.sigmoid(sigmoid_sharp * clipped)
            * (jnp.clip(up_h, -clamp_top, clamp_top) + 1.0)
        )
        .astype(jnp.bfloat16)
        .reshape(shard_rows.shape[0], capacity, -1)
    )
    hidden_act = hidden_act.reshape(groups_tp * experts * capacity, -1)
    summed = lax.psum_scatter(
        jnp.dot(hidden_act, shrink_projection[0], preferred_element_type=jnp.float32).astype(
            jnp.bfloat16
        ),
        "tp",
        scatter_dimension=0,
        tiled=True,
    )
    returned = lax.all_to_all(
        summed.reshape(experts, capacity, feature_count),
        "ep",
        split_axis=0,
        concat_axis=0,
        tiled=True,
    )
    slot_out = returned.reshape(experts * capacity, feature_count)[target].reshape(
        tok_rows, top_count, feature_count
    )
    combined = jnp.einsum("tk,tkd->td", route_weight, slot_out.astype(jnp.float32))
    return combined.astype(jnp.bfloat16)


def routing_kernel(experts, x_ref, scale_ref, chosen_ref, score_ref, out_ref):
    features = x_ref.shape[1]
    rows, top_count = chosen_ref.shape
    value = x_ref[...].astype(jnp.float32)
    centred = value - jnp.mean(value, axis=1, keepdims=True)
    spread_of = jnp.mean(centred * centred, axis=1, keepdims=True)
    normed = centred * lax.rsqrt(spread_of + norm_eps) * scale_ref[...]
    out_ref[:, :features] = normed.astype(jnp.bfloat16)
    raised = jnp.exp(score_ref[...])
    weight = raised / jnp.sum(raised, axis=1, keepdims=True)
    lane = lax.broadcasted_iota(jnp.int32, (rows, LANES), 1)
    named = lax.rem(lane, experts)
    chosen = chosen_ref[...]
    held = jnp.zeros((rows, LANES), jnp.float32)
    share = jnp.zeros((rows, LANES), jnp.float32)
    for k in range(top_count):
        same = chosen[:, k : k + 1] == named
        held = held + jnp.where(same, 1.0, 0.0)
        share = share + jnp.where(same, weight[:, k : k + 1], 0.0)
    earlier = lax.broadcasted_iota(jnp.int32, (rows, rows), 0) > lax.broadcasted_iota(
        jnp.int32, (rows, rows), 1
    )
    place = jnp.dot(
        jnp.where(earlier, 1.0, 0.0).astype(jnp.bfloat16),
        held.astype(jnp.bfloat16),
        preferred_element_type=jnp.float32,
    )
    place = jnp.where(held > 0.0, place, 255.0)
    coarse = share.astype(jnp.bfloat16).astype(jnp.float32)
    table = jnp.where(lane < experts, place, jnp.where(lane < 2 * experts, coarse, share - coarse))
    out_ref[:, features:] = table.astype(jnp.bfloat16)


def experts_kernel(
    experts, capacity, tokens_ref, gate_ref, up_ref, down_ref, out_ref,
    tokens, slots, own, outgoing, incoming, place, place_next, from_x, from_y,
    to_y, came_y, to_x, came_x, keep_a, keep_b, to_z, from_z,
    token_sem, core_send, core_recv, x_send, x_recv, y_send, y_recv,
    a_send, a_recv, b_send, b_recv, z_send, z_recv,
):
    depth = experts // 2
    steps = experts
    ep, tp = lax.axis_index("ep"), lax.axis_index("tp")
    z, y, x, core = ep // 2, ep % 2, tp // 2, tp % 2
    next_ep = z * 2 + 1 - y
    sibling = {"tp": x * 2 + 1 - core}
    x_next = {"tp": (1 - x) * 2 + core}
    y_next = {"ep": next_ep}
    rows = out_ref.shape[0]
    features = out_ref.shape[1]
    half = features // 2
    mesh_id = pl.DeviceIdType.MESH

    def z_next(k):
        return {"ep": ((z + k) % depth) * 2 + y}

    def fetch(s):
        k, dy = (s // 2 + 1) % depth, 1 - s % 2
        block = ((z + k) % depth) * 2 + (y + dy) % 2
        span = 4 * rows
        return pltpu.make_async_copy(
            tokens_ref.at[pl.ds(pl.multiple_of(block * span, span), span)],
            tokens.at[s % 2],
            token_sem.at[s % 2],
        )

    def remote(source, target, send, recv, device):
        return pltpu.make_async_remote_copy(
            src_ref=source, dst_ref=target, send_sem=send, recv_sem=recv,
            device_id=device, device_id_type=mesh_id,
        )

    def core_copy(s):
        return remote(outgoing.at[s], incoming.at[s], core_send.at[s], core_recv.at[s], sibling)

    def x_copy(s):
        return remote(own.at[s, 0, 1], from_x.at[s], x_send.at[s], x_recv.at[s], x_next)

    def y_copy(i):
        return remote(own.at[2 * i, 1], from_y.at[i], y_send.at[i], y_recv.at[i], y_next)

    def a_copy(i):
        return remote(to_y.at[i], came_y.at[i], a_send.at[i], a_recv.at[i], y_next)

    def b_copy(i):
        return remote(to_x.at[i], came_x.at[i], b_send.at[i], b_recv.at[i], x_next)

    def z_copy(i):
        return remote(to_z.at[i], from_z.at[i], z_send.at[i], z_recv.at[i], z_next(i + 1))

    fetch(0).start()
    barrier = pltpu.get_barrier_semaphore()
    partners = [sibling, x_next, y_next] + [z_next(k) for k in range(1, depth)]
    for partner in partners:
        pl.semaphore_signal(barrier, inc=1, device_id=partner, device_id_type=mesh_id)
    pl.semaphore_wait(barrier, len(partners))

    lane = lax.broadcasted_iota(jnp.int32, (rows, LANES), 1)
    lane_value = lane.astype(jnp.float32)
    slot_lane = lax.broadcasted_iota(jnp.int32, (capacity, LANES), 1)

    def chosen_slots(table, expert):
        column = jnp.sum(jnp.where(lane == expert, table, 0.0), axis=1, keepdims=True)
        return jnp.where(column == lane_value, 1.0, 0.0)

    def compute(s):
        weights = []
        for dx in (0, 1):
            for q in (0, 1):
                c = core if q == 0 else 1 - core
                block = ((x + dx) % 2) * 2 + c
                start = pl.multiple_of(block * rows, rows)
                arrived = tokens[s % 2, pl.ds(start, rows), :]
                table = arrived[:, features:].astype(jnp.float32)
                picked = chosen_slots(table, ep)
                if q == 0:
                    place[s, dx] = picked.astype(jnp.bfloat16)
                    place_next[s, dx] = chosen_slots(table, next_ep).astype(jnp.bfloat16)
                select = picked.T[:capacity].astype(jnp.bfloat16)
                taken = jnp.dot(select, arrived, preferred_element_type=jnp.float32)
                first = (dx * 2 + q) * capacity
                slots[first : first + capacity, :] = taken[:, :features].astype(jnp.bfloat16)
                mine = (slot_lane == experts + ep) | (slot_lane == 2 * experts + ep)
                weights.append(
                    jnp.sum(jnp.where(mine, taken[:, features:], 0.0), axis=1, keepdims=True)
                )
        value = slots[...]
        gate_h = jnp.dot(value, gate_ref[...], preferred_element_type=jnp.float32)
        up_h = jnp.dot(value, up_ref[...], preferred_element_type=jnp.float32)
        clipped = jnp.minimum(gate_h, clamp_top)
        act = (
            clipped
            * jax.nn.sigmoid(sigmoid_sharp * clipped)
            * (jnp.clip(up_h, -clamp_top, clamp_top) + 1.0)
        ).astype(jnp.bfloat16)
        for side in (0, 1):
            columns = slice(side * half, (side + 1) * half)
            part = jnp.dot(act, down_ref[:, columns], preferred_element_type=jnp.float32)
            for dx in (0, 1):
                for q in (0, 1):
                    first = (dx * 2 + q) * capacity
                    scaled = (part[first : first + capacity] * weights[dx * 2 + q]).astype(
                        jnp.bfloat16
                    )
                    if q == 0:
                        own[s, side, dx] = scaled
                    else:
                        outgoing[s, side, dx] = scaled

    def spread_out(where, value):
        return jnp.dot(where[:, :capacity], value, preferred_element_type=jnp.float32)

    def step(s, carry):
        @pl.when(s < steps)
        def _():
            @pl.when(s + 1 < steps)
            def _():
                fetch(s + 1).start()

            fetch(s).wait()
            compute(s)

        @pl.when((s >= 1) & (s <= steps))
        def _():
            t = s - 1
            core_copy(t).wait_recv()
            for side in (0, 1):
                for dx in (0, 1):
                    own[t, side, dx] = (
                        own[t, side, dx].astype(jnp.float32)
                        + incoming[t, side, dx].astype(jnp.float32)
                    ).astype(jnp.bfloat16)

        @pl.when(s < steps)
        def _():
            core_copy(s).start()

        i = (s - 4) // 2

        @pl.when((s >= 4) & (s % 2 == 0) & (i < depth))
        def _():
            far, near = 2 * i, 2 * i + 1
            x_copy(far).wait_recv()
            where = place[far, 0]
            to_y[i] = (spread_out(where, own[far, 0, 0]) + spread_out(where, from_x[far])).astype(
                jnp.bfloat16
            )
            y_copy(i).wait_recv()
            to_x[i] = (
                spread_out(place[near, 1], own[near, 1, 1])
                + spread_out(place_next[near, 1], from_y[i, 1])
            ).astype(jnp.bfloat16)
            x_copy(near).wait_recv()
            where = place[near, 0]
            keep_a[i] = spread_out(where, own[near, 0, 0]) + spread_out(where, from_x[near])
            keep_b[i] = spread_out(where, own[near, 1, 0]) + spread_out(
                place_next[near, 0], from_y[i, 0]
            )
            a_copy(i).start()
            b_copy(i).start()

        @pl.when((s >= 1) & (s <= steps))
        def _():
            t = s - 1
            x_copy(t).start()

            @pl.when(t % 2 == 0)
            def _():
                y_copy(t // 2).start()

        j = (s - 6) // 2

        @pl.when((s >= 6) & (s % 2 == 0) & (j < depth))
        def _():
            a_copy(j).wait_recv()
            b_copy(j).wait_recv()
            sum_a = keep_a[j] + came_y[j].astype(jnp.float32)
            sum_b = keep_b[j] + came_x[j].astype(jnp.float32)

            @pl.when(j < depth - 1)
            def _():
                to_z[j, :, :half] = sum_a.astype(jnp.bfloat16)
                to_z[j, :, half:] = sum_b.astype(jnp.bfloat16)
                z_copy(j).start()

            @pl.when(j == depth - 1)
            def _():
                keep_a[j] = sum_a
                keep_b[j] = sum_b

        return carry

    lax.fori_loop(0, 2 * depth + 5, step, 0)
    for i in range(depth - 1):
        z_copy(i).wait_recv()
    for side, keep in ((0, keep_a), (1, keep_b)):
        columns = slice(side * half, (side + 1) * half)
        total = keep[depth - 1]
        for i in range(depth - 1):
            total = total + from_z[i, :, columns].astype(jnp.float32)
        out_ref[:, columns] = total.astype(jnp.bfloat16)
    for s in range(steps):
        core_copy(s).wait_send()
        x_copy(s).wait_send()
    for i in range(depth):
        y_copy(i).wait_send()
        a_copy(i).wait_send()
        b_copy(i).wait_send()
    for i in range(depth - 1):
        z_copy(i).wait_send()


def dense_experts_fit(tok_rows, top_count, capacity):
    experts = lax.axis_size("ep")
    fits = experts % 2 == 0 and experts >= 4 and 3 * experts <= LANES and lax.axis_size("tp") == 4
    return fits and 2 * top_count >= experts and tok_rows == LANES and capacity % 16 == 0


def gathered_tokens(
    specialist_sample_slice, specialist_scaling_vector, chosen_specialists, dispatcher_affinity_matrix
):
    rows, features = specialist_sample_slice.shape
    marked = pl.pallas_call(
        functools.partial(routing_kernel, lax.axis_size("ep")),
        out_shape=jax.ShapeDtypeStruct((rows, features + LANES), jnp.bfloat16),
        name="routing",
    )(
        specialist_sample_slice, specialist_scaling_vector[None], chosen_specialists,
        dispatcher_affinity_matrix,
    )
    return lax.all_gather(marked, ("ep", "tp"), axis=0, tiled=True)


def experts_dense(
    tokens, rows, capacity, gating_projection, expand_projection, shrink_projection
):
    experts = lax.axis_size("ep")
    features = gating_projection.shape[1]
    half, depth, steps = features // 2, experts // 2, experts
    hidden = gating_projection.shape[2]
    narrow = jnp.bfloat16
    dma = pltpu.SemaphoreType.DMA
    work = 2 * experts * 4 * capacity * features * hidden * 3
    return pl.pallas_call(
        functools.partial(experts_kernel, experts, capacity),
        in_specs=[pl.BlockSpec(memory_space=pl.ANY)]
        + [pl.BlockSpec(memory_space=pltpu.VMEM)] * 3,
        out_specs=pl.BlockSpec(memory_space=pltpu.VMEM),
        out_shape=jax.ShapeDtypeStruct((rows, features), narrow),
        scratch_shapes=[
            pltpu.VMEM((2, 4 * rows, features + LANES), narrow),
            pltpu.VMEM((4 * capacity, features), narrow),
            pltpu.VMEM((steps, 2, 2, capacity, half), narrow),
            pltpu.VMEM((steps, 2, 2, capacity, half), narrow),
            pltpu.VMEM((steps, 2, 2, capacity, half), narrow),
            pltpu.VMEM((steps, 2, rows, LANES), narrow),
            pltpu.VMEM((steps, 2, rows, LANES), narrow),
            pltpu.VMEM((steps, capacity, half), narrow),
            pltpu.VMEM((depth, 2, capacity, half), narrow),
            pltpu.VMEM((depth, rows, half), narrow),
            pltpu.VMEM((depth, rows, half), narrow),
            pltpu.VMEM((depth, rows, half), narrow),
            pltpu.VMEM((depth, rows, half), narrow),
            pltpu.VMEM((depth, rows, half), jnp.float32),
            pltpu.VMEM((depth, rows, half), jnp.float32),
            pltpu.VMEM((depth - 1, rows, features), narrow),
            pltpu.VMEM((depth - 1, rows, features), narrow),
            dma((2,)), dma((steps,)), dma((steps,)), dma((steps,)), dma((steps,)),
            dma((depth,)), dma((depth,)), dma((depth,)), dma((depth,)), dma((depth,)),
            dma((depth,)), dma((depth - 1,)), dma((depth - 1,)),
        ],
        compiler_params=pltpu.CompilerParams(
            collective_id=0, has_side_effects=True, vmem_limit_bytes=60 * 1024 * 1024
        ),
        cost_estimate=pl.CostEstimate(
            flops=8 * work, bytes_accessed=4 * tokens.size, transcendentals=0
        ),
        name="experts",
    )(tokens, gating_projection[0], expand_projection[0], shrink_projection[0])


def body(
    sequence_entry_features,
    sequence_exit_gating,
    memory_insert_clusters,
    memory_query_clusters,
    interval_presoftplus,
    entry_filter_taps,
    insert_filter_taps,
    query_filter_taps,
    interval_offset,
    head_fading_exponent,
    skip_connection_factor,
    spike_fading_exponent,
    cluster_scaling_vector,
    sequence_exit_projection,
    specialist_sample_slice,
    specialist_scaling_vector,
    chosen_specialists,
    dispatcher_affinity_matrix,
    gating_projection,
    expand_projection,
    shrink_projection,
):
    tok_rows, top_count = chosen_specialists.shape
    capacity = tok_rows * top_count * 5 // (4 * lax.axis_size("ep"))
    dense = dense_experts_fit(tok_rows, top_count, capacity)
    if dense:
        tokens = gathered_tokens(
            specialist_sample_slice,
            specialist_scaling_vector,
            chosen_specialists,
            dispatcher_affinity_matrix,
        )
    mixed = mixer_half(
        sequence_entry_features,
        sequence_exit_gating,
        memory_insert_clusters,
        memory_query_clusters,
        interval_presoftplus,
        entry_filter_taps,
        insert_filter_taps,
        query_filter_taps,
        interval_offset,
        head_fading_exponent,
        skip_connection_factor,
        spike_fading_exponent,
        cluster_scaling_vector,
        sequence_exit_projection,
    )
    if dense:
        moe_out = experts_dense(
            tokens, tok_rows, capacity, gating_projection, expand_projection, shrink_projection
        )
        return (mixed, moe_out)
    moe_out = experts_half(
        specialist_sample_slice,
        specialist_scaling_vector,
        chosen_specialists,
        dispatcher_affinity_matrix,
        gating_projection,
        expand_projection,
        shrink_projection,
    )
    return (mixed, moe_out)


def solution(mesh):
    in_specs = (
        P("ep", "tp"),
        P("ep", "tp"),
        P("ep", "tp"),
        P("ep", "tp"),
        P("ep", "tp"),
        P(None, "tp"),
        P(None, "tp"),
        P(None, "tp"),
        P("tp"),
        P("tp"),
        P("tp"),
        P("ep", "tp"),
        P("tp"),
        P("tp", None),
        P(("ep", "tp"), None),
        P(),
        P(("ep", "tp"), None),
        P(("ep", "tp"), None),
        P("ep", None, "tp"),
        P("ep", None, "tp"),
        P("ep", "tp", None),
    )
    out_specs = (P(("ep", "tp"), None), P(("ep", "tp"), None))
    return jax.shard_map(body, mesh=mesh, in_specs=in_specs, out_specs=out_specs, check_vma=False)
```

```python
import functools
import jax
import jax.numpy as jnp
from jax import lax
from jax.experimental import pallas as pl
from jax.experimental.pallas import tpu as pltpu
from jax.sharding import PartitionSpec as P

HEAD = 64
STATE = 128
SPAN = 128
RIM = 8
LANES = 128
MIX_ROWS = 32

norm_eps = 1e-05
clamp_top = 7.0
sigmoid_sharp = 1.702
highest = lax.Precision.HIGHEST


def passed_along(block, axis, distance):
    devices = range(lax.axis_size(axis))
    route = [(i - distance, i) for i in devices if i - distance in devices]
    return lax.ppermute(block, axis, route)


def conv_block(buf, first, value_ref, rim_ref, taps_ref):
    @pl.when(first)
    def _():
        buf[0:RIM, :] = rim_ref[...].astype(jnp.float32)

    @pl.when(jnp.logical_not(first))
    def _():
        buf[0:RIM, :] = buf[SPAN : SPAN + RIM, :]

    buf[RIM : RIM + SPAN, :] = value_ref[...].astype(jnp.float32)
    taps = taps_ref[...].astype(jnp.float32)
    count = taps.shape[0]
    total = buf[RIM : RIM + SPAN, :] * taps[count - 1 : count]
    for j in range(count - 1):
        start = RIM - (count - 1) + j
        total = total + buf[start : start + SPAN, :] * taps[j : j + 1]
    return total * jax.nn.sigmoid(total)


def spread(cols, h, width):
    return jnp.broadcast_to(cols[:, h : h + 1], (SPAN, width))


def state_kernel(per_group, groups, x_ref, xr_ref, xt_ref, b_ref, br_ref, bt_ref, lw_ref, end_ref,
                 state_ref, xbuf, bbuf):
    first = pl.program_id(0) == 0
    x = conv_block(xbuf, first, x_ref, xr_ref, xt_ref)
    b = conv_block(bbuf, first, b_ref, br_ref, bt_ref)

    @pl.when(first)
    def _():
        state_ref[...] = jnp.zeros_like(state_ref)

    lw = lw_ref[...]
    low = lax.broadcasted_iota(jnp.int32, (SPAN, 2 * HEAD), 1) < HEAD
    for g in range(groups):
        bt = b[:, g * STATE : (g + 1) * STATE].T.astype(jnp.bfloat16)
        for pair in range(per_group // 2):
            h = g * per_group + 2 * pair
            cols = slice(h * HEAD, (h + 2) * HEAD)
            factor = jnp.exp(jnp.where(low, spread(lw, h, 2 * HEAD), spread(lw, h + 1, 2 * HEAD)))
            xw = (x[:, cols] * factor).astype(jnp.bfloat16)
            added = jnp.dot(bt, xw, preferred_element_type=jnp.float32)
            state_ref[:, cols] = state_ref[:, cols] * end_ref[0, :, cols] + added


def output_kernel(per_group, groups, x_ref, xr_ref, xt_ref, b_ref, br_ref, bt_ref, c_ref, cr_ref,
                  ct_ref, z_ref, lw_ref, cum_ref, row_ref, end_ref, enter_ref, skip_ref, scale_ref,
                  out_ref, xbuf, bbuf, cbuf, state, ybuf):
    first = pl.program_id(0) == 0
    x = conv_block(xbuf, first, x_ref, xr_ref, xt_ref)
    b = conv_block(bbuf, first, b_ref, br_ref, bt_ref)
    c = conv_block(cbuf, first, c_ref, cr_ref, ct_ref)

    @pl.when(first)
    def _():
        state[...] = enter_ref[...]

    lw = lw_ref[...]
    cum = cum_ref[...]
    low = lax.broadcasted_iota(jnp.int32, (SPAN, 2 * HEAD), 1) < HEAD
    causal = lax.broadcasted_iota(jnp.int32, (SPAN, SPAN), 0) >= lax.broadcasted_iota(
        jnp.int32, (SPAN, SPAN), 1
    )
    group_cols = per_group * HEAD
    for g in range(groups):
        bg = b[:, g * STATE : (g + 1) * STATE]
        bt = bg.T.astype(jnp.bfloat16)
        cg = c[:, g * STATE : (g + 1) * STATE].astype(jnp.bfloat16)
        scores = jnp.dot(cg, bt, preferred_element_type=jnp.float32)
        squares = jnp.zeros((SPAN, 2 * HEAD), jnp.float32)
        for pair in range(per_group // 2):
            h = g * per_group + 2 * pair
            cols = slice(h * HEAD, (h + 2) * HEAD)
            xp = x[:, cols]
            cum_0, cum_1 = spread(cum, h, SPAN), spread(cum, h + 1, SPAN)
            m_0 = scores * jnp.exp(jnp.where(causal, cum_0 + row_ref[0, h : h + 1, :], -jnp.inf))
            m_1 = scores * jnp.exp(jnp.where(causal, cum_1 + row_ref[0, h + 1 : h + 2, :], -jnp.inf))
            mixing = jnp.concatenate([m_0.astype(jnp.bfloat16), m_1.astype(jnp.bfloat16)], axis=1)
            x_0 = jnp.where(low, xp, 0.0).astype(jnp.bfloat16)
            x_1 = jnp.where(low, 0.0, xp).astype(jnp.bfloat16)
            y = jnp.dot(
                mixing, jnp.concatenate([x_0, x_1], axis=0), preferred_element_type=jnp.float32
            )
            before = state[:, cols]
            carried = jnp.dot(cg, before.astype(jnp.bfloat16), preferred_element_type=jnp.float32)
            y = y + carried * jnp.exp(jnp.where(low, cum_0, cum_1)) + xp * skip_ref[:, cols]
            factor = jnp.exp(jnp.where(low, spread(lw, h, 2 * HEAD), spread(lw, h + 1, 2 * HEAD)))
            xw = (xp * factor).astype(jnp.bfloat16)
            added = jnp.dot(bt, xw, preferred_element_type=jnp.float32)
            state[:, cols] = before * end_ref[0, :, cols] + added
            gate = z_ref[:, cols].astype(jnp.float32)
            gated = y * (gate * jax.nn.sigmoid(gate))
            squares = squares + gated * gated
            ybuf[:, cols] = gated
        mean = jnp.sum(squares, axis=1, keepdims=True) / group_cols
        inverse = lax.rsqrt(mean + norm_eps)
        cols = slice(g * group_cols, (g + 1) * group_cols)
        out_ref[:, cols] = (ybuf[:, cols] * inverse * scale_ref[:, cols]).astype(jnp.bfloat16)


def entering_state(own_state, own_decay):
    size, mine = (lax.axis_size("ep"), lax.axis_index("ep"))
    rows = own_state.shape[0]
    total = own_state
    decay = own_decay

    def joined():
        return jnp.concatenate(
            [total, jnp.broadcast_to(decay, (RIM, decay.shape[1]))], axis=0
        ).astype(jnp.bfloat16)

    distance = 1
    while distance < size:
        came = passed_along(joined(), "ep", distance)
        there = mine >= distance
        earlier = came[:rows].astype(jnp.float32)
        earlier_decay = jnp.where(there, came[rows : rows + 1].astype(jnp.float32), 1.0)
        total = earlier * decay + total
        decay = earlier_decay * decay
        distance *= 2
    return passed_along(total.astype(jnp.bfloat16), "ep", 1).astype(jnp.float32)


def mixer_half(
    sequence_entry_features,
    sequence_exit_gating,
    memory_insert_clusters,
    memory_query_clusters,
    interval_presoftplus,
    entry_filter_taps,
    insert_filter_taps,
    query_filter_taps,
    interval_offset,
    head_fading_exponent,
    skip_connection_factor,
    spike_fading_exponent,
    cluster_scaling_vector,
    sequence_exit_projection,
):
    tok_rows = sequence_entry_features.shape[0]
    local_heads = interval_offset.shape[0]
    local_groups = memory_insert_clusters.shape[1] // STATE
    per_group = local_heads // local_groups
    inner_cols = sequence_entry_features.shape[1]
    state_cols = memory_insert_clusters.shape[1]
    last_rows = jnp.concatenate(
        [
            sequence_entry_features[tok_rows - RIM :],
            memory_insert_clusters[tok_rows - RIM :],
            memory_query_clusters[tok_rows - RIM :],
        ],
        axis=1,
    )
    rims = passed_along(last_rows, "ep", 1)
    rim_x = rims[:, :inner_cols]
    rim_b = rims[:, inner_cols : inner_cols + state_cols]
    rim_c = rims[:, inner_cols + state_cols :]
    blocks = tok_rows // SPAN
    interval = jax.nn.softplus(interval_presoftplus.astype(jnp.float32) + interval_offset)
    fading = spike_fading_exponent - jnp.exp(head_fading_exponent) * interval
    lower = jnp.tril(jnp.ones((SPAN, SPAN), jnp.float32))
    cumulative = jnp.einsum(
        "ts,csh->cth", lower, fading.reshape(blocks, SPAN, local_heads), precision=highest
    )
    log_step = jnp.log(interval).reshape(blocks, SPAN, local_heads)
    block_end = cumulative[:, -1:]
    key_log = (log_step - cumulative + block_end).reshape(tok_rows, local_heads)
    row_log = jnp.swapaxes(log_step - cumulative, 1, 2)
    end_factor = jnp.repeat(jnp.exp(block_end), HEAD, axis=2)
    own_decay = jnp.repeat(jnp.exp(jnp.sum(block_end, axis=0)), HEAD, axis=1)
    cumulative = cumulative.reshape(tok_rows, local_heads)

    def rows_of(width):
        return pl.BlockSpec((SPAN, width), lambda i: (i, 0))

    def fixed(shape):
        return pl.BlockSpec(shape, lambda i: (0, 0))

    def block_of(rows, width):
        return pl.BlockSpec((1, rows, width), lambda i: (i, 0, 0))

    def cost(dots):
        return pl.CostEstimate(
            flops=dots * tok_rows * inner_cols * STATE * 8,
            bytes_accessed=dots * tok_rows * inner_cols * 8,
            transcendentals=0,
        )

    taps = entry_filter_taps.shape[0]
    x_specs = [rows_of(inner_cols), fixed((RIM, inner_cols)), fixed((taps, inner_cols))]
    s_specs = [rows_of(state_cols), fixed((RIM, state_cols)), fixed((taps, state_cols))]
    x_args = (sequence_entry_features, rim_x, entry_filter_taps)
    b_args = (memory_insert_clusters, rim_b, insert_filter_taps)
    c_args = (memory_query_clusters, rim_c, query_filter_taps)
    own_state = pl.pallas_call(
        functools.partial(state_kernel, per_group, local_groups),
        grid=(blocks,),
        in_specs=x_specs + s_specs + [rows_of(local_heads), block_of(1, inner_cols)],
        out_specs=fixed((STATE, inner_cols)),
        out_shape=jax.ShapeDtypeStruct((STATE, inner_cols), jnp.float32),
        scratch_shapes=[
            pltpu.VMEM((SPAN + RIM, inner_cols), jnp.float32),
            pltpu.VMEM((SPAN + RIM, state_cols), jnp.float32),
        ],
        cost_estimate=cost(1),
        name="own_state",
    )(*x_args, *b_args, key_log, end_factor)
    entering = entering_state(own_state, own_decay)
    normed = pl.pallas_call(
        functools.partial(output_kernel, per_group, local_groups),
        grid=(blocks,),
        in_specs=x_specs + s_specs + s_specs + [
            rows_of(inner_cols),
            rows_of(local_heads),
            rows_of(local_heads),
            block_of(local_heads, SPAN),
            block_of(1, inner_cols),
            fixed((STATE, inner_cols)),
            fixed((1, inner_cols)),
            fixed((1, inner_cols)),
        ],
        out_specs=rows_of(inner_cols),
        out_shape=jax.ShapeDtypeStruct((tok_rows, inner_cols), jnp.bfloat16),
        scratch_shapes=[
            pltpu.VMEM((SPAN + RIM, inner_cols), jnp.float32),
            pltpu.VMEM((SPAN + RIM, state_cols), jnp.float32),
            pltpu.VMEM((SPAN + RIM, state_cols), jnp.float32),
            pltpu.VMEM((STATE, inner_cols), jnp.float32),
            pltpu.VMEM((SPAN, inner_cols), jnp.float32),
        ],
        cost_estimate=cost(3),
        name="mixer_output",
    )(
        *x_args, *b_args, *c_args, sequence_exit_gating, key_log, cumulative, row_log, end_factor,
        entering, jnp.repeat(skip_connection_factor, HEAD)[None], cluster_scaling_vector[None],
    )
    return jnp.dot(normed, sequence_exit_projection, preferred_element_type=jnp.float32).astype(
        jnp.bfloat16
    )


def experts_half(
    specialist_sample_slice,
    specialist_scaling_vector,
    chosen_specialists,
    dispatcher_affinity_matrix,
    gating_projection,
    expand_projection,
    shrink_projection,
):
    tok_rows = specialist_sample_slice.shape[0]
    feature_count = specialist_sample_slice.shape[1]
    top_count = chosen_specialists.shape[1]
    experts = lax.axis_size("ep")
    groups_tp = lax.axis_size("tp")
    capacity = tok_rows * top_count * 5 // (4 * experts)
    as_float = specialist_sample_slice.astype(jnp.float32)
    centred = as_float - jnp.mean(as_float, axis=1, keepdims=True)
    normed = (
        centred
        * lax.rsqrt(jnp.mean(centred * centred, axis=1, keepdims=True) + norm_eps)
        * specialist_scaling_vector
    ).astype(jnp.bfloat16)
    route_weight = jnp.exp(dispatcher_affinity_matrix) / jnp.sum(
        jnp.exp(dispatcher_affinity_matrix), axis=1, keepdims=True
    )
    flat_routes = chosen_specialists.reshape(-1)
    onehot = (flat_routes[:, None] == jnp.arange(experts, dtype=jnp.int32)[None, :]).astype(
        jnp.int32
    )
    position = jnp.sum(onehot * (jnp.cumsum(onehot, axis=0) - 1), axis=1)
    target = flat_routes * capacity + position
    token_ids = jnp.arange(tok_rows * top_count, dtype=jnp.int32) // top_count
    source_table = jnp.full((experts * capacity,), tok_rows, jnp.int32).at[target].set(token_ids)
    padded = jnp.concatenate([normed, jnp.zeros((1, feature_count), jnp.bfloat16)], axis=0)
    outgoing = padded[source_table].reshape(experts, capacity, feature_count)
    arrived = lax.all_to_all(outgoing, "ep", split_axis=0, concat_axis=0, tiled=True)
    shard_rows = lax.all_gather(arrived, "tp", axis=0, tiled=True)
    rows_in = shard_rows.reshape(-1, feature_count)
    gate_h = jnp.dot(rows_in, gating_projection[0], preferred_element_type=jnp.float32)
    up_h = jnp.dot(rows_in, expand_projection[0], preferred_element_type=jnp.float32)
    clipped = jnp.minimum(gate_h, clamp_top)
    hidden_act = (
        (
            clipped
            * jax.nn.sigmoid(sigmoid_sharp * clipped)
            * (jnp.clip(up_h, -clamp_top, clamp_top) + 1.0)
        )
        .astype(jnp.bfloat16)
        .reshape(shard_rows.shape[0], capacity, -1)
    )
    hidden_act = hidden_act.reshape(groups_tp * experts * capacity, -1)
    summed = lax.psum_scatter(
        jnp.dot(hidden_act, shrink_projection[0], preferred_element_type=jnp.float32).astype(
            jnp.bfloat16
        ),
        "tp",
        scatter_dimension=0,
        tiled=True,
    )
    returned = lax.all_to_all(
        summed.reshape(experts, capacity, feature_count),
        "ep",
        split_axis=0,
        concat_axis=0,
        tiled=True,
    )
    slot_out = returned.reshape(experts * capacity, feature_count)[target].reshape(
        tok_rows, top_count, feature_count
    )
    combined = jnp.einsum("tk,tkd->td", route_weight, slot_out.astype(jnp.float32))
    return combined.astype(jnp.bfloat16)


def routing_kernel(experts, x_ref, scale_ref, chosen_ref, score_ref, out_ref):
    features = x_ref.shape[1]
    rows, top_count = chosen_ref.shape
    value = x_ref[...].astype(jnp.float32)
    centred = value - jnp.mean(value, axis=1, keepdims=True)
    spread_of = jnp.mean(centred * centred, axis=1, keepdims=True)
    normed = centred * lax.rsqrt(spread_of + norm_eps) * scale_ref[...]
    out_ref[:, :features] = normed.astype(jnp.bfloat16)
    raised = jnp.exp(score_ref[...])
    weight = raised / jnp.sum(raised, axis=1, keepdims=True)
    lane = lax.broadcasted_iota(jnp.int32, (rows, LANES), 1)
    named = lax.rem(lane, experts)
    chosen = chosen_ref[...]
    held = jnp.zeros((rows, LANES), jnp.float32)
    share = jnp.zeros((rows, LANES), jnp.float32)
    for k in range(top_count):
        same = chosen[:, k : k + 1] == named
        held = held + jnp.where(same, 1.0, 0.0)
        share = share + jnp.where(same, weight[:, k : k + 1], 0.0)
    earlier = lax.broadcasted_iota(jnp.int32, (rows, rows), 0) > lax.broadcasted_iota(
        jnp.int32, (rows, rows), 1
    )
    place = jnp.dot(
        jnp.where(earlier, 1.0, 0.0).astype(jnp.bfloat16),
        held.astype(jnp.bfloat16),
        preferred_element_type=jnp.float32,
    )
    place = jnp.where(held > 0.0, place, 255.0)
    coarse = share.astype(jnp.bfloat16).astype(jnp.float32)
    table = jnp.where(lane < experts, place, jnp.where(lane < 2 * experts, coarse, share - coarse))
    out_ref[:, features:] = table.astype(jnp.bfloat16)


def experts_kernel(
    experts, capacity, tokens_ref, mix_ref, gate_ref, up_ref, down_ref, out_ref, mixed_ref,
    tokens, slots, own, outgoing, incoming, place, place_next, from_x, from_y,
    to_y, came_y, to_x, came_x, keep_a, keep_b, to_z, from_z,
    mix_own, mix_core, mix_out, mix_in, mix_sem, mc_send, mc_recv, mx_send, mx_recv,
    token_sem, core_send, core_recv, x_send, x_recv, y_send, y_recv,
    a_send, a_recv, b_send, b_recv, z_send, z_recv,
):
    depth = experts // 2
    steps = experts
    ep, tp = lax.axis_index("ep"), lax.axis_index("tp")
    z, y, x, core = ep // 2, ep % 2, tp // 2, tp % 2
    next_ep = z * 2 + 1 - y
    sibling = {"tp": x * 2 + 1 - core}
    x_next = {"tp": (1 - x) * 2 + core}
    y_next = {"ep": next_ep}
    rows = out_ref.shape[0]
    features = out_ref.shape[1]
    half = features // 2
    mesh_id = pl.DeviceIdType.MESH

    def z_next(k):
        return {"ep": ((z + k) % depth) * 2 + y}

    def fetch(s):
        k, dy = (s // 2 + 1) % depth, 1 - s % 2
        block = ((z + k) % depth) * 2 + (y + dy) % 2
        span = 4 * rows
        return pltpu.make_async_copy(
            tokens_ref.at[pl.ds(pl.multiple_of(block * span, span), span)],
            tokens.at[s % 2],
            token_sem.at[s % 2],
        )

    def remote(source, target, send, recv, device):
        return pltpu.make_async_remote_copy(
            src_ref=source, dst_ref=target, send_sem=send, recv_sem=recv,
            device_id=device, device_id_type=mesh_id,
        )

    def core_copy(s):
        return remote(outgoing.at[s], incoming.at[s], core_send.at[s], core_recv.at[s], sibling)

    def x_copy(s):
        return remote(own.at[s, 0, 1], from_x.at[s], x_send.at[s], x_recv.at[s], x_next)

    def y_copy(i):
        return remote(own.at[2 * i, 1], from_y.at[i], y_send.at[i], y_recv.at[i], y_next)

    def a_copy(i):
        return remote(to_y.at[i], came_y.at[i], a_send.at[i], a_recv.at[i], y_next)

    def b_copy(i):
        return remote(to_x.at[i], came_x.at[i], b_send.at[i], b_recv.at[i], x_next)

    def z_copy(i):
        return remote(to_z.at[i], from_z.at[i], z_send.at[i], z_recv.at[i], z_next(i + 1))

    chunks, piece = mixed_ref.shape[0] // MIX_ROWS, MIX_ROWS
    share = mixed_ref.shape[0]

    def mix_rows(dx, c):
        block = ((x + dx) % 2) * 2 + c
        return mix_ref.at[pl.ds(pl.multiple_of(block * share, share), share)]

    def mix_fetch(dx):
        return pltpu.make_async_copy(mix_rows(dx, core), mix_own.at[dx], mix_sem.at[dx])

    def mix_core_copy(dx):
        return remote(
            mix_rows(dx, 1 - core), mix_core.at[dx], mc_send.at[dx], mc_recv.at[dx], sibling
        )

    def mix_x_copy(j):
        rows_j = pl.ds(pl.multiple_of(j * piece, piece), piece)
        return remote(
            mix_out.at[rows_j], mix_in.at[rows_j], mx_send.at[j], mx_recv.at[j], x_next
        )

    def mix_piece(j, carry):
        rows_j = pl.ds(pl.multiple_of(j * piece, piece), piece)
        mix_out[rows_j, :] = (
            mix_own[1, rows_j, :].astype(jnp.float32) + mix_core[1, rows_j, :].astype(jnp.float32)
        ).astype(jnp.bfloat16)
        mix_own[0, rows_j, :] = (
            mix_own[0, rows_j, :].astype(jnp.float32) + mix_core[0, rows_j, :].astype(jnp.float32)
        ).astype(jnp.bfloat16)
        return carry

    def mix_send(j, carry):
        mix_x_copy(j).start()
        return carry

    def mix_finish(j, carry):
        rows_j = pl.ds(pl.multiple_of(j * piece, piece), piece)
        mix_x_copy(j).wait_recv()
        mixed_ref[rows_j, :] = (
            mix_own[0, rows_j, :].astype(jnp.float32) + mix_in[rows_j, :].astype(jnp.float32)
        ).astype(jnp.bfloat16)
        return carry

    def mix_sent(j, carry):
        mix_x_copy(j).wait_send()
        return carry

    fetch(0).start()
    for dx in (1, 0):
        mix_fetch(dx).start()
    barrier = pltpu.get_barrier_semaphore()
    partners = [sibling, x_next, y_next] + [z_next(k) for k in range(1, depth)]
    for partner in partners:
        pl.semaphore_signal(barrier, inc=1, device_id=partner, device_id_type=mesh_id)
    pl.semaphore_wait(barrier, len(partners))

    for dx in (1, 0):
        mix_core_copy(dx).start()

    lane = lax.broadcasted_iota(jnp.int32, (rows, LANES), 1)
    lane_value = lane.astype(jnp.float32)
    slot_lane = lax.broadcasted_iota(jnp.int32, (capacity, LANES), 1)

    def chosen_slots(table, expert):
        column = jnp.sum(jnp.where(lane == expert, table, 0.0), axis=1, keepdims=True)
        return jnp.where(column == lane_value, 1.0, 0.0)

    def compute(s):
        weights = []
        for dx in (0, 1):
            for q in (0, 1):
                c = core if q == 0 else 1 - core
                block = ((x + dx) % 2) * 2 + c
                start = pl.multiple_of(block * rows, rows)
                arrived = tokens[s % 2, pl.ds(start, rows), :]
                table = arrived[:, features:].astype(jnp.float32)
                picked = chosen_slots(table, ep)
                if q == 0:
                    place[s, dx] = picked.astype(jnp.bfloat16)
                    place_next[s, dx] = chosen_slots(table, next_ep).astype(jnp.bfloat16)
                select = picked.T[:capacity].astype(jnp.bfloat16)
                taken = jnp.dot(select, arrived, preferred_element_type=jnp.float32)
                first = (dx * 2 + q) * capacity
                slots[first : first + capacity, :] = taken[:, :features].astype(jnp.bfloat16)
                mine = (slot_lane == experts + ep) | (slot_lane == 2 * experts + ep)
                weights.append(
                    jnp.sum(jnp.where(mine, taken[:, features:], 0.0), axis=1, keepdims=True)
                )
        value = slots[...]
        gate_h = jnp.dot(value, gate_ref[...], preferred_element_type=jnp.float32)
        up_h = jnp.dot(value, up_ref[...], preferred_element_type=jnp.float32)
        clipped = jnp.minimum(gate_h, clamp_top)
        act = (
            clipped
            * jax.nn.sigmoid(sigmoid_sharp * clipped)
            * (jnp.clip(up_h, -clamp_top, clamp_top) + 1.0)
        ).astype(jnp.bfloat16)
        for side in (0, 1):
            columns = slice(side * half, (side + 1) * half)
            part = jnp.dot(act, down_ref[:, columns], preferred_element_type=jnp.float32)
            for dx in (0, 1):
                for q in (0, 1):
                    first = (dx * 2 + q) * capacity
                    scaled = (part[first : first + capacity] * weights[dx * 2 + q]).astype(
                        jnp.bfloat16
                    )
                    if q == 0:
                        own[s, side, dx] = scaled
                    else:
                        outgoing[s, side, dx] = scaled

    def spread_out(where, value):
        return jnp.dot(where[:, :capacity], value, preferred_element_type=jnp.float32)

    last_x = 2 * depth + 2

    def step(s, carry):
        @pl.when(s < steps)
        def _():
            @pl.when(s + 1 < steps)
            def _():
                fetch(s + 1).start()

            fetch(s).wait()
            compute(s)

        @pl.when((s >= 1) & (s <= steps))
        def _():
            t = s - 1
            core_copy(t).wait_recv()
            for side in (0, 1):
                for dx in (0, 1):
                    own[t, side, dx] = (
                        own[t, side, dx].astype(jnp.float32)
                        + incoming[t, side, dx].astype(jnp.float32)
                    ).astype(jnp.bfloat16)

        @pl.when(s < steps)
        def _():
            core_copy(s).start()

        @pl.when(s == 0)
        def _():
            for dx in (1, 0):
                mix_fetch(dx).wait()
                mix_core_copy(dx).wait_recv()
            lax.fori_loop(0, chunks, mix_piece, 0)

        i = (s - 4) // 2

        @pl.when((s >= 4) & (s % 2 == 0) & (i < depth))
        def _():
            far, near = 2 * i, 2 * i + 1
            x_copy(far).wait_recv()
            where = place[far, 0]
            to_y[i] = (spread_out(where, own[far, 0, 0]) + spread_out(where, from_x[far])).astype(
                jnp.bfloat16
            )
            y_copy(i).wait_recv()
            to_x[i] = (
                spread_out(place[near, 1], own[near, 1, 1])
                + spread_out(place_next[near, 1], from_y[i, 1])
            ).astype(jnp.bfloat16)
            x_copy(near).wait_recv()
            where = place[near, 0]
            keep_a[i] = spread_out(where, own[near, 0, 0]) + spread_out(where, from_x[near])
            keep_b[i] = spread_out(where, own[near, 1, 0]) + spread_out(
                place_next[near, 0], from_y[i, 0]
            )
            a_copy(i).start()
            b_copy(i).start()

        @pl.when((s >= 1) & (s <= steps))
        def _():
            t = s - 1
            x_copy(t).start()

            @pl.when(t % 2 == 0)
            def _():
                y_copy(t // 2).start()

        early, late = chunks // 4, chunks // 2
        begin = jnp.where(s == 0, 0, jnp.where(s < last_x, early + s - 3, late))
        end = jnp.where(s == 0, early, jnp.where(s < last_x, early + s - 2, chunks))
        lax.fori_loop(
            jnp.where((s == 0) | (s == last_x), begin, jnp.clip(begin, early, late)),
            jnp.where((s == 0) | (s == last_x), end,
                      jnp.where(s > last_x, 0, jnp.clip(end, early, late))),
            mix_send, 0,
        )

        j = (s - 6) // 2

        @pl.when((s >= 6) & (s % 2 == 0) & (j < depth))
        def _():
            a_copy(j).wait_recv()
            b_copy(j).wait_recv()
            sum_a = keep_a[j] + came_y[j].astype(jnp.float32)
            sum_b = keep_b[j] + came_x[j].astype(jnp.float32)

            @pl.when(j < depth - 1)
            def _():
                to_z[j, :, :half] = sum_a.astype(jnp.bfloat16)
                to_z[j, :, half:] = sum_b.astype(jnp.bfloat16)
                z_copy(j).start()

            @pl.when(j == depth - 1)
            def _():
                keep_a[j] = sum_a
                keep_b[j] = sum_b

        return carry

    lax.fori_loop(0, 2 * depth + 5, step, 0)
    for i in range(depth - 1):
        z_copy(i).wait_recv()
    for side, keep in ((0, keep_a), (1, keep_b)):
        columns = slice(side * half, (side + 1) * half)
        total = keep[depth - 1]
        for i in range(depth - 1):
            total = total + from_z[i, :, columns].astype(jnp.float32)
        out_ref[:, columns] = total.astype(jnp.bfloat16)
    lax.fori_loop(0, chunks, mix_finish, 0)
    lax.fori_loop(0, chunks, mix_sent, 0)
    for dx in (0, 1):
        mix_core_copy(dx).wait_send()
    for s in range(steps):
        core_copy(s).wait_send()
        x_copy(s).wait_send()
    for i in range(depth):
        y_copy(i).wait_send()
        a_copy(i).wait_send()
        b_copy(i).wait_send()
    for i in range(depth - 1):
        z_copy(i).wait_send()


def dense_experts_fit(tok_rows, top_count, capacity, mix_rows):
    experts = lax.axis_size("ep")
    fits = experts % 2 == 0 and experts >= 4 and 3 * experts <= LANES and lax.axis_size("tp") == 4
    return fits and 2 * top_count >= experts and mix_rows % (4 * MIX_ROWS) == 0 and tok_rows == LANES and capacity % 16 == 0


def gathered_tokens(
    specialist_sample_slice, specialist_scaling_vector, chosen_specialists, dispatcher_affinity_matrix
):
    rows, features = specialist_sample_slice.shape
    marked = pl.pallas_call(
        functools.partial(routing_kernel, lax.axis_size("ep")),
        out_shape=jax.ShapeDtypeStruct((rows, features + LANES), jnp.bfloat16),
        name="routing",
    )(
        specialist_sample_slice, specialist_scaling_vector[None], chosen_specialists,
        dispatcher_affinity_matrix,
    )
    return lax.all_gather(marked, ("ep", "tp"), axis=0, tiled=True)


def experts_dense(
    tokens, mix_part, rows, capacity, gating_projection, expand_projection, shrink_projection
):
    experts = lax.axis_size("ep")
    features = gating_projection.shape[1]
    half, depth, steps = features // 2, experts // 2, experts
    hidden = gating_projection.shape[2]
    narrow = jnp.bfloat16
    dma = pltpu.SemaphoreType.DMA
    share = mix_part.shape[0] // 4
    pieces = share // MIX_ROWS
    work = 2 * experts * 4 * capacity * features * hidden * 3
    return pl.pallas_call(
        functools.partial(experts_kernel, experts, capacity),
        in_specs=[pl.BlockSpec(memory_space=pl.ANY)] * 2
        + [pl.BlockSpec(memory_space=pltpu.VMEM)] * 3,
        out_specs=[pl.BlockSpec(memory_space=pltpu.VMEM)] * 2,
        out_shape=[
            jax.ShapeDtypeStruct((rows, features), narrow),
            jax.ShapeDtypeStruct((share, features), narrow),
        ],
        scratch_shapes=[
            pltpu.VMEM((2, 4 * rows, features + LANES), narrow),
            pltpu.VMEM((4 * capacity, features), narrow),
            pltpu.VMEM((steps, 2, 2, capacity, half), narrow),
            pltpu.VMEM((steps, 2, 2, capacity, half), narrow),
            pltpu.VMEM((steps, 2, 2, capacity, half), narrow),
            pltpu.VMEM((steps, 2, rows, LANES), narrow),
            pltpu.VMEM((steps, 2, rows, LANES), narrow),
            pltpu.VMEM((steps, capacity, half), narrow),
            pltpu.VMEM((depth, 2, capacity, half), narrow),
            pltpu.VMEM((depth, rows, half), narrow),
            pltpu.VMEM((depth, rows, half), narrow),
            pltpu.VMEM((depth, rows, half), narrow),
            pltpu.VMEM((depth, rows, half), narrow),
            pltpu.VMEM((depth, rows, half), jnp.float32),
            pltpu.VMEM((depth, rows, half), jnp.float32),
            pltpu.VMEM((depth - 1, rows, features), narrow),
            pltpu.VMEM((depth - 1, rows, features), narrow),
            pltpu.VMEM((2, share, features), narrow),
            pltpu.VMEM((2, share, features), narrow),
            pltpu.VMEM((share, features), narrow),
            pltpu.VMEM((share, features), narrow),
            dma((2,)), dma((2,)), dma((2,)), dma((pieces,)), dma((pieces,)),
            dma((2,)), dma((steps,)), dma((steps,)), dma((steps,)), dma((steps,)),
            dma((depth,)), dma((depth,)), dma((depth,)), dma((depth,)), dma((depth,)),
            dma((depth,)), dma((depth - 1,)), dma((depth - 1,)),
        ],
        compiler_params=pltpu.CompilerParams(
            collective_id=0, has_side_effects=True, vmem_limit_bytes=63 * 1024 * 1024
        ),
        cost_estimate=pl.CostEstimate(
            flops=8 * work, bytes_accessed=4 * tokens.size, transcendentals=0
        ),
        name="experts",
    )(tokens, mix_part, gating_projection[0], expand_projection[0], shrink_projection[0])


def body(
    sequence_entry_features,
    sequence_exit_gating,
    memory_insert_clusters,
    memory_query_clusters,
    interval_presoftplus,
    entry_filter_taps,
    insert_filter_taps,
    query_filter_taps,
    interval_offset,
    head_fading_exponent,
    skip_connection_factor,
    spike_fading_exponent,
    cluster_scaling_vector,
    sequence_exit_projection,
    specialist_sample_slice,
    specialist_scaling_vector,
    chosen_specialists,
    dispatcher_affinity_matrix,
    gating_projection,
    expand_projection,
    shrink_projection,
):
    tok_rows, top_count = chosen_specialists.shape
    capacity = tok_rows * top_count * 5 // (4 * lax.axis_size("ep"))
    dense = dense_experts_fit(tok_rows, top_count, capacity, sequence_entry_features.shape[0])
    if dense:
        tokens = gathered_tokens(
            specialist_sample_slice,
            specialist_scaling_vector,
            chosen_specialists,
            dispatcher_affinity_matrix,
        )
    mix_part = mixer_half(
        sequence_entry_features,
        sequence_exit_gating,
        memory_insert_clusters,
        memory_query_clusters,
        interval_presoftplus,
        entry_filter_taps,
        insert_filter_taps,
        query_filter_taps,
        interval_offset,
        head_fading_exponent,
        skip_connection_factor,
        spike_fading_exponent,
        cluster_scaling_vector,
        sequence_exit_projection,
    )
    if dense:
        moe_out, mixed = experts_dense(
            tokens, mix_part, tok_rows, capacity, gating_projection, expand_projection, shrink_projection
        )
        return (mixed, moe_out)
    mixed = lax.psum_scatter(mix_part, "tp", scatter_dimension=0, tiled=True)
    moe_out = experts_half(
        specialist_sample_slice,
        specialist_scaling_vector,
        chosen_specialists,
        dispatcher_affinity_matrix,
        gating_projection,
        expand_projection,
        shrink_projection,
    )
    return (mixed, moe_out)


def solution(mesh):
    in_specs = (
        P("ep", "tp"),
        P("ep", "tp"),
        P("ep", "tp"),
        P("ep", "tp"),
        P("ep", "tp"),
        P(None, "tp"),
        P(None, "tp"),
        P(None, "tp"),
        P("tp"),
        P("tp"),
        P("tp"),
        P("ep", "tp"),
        P("tp"),
        P("tp", None),
        P(("ep", "tp"), None),
        P(),
        P(("ep", "tp"), None),
        P(("ep", "tp"), None),
        P("ep", None, "tp"),
        P("ep", None, "tp"),
        P("ep", "tp", None),
    )
    out_specs = (P(("ep", "tp"), None), P(("ep", "tp"), None))
    return jax.shard_map(body, mesh=mesh, in_specs=in_specs, out_specs=out_specs, check_vma=False)
```

```python
import functools
import jax
import jax.numpy as jnp
from jax import lax
from jax.experimental import pallas as pl
from jax.experimental.pallas import tpu as pltpu
from jax.sharding import PartitionSpec as P

HEAD = 64
STATE = 128
SPAN = 128
RIM = 8
LANES = 128
MIX_ROWS = 32

norm_eps = 1e-05
clamp_top = 7.0
sigmoid_sharp = 1.702
highest = lax.Precision.HIGHEST


def passed_along(block, axis, distance):
    devices = range(lax.axis_size(axis))
    route = [(i - distance, i) for i in devices if i - distance in devices]
    return lax.ppermute(block, axis, route)


def conv_block(buf, first, value_ref, rim_ref, taps_ref):
    @pl.when(first)
    def _():
        buf[0:RIM, :] = rim_ref[...].astype(jnp.float32)

    @pl.when(jnp.logical_not(first))
    def _():
        buf[0:RIM, :] = buf[SPAN : SPAN + RIM, :]

    buf[RIM : RIM + SPAN, :] = value_ref[...].astype(jnp.float32)
    taps = taps_ref[...].astype(jnp.float32)
    count = taps.shape[0]
    total = buf[RIM : RIM + SPAN, :] * taps[count - 1 : count]
    for j in range(count - 1):
        start = RIM - (count - 1) + j
        total = total + buf[start : start + SPAN, :] * taps[j : j + 1]
    return total * jax.nn.sigmoid(total)


def spread(cols, h, width):
    return jnp.broadcast_to(cols[:, h : h + 1], (SPAN, width))


def state_kernel(per_group, groups, x_ref, xr_ref, xt_ref, b_ref, br_ref, bt_ref, lw_ref, end_ref,
                 state_ref, xbuf, bbuf):
    first = pl.program_id(0) == 0
    x = conv_block(xbuf, first, x_ref, xr_ref, xt_ref)
    b = conv_block(bbuf, first, b_ref, br_ref, bt_ref)

    @pl.when(first)
    def _():
        state_ref[...] = jnp.zeros_like(state_ref)

    lw = lw_ref[...]
    low = lax.broadcasted_iota(jnp.int32, (SPAN, 2 * HEAD), 1) < HEAD
    for g in range(groups):
        bt = b[:, g * STATE : (g + 1) * STATE].T.astype(jnp.bfloat16)
        for pair in range(per_group // 2):
            h = g * per_group + 2 * pair
            cols = slice(h * HEAD, (h + 2) * HEAD)
            factor = jnp.exp(jnp.where(low, spread(lw, h, 2 * HEAD), spread(lw, h + 1, 2 * HEAD)))
            xw = (x[:, cols] * factor).astype(jnp.bfloat16)
            added = jnp.dot(bt, xw, preferred_element_type=jnp.float32)
            state_ref[:, cols] = state_ref[:, cols] * end_ref[0, :, cols] + added


def output_kernel(per_group, groups, x_ref, xr_ref, xt_ref, b_ref, br_ref, bt_ref, c_ref, cr_ref,
                  ct_ref, z_ref, lw_ref, cum_ref, row_ref, end_ref, enter_ref, skip_ref, scale_ref,
                  out_ref, xbuf, bbuf, cbuf, state, ybuf):
    first = pl.program_id(0) == 0
    x = conv_block(xbuf, first, x_ref, xr_ref, xt_ref)
    b = conv_block(bbuf, first, b_ref, br_ref, bt_ref)
    c = conv_block(cbuf, first, c_ref, cr_ref, ct_ref)

    @pl.when(first)
    def _():
        state[...] = enter_ref[...]

    lw = lw_ref[...]
    cum = cum_ref[...]
    low = lax.broadcasted_iota(jnp.int32, (SPAN, 2 * HEAD), 1) < HEAD
    causal = lax.broadcasted_iota(jnp.int32, (SPAN, SPAN), 0) >= lax.broadcasted_iota(
        jnp.int32, (SPAN, SPAN), 1
    )
    group_cols = per_group * HEAD
    for g in range(groups):
        bg = b[:, g * STATE : (g + 1) * STATE]
        bt = bg.T.astype(jnp.bfloat16)
        cg = c[:, g * STATE : (g + 1) * STATE].astype(jnp.bfloat16)
        scores = jnp.dot(cg, bt, preferred_element_type=jnp.float32)
        squares = jnp.zeros((SPAN, 2 * HEAD), jnp.float32)
        for pair in range(per_group // 2):
            h = g * per_group + 2 * pair
            cols = slice(h * HEAD, (h + 2) * HEAD)
            xp = x[:, cols]
            cum_0, cum_1 = spread(cum, h, SPAN), spread(cum, h + 1, SPAN)
            m_0 = scores * jnp.exp(jnp.where(causal, cum_0 + row_ref[0, h : h + 1, :], -jnp.inf))
            m_1 = scores * jnp.exp(jnp.where(causal, cum_1 + row_ref[0, h + 1 : h + 2, :], -jnp.inf))
            mixing = jnp.concatenate([m_0.astype(jnp.bfloat16), m_1.astype(jnp.bfloat16)], axis=1)
            x_0 = jnp.where(low, xp, 0.0).astype(jnp.bfloat16)
            x_1 = jnp.where(low, 0.0, xp).astype(jnp.bfloat16)
            y = jnp.dot(
                mixing, jnp.concatenate([x_0, x_1], axis=0), preferred_element_type=jnp.float32
            )
            before = state[:, cols]
            carried = jnp.dot(cg, before.astype(jnp.bfloat16), preferred_element_type=jnp.float32)
            y = y + carried * jnp.exp(jnp.where(low, cum_0, cum_1)) + xp * skip_ref[:, cols]
            factor = jnp.exp(jnp.where(low, spread(lw, h, 2 * HEAD), spread(lw, h + 1, 2 * HEAD)))
            xw = (xp * factor).astype(jnp.bfloat16)
            added = jnp.dot(bt, xw, preferred_element_type=jnp.float32)
            state[:, cols] = before * end_ref[0, :, cols] + added
            gate = z_ref[:, cols].astype(jnp.float32)
            gated = y * (gate * jax.nn.sigmoid(gate))
            squares = squares + gated * gated
            ybuf[:, cols] = gated
        mean = jnp.sum(squares, axis=1, keepdims=True) / group_cols
        inverse = lax.rsqrt(mean + norm_eps)
        cols = slice(g * group_cols, (g + 1) * group_cols)
        out_ref[:, cols] = (ybuf[:, cols] * inverse * scale_ref[:, cols]).astype(jnp.bfloat16)


def entering_state(own_state, own_decay):
    size, mine = (lax.axis_size("ep"), lax.axis_index("ep"))
    rows = own_state.shape[0]
    total = own_state
    decay = own_decay

    def joined():
        return jnp.concatenate(
            [total, jnp.broadcast_to(decay, (RIM, decay.shape[1]))], axis=0
        ).astype(jnp.bfloat16)

    distance = 1
    while distance < size:
        came = passed_along(joined(), "ep", distance)
        there = mine >= distance
        earlier = came[:rows].astype(jnp.float32)
        earlier_decay = jnp.where(there, came[rows : rows + 1].astype(jnp.float32), 1.0)
        total = earlier * decay + total
        decay = earlier_decay * decay
        distance *= 2
    return passed_along(total.astype(jnp.bfloat16), "ep", 1).astype(jnp.float32)


def mixer_half(
    sequence_entry_features,
    sequence_exit_gating,
    memory_insert_clusters,
    memory_query_clusters,
    interval_presoftplus,
    entry_filter_taps,
    insert_filter_taps,
    query_filter_taps,
    interval_offset,
    head_fading_exponent,
    skip_connection_factor,
    spike_fading_exponent,
    cluster_scaling_vector,
    sequence_exit_projection,
    marked,
):
    tok_rows = sequence_entry_features.shape[0]
    local_heads = interval_offset.shape[0]
    local_groups = memory_insert_clusters.shape[1] // STATE
    per_group = local_heads // local_groups
    inner_cols = sequence_entry_features.shape[1]
    state_cols = memory_insert_clusters.shape[1]
    last_rows = jnp.concatenate(
        [
            sequence_entry_features[tok_rows - RIM :],
            memory_insert_clusters[tok_rows - RIM :],
            memory_query_clusters[tok_rows - RIM :],
        ],
        axis=1,
    )
    rims = passed_along(last_rows, "ep", 1)
    rim_x = rims[:, :inner_cols]
    rim_b = rims[:, inner_cols : inner_cols + state_cols]
    rim_c = rims[:, inner_cols + state_cols :]
    blocks = tok_rows // SPAN
    interval = jax.nn.softplus(interval_presoftplus.astype(jnp.float32) + interval_offset)
    fading = spike_fading_exponent - jnp.exp(head_fading_exponent) * interval
    lower = jnp.tril(jnp.ones((SPAN, SPAN), jnp.float32))
    cumulative = jnp.einsum(
        "ts,csh->cth", lower, fading.reshape(blocks, SPAN, local_heads), precision=highest
    )
    log_step = jnp.log(interval).reshape(blocks, SPAN, local_heads)
    block_end = cumulative[:, -1:]
    key_log = (log_step - cumulative + block_end).reshape(tok_rows, local_heads)
    row_log = jnp.swapaxes(log_step - cumulative, 1, 2)
    end_factor = jnp.repeat(jnp.exp(block_end), HEAD, axis=2)
    own_decay = jnp.repeat(jnp.exp(jnp.sum(block_end, axis=0)), HEAD, axis=1)
    cumulative = cumulative.reshape(tok_rows, local_heads)

    def rows_of(width):
        return pl.BlockSpec((SPAN, width), lambda i: (i, 0))

    def fixed(shape):
        return pl.BlockSpec(shape, lambda i: (0, 0))

    def block_of(rows, width):
        return pl.BlockSpec((1, rows, width), lambda i: (i, 0, 0))

    def cost(dots):
        return pl.CostEstimate(
            flops=dots * tok_rows * inner_cols * STATE * 8,
            bytes_accessed=dots * tok_rows * inner_cols * 8,
            transcendentals=0,
        )

    taps = entry_filter_taps.shape[0]
    x_specs = [rows_of(inner_cols), fixed((RIM, inner_cols)), fixed((taps, inner_cols))]
    s_specs = [rows_of(state_cols), fixed((RIM, state_cols)), fixed((taps, state_cols))]
    x_args = (sequence_entry_features, rim_x, entry_filter_taps)
    b_args = (memory_insert_clusters, rim_b, insert_filter_taps)
    c_args = (memory_query_clusters, rim_c, query_filter_taps)
    if marked is not None:
        return mixer_gather(
            per_group, local_groups, blocks, x_args, b_args, c_args, sequence_exit_gating, key_log,
            cumulative, row_log, end_factor, own_decay,
            jnp.repeat(skip_connection_factor, HEAD)[None], cluster_scaling_vector[None],
            sequence_exit_projection, marked,
        )
    own_state = pl.pallas_call(
        functools.partial(state_kernel, per_group, local_groups),
        grid=(blocks,),
        in_specs=x_specs + s_specs + [rows_of(local_heads), block_of(1, inner_cols)],
        out_specs=fixed((STATE, inner_cols)),
        out_shape=jax.ShapeDtypeStruct((STATE, inner_cols), jnp.float32),
        scratch_shapes=[
            pltpu.VMEM((SPAN + RIM, inner_cols), jnp.float32),
            pltpu.VMEM((SPAN + RIM, state_cols), jnp.float32),
        ],
        cost_estimate=cost(1),
        name="own_state",
    )(*x_args, *b_args, key_log, end_factor)
    entering = entering_state(own_state, own_decay)
    normed = pl.pallas_call(
        functools.partial(output_kernel, per_group, local_groups),
        grid=(blocks,),
        in_specs=x_specs + s_specs + s_specs + [
            rows_of(inner_cols),
            rows_of(local_heads),
            rows_of(local_heads),
            block_of(local_heads, SPAN),
            block_of(1, inner_cols),
            fixed((STATE, inner_cols)),
            fixed((1, inner_cols)),
            fixed((1, inner_cols)),
        ],
        out_specs=rows_of(inner_cols),
        out_shape=jax.ShapeDtypeStruct((tok_rows, inner_cols), jnp.bfloat16),
        scratch_shapes=[
            pltpu.VMEM((SPAN + RIM, inner_cols), jnp.float32),
            pltpu.VMEM((SPAN + RIM, state_cols), jnp.float32),
            pltpu.VMEM((SPAN + RIM, state_cols), jnp.float32),
            pltpu.VMEM((STATE, inner_cols), jnp.float32),
            pltpu.VMEM((SPAN, inner_cols), jnp.float32),
        ],
        cost_estimate=cost(3),
        name="mixer_output",
    )(
        *x_args, *b_args, *c_args, sequence_exit_gating, key_log, cumulative, row_log, end_factor,
        entering, jnp.repeat(skip_connection_factor, HEAD)[None], cluster_scaling_vector[None],
    )
    return jnp.dot(normed, sequence_exit_projection, preferred_element_type=jnp.float32).astype(
        jnp.bfloat16
    )


def mixer_gather(
    per_group, groups, blocks, x_args, b_args, c_args, gating, key_log, cumulative, row_log,
    end_factor, own_decay, skip, scale, exit_projection, marked,
):
    tok_rows, inner_cols = gating.shape
    state_cols = b_args[0].shape[1]
    heads = key_log.shape[1]
    features = exit_projection.shape[1]
    rows, marked_cols = marked.shape
    taps = x_args[2].shape[0]
    devices = lax.axis_size("ep") * lax.axis_size("tp")
    depth = lax.axis_size("ep") // 2
    narrow, wide = jnp.bfloat16, inner_cols // 2
    pieces = 7 * depth

    def either(i):
        return jnp.where(i < blocks, i, jnp.maximum(i - blocks - 1, 0))

    def late(i):
        return jnp.maximum(i - blocks - 1, 0)

    def by_rows(width, at):
        return pl.BlockSpec((SPAN, width), lambda i: (at(i), 0))

    def by_block(count, width, at):
        return pl.BlockSpec((1, count, width), lambda i: (at(i), 0, 0))

    def fixed(shape):
        return pl.BlockSpec(shape, lambda i: (0, 0))

    def conv_specs(width, at):
        return [by_rows(width, at), fixed((RIM, width)), fixed((taps, width))]

    dma = pltpu.SemaphoreType.DMA
    hops = [dma((depth,)) for _ in range(12)]
    return pl.pallas_call(
        functools.partial(mixer_gather_kernel, per_group, groups, blocks, depth),
        grid=(2 * blocks + 1,),
        in_specs=conv_specs(inner_cols, either)
        + conv_specs(state_cols, either)
        + conv_specs(state_cols, late)
        + [
            by_rows(inner_cols, late),
            by_rows(heads, either),
            by_rows(heads, late),
            by_block(heads, SPAN, late),
            by_block(1, inner_cols, either),
            fixed((1, inner_cols)),
            fixed((1, inner_cols)),
            fixed((1, inner_cols)),
            fixed((inner_cols, features)),
            fixed((rows, marked_cols)),
        ],
        out_specs=[by_rows(features, late), pl.BlockSpec(memory_space=pl.ANY)],
        out_shape=[
            jax.ShapeDtypeStruct((tok_rows, features), narrow),
            jax.ShapeDtypeStruct((devices * rows, marked_cols), narrow),
        ],
        scratch_shapes=[
            pltpu.VMEM((SPAN + RIM, inner_cols), jnp.float32),
            pltpu.VMEM((SPAN + RIM, state_cols), jnp.float32),
            pltpu.VMEM((SPAN + RIM, state_cols), jnp.float32),
            pltpu.VMEM((STATE, inner_cols), jnp.float32),
            pltpu.VMEM((SPAN, inner_cols), jnp.float32),
            pltpu.VMEM((SPAN, inner_cols), narrow),
            pltpu.VMEM((STATE + 2 * RIM, inner_cols), narrow),
            pltpu.VMEM((STATE + 2 * RIM, inner_cols), narrow),
            pltpu.VMEM((STATE + 2 * RIM, wide), narrow),
            pltpu.VMEM((depth - 1, STATE + 2 * RIM, wide), narrow),
            pltpu.VMEM((STATE, wide), jnp.float32),
            pltpu.VMEM((STATE, wide), narrow),
            pltpu.VMEM((STATE, wide), narrow),
            dma((1,)), dma((depth - 1,)), dma((depth - 1,)),
            *hops,
            dma((pieces,)), dma((pieces,)), dma((1,)), dma((1,)), dma((depth - 1,)),
            dma((depth - 1,)), dma((1,)), dma((1,)),
        ],
        compiler_params=pltpu.CompilerParams(
            collective_id=1, has_side_effects=True, vmem_limit_bytes=56 * 1024 * 1024,
            dimension_semantics=("arbitrary",),
        ),
        cost_estimate=pl.CostEstimate(
            flops=tok_rows * inner_cols * (features * 2 + STATE * 16),
            bytes_accessed=tok_rows * inner_cols * 16,
            transcendentals=0,
        ),
        name="mixer_gather",
    )(
        *x_args, *b_args, *c_args, gating, key_log, cumulative, row_log, end_factor, own_decay,
        skip, scale, exit_projection, marked,
    )


def experts_half(
    specialist_sample_slice,
    specialist_scaling_vector,
    chosen_specialists,
    dispatcher_affinity_matrix,
    gating_projection,
    expand_projection,
    shrink_projection,
):
    tok_rows = specialist_sample_slice.shape[0]
    feature_count = specialist_sample_slice.shape[1]
    top_count = chosen_specialists.shape[1]
    experts = lax.axis_size("ep")
    groups_tp = lax.axis_size("tp")
    capacity = tok_rows * top_count * 5 // (4 * experts)
    as_float = specialist_sample_slice.astype(jnp.float32)
    centred = as_float - jnp.mean(as_float, axis=1, keepdims=True)
    normed = (
        centred
        * lax.rsqrt(jnp.mean(centred * centred, axis=1, keepdims=True) + norm_eps)
        * specialist_scaling_vector
    ).astype(jnp.bfloat16)
    route_weight = jnp.exp(dispatcher_affinity_matrix) / jnp.sum(
        jnp.exp(dispatcher_affinity_matrix), axis=1, keepdims=True
    )
    flat_routes = chosen_specialists.reshape(-1)
    onehot = (flat_routes[:, None] == jnp.arange(experts, dtype=jnp.int32)[None, :]).astype(
        jnp.int32
    )
    position = jnp.sum(onehot * (jnp.cumsum(onehot, axis=0) - 1), axis=1)
    target = flat_routes * capacity + position
    token_ids = jnp.arange(tok_rows * top_count, dtype=jnp.int32) // top_count
    source_table = jnp.full((experts * capacity,), tok_rows, jnp.int32).at[target].set(token_ids)
    padded = jnp.concatenate([normed, jnp.zeros((1, feature_count), jnp.bfloat16)], axis=0)
    outgoing = padded[source_table].reshape(experts, capacity, feature_count)
    arrived = lax.all_to_all(outgoing, "ep", split_axis=0, concat_axis=0, tiled=True)
    shard_rows = lax.all_gather(arrived, "tp", axis=0, tiled=True)
    rows_in = shard_rows.reshape(-1, feature_count)
    gate_h = jnp.dot(rows_in, gating_projection[0], preferred_element_type=jnp.float32)
    up_h = jnp.dot(rows_in, expand_projection[0], preferred_element_type=jnp.float32)
    clipped = jnp.minimum(gate_h, clamp_top)
    hidden_act = (
        (
            clipped
            * jax.nn.sigmoid(sigmoid_sharp * clipped)
            * (jnp.clip(up_h, -clamp_top, clamp_top) + 1.0)
        )
        .astype(jnp.bfloat16)
        .reshape(shard_rows.shape[0], capacity, -1)
    )
    hidden_act = hidden_act.reshape(groups_tp * experts * capacity, -1)
    summed = lax.psum_scatter(
        jnp.dot(hidden_act, shrink_projection[0], preferred_element_type=jnp.float32).astype(
            jnp.bfloat16
        ),
        "tp",
        scatter_dimension=0,
        tiled=True,
    )
    returned = lax.all_to_all(
        summed.reshape(experts, capacity, feature_count),
        "ep",
        split_axis=0,
        concat_axis=0,
        tiled=True,
    )
    slot_out = returned.reshape(experts * capacity, feature_count)[target].reshape(
        tok_rows, top_count, feature_count
    )
    combined = jnp.einsum("tk,tkd->td", route_weight, slot_out.astype(jnp.float32))
    return combined.astype(jnp.bfloat16)


def routing_kernel(experts, x_ref, scale_ref, chosen_ref, score_ref, out_ref):
    features = x_ref.shape[1]
    rows, top_count = chosen_ref.shape
    value = x_ref[...].astype(jnp.float32)
    centred = value - jnp.mean(value, axis=1, keepdims=True)
    spread_of = jnp.mean(centred * centred, axis=1, keepdims=True)
    normed = centred * lax.rsqrt(spread_of + norm_eps) * scale_ref[...]
    out_ref[:, :features] = normed.astype(jnp.bfloat16)
    raised = jnp.exp(score_ref[...])
    weight = raised / jnp.sum(raised, axis=1, keepdims=True)
    lane = lax.broadcasted_iota(jnp.int32, (rows, LANES), 1)
    named = lax.rem(lane, experts)
    chosen = chosen_ref[...]
    held = jnp.zeros((rows, LANES), jnp.float32)
    share = jnp.zeros((rows, LANES), jnp.float32)
    for k in range(top_count):
        same = chosen[:, k : k + 1] == named
        held = held + jnp.where(same, 1.0, 0.0)
        share = share + jnp.where(same, weight[:, k : k + 1], 0.0)
    earlier = lax.broadcasted_iota(jnp.int32, (rows, rows), 0) > lax.broadcasted_iota(
        jnp.int32, (rows, rows), 1
    )
    place = jnp.dot(
        jnp.where(earlier, 1.0, 0.0).astype(jnp.bfloat16),
        held.astype(jnp.bfloat16),
        preferred_element_type=jnp.float32,
    )
    place = jnp.where(held > 0.0, place, 255.0)
    coarse = share.astype(jnp.bfloat16).astype(jnp.float32)
    table = jnp.where(lane < experts, place, jnp.where(lane < 2 * experts, coarse, share - coarse))
    out_ref[:, features:] = table.astype(jnp.bfloat16)


def experts_kernel(
    experts, capacity, tokens_ref, mix_ref, gate_ref, up_ref, down_ref, out_ref, mixed_ref,
    tokens, slots, own, outgoing, incoming, place, place_next, from_x, from_y,
    to_y, came_y, to_x, came_x, keep_a, keep_b, to_z, from_z,
    mix_own, mix_core, mix_out, mix_in, mix_sem, mc_send, mc_recv, mx_send, mx_recv,
    token_sem, core_send, core_recv, x_send, x_recv, y_send, y_recv,
    a_send, a_recv, b_send, b_recv, z_send, z_recv,
):
    depth = experts // 2
    steps = experts
    ep, tp = lax.axis_index("ep"), lax.axis_index("tp")
    z, y, x, core = ep // 2, ep % 2, tp // 2, tp % 2
    next_ep = z * 2 + 1 - y
    sibling = {"tp": x * 2 + 1 - core}
    x_next = {"tp": (1 - x) * 2 + core}
    y_next = {"ep": next_ep}
    rows = out_ref.shape[0]
    features = out_ref.shape[1]
    half = features // 2
    mesh_id = pl.DeviceIdType.MESH

    def z_next(k):
        return {"ep": ((z + k) % depth) * 2 + y}

    def fetch(s):
        k, dy = (s // 2 + 1) % depth, 1 - s % 2
        block = ((z + k) % depth) * 2 + (y + dy) % 2
        span = 4 * rows
        return pltpu.make_async_copy(
            tokens_ref.at[pl.ds(pl.multiple_of(block * span, span), span)],
            tokens.at[s % 2],
            token_sem.at[s % 2],
        )

    def remote(source, target, send, recv, device):
        return pltpu.make_async_remote_copy(
            src_ref=source, dst_ref=target, send_sem=send, recv_sem=recv,
            device_id=device, device_id_type=mesh_id,
        )

    def core_copy(s):
        return remote(outgoing.at[s], incoming.at[s], core_send.at[s], core_recv.at[s], sibling)

    def x_copy(s):
        return remote(own.at[s, 0, 1], from_x.at[s], x_send.at[s], x_recv.at[s], x_next)

    def y_copy(i):
        return remote(own.at[2 * i, 1], from_y.at[i], y_send.at[i], y_recv.at[i], y_next)

    def a_copy(i):
        return remote(to_y.at[i], came_y.at[i], a_send.at[i], a_recv.at[i], y_next)

    def b_copy(i):
        return remote(to_x.at[i], came_x.at[i], b_send.at[i], b_recv.at[i], x_next)

    def z_copy(i):
        return remote(to_z.at[i], from_z.at[i], z_send.at[i], z_recv.at[i], z_next(i + 1))

    chunks, piece = mixed_ref.shape[0] // MIX_ROWS, MIX_ROWS
    share = mixed_ref.shape[0]

    def mix_rows(dx, c):
        block = ((x + dx) % 2) * 2 + c
        return mix_ref.at[pl.ds(pl.multiple_of(block * share, share), share)]

    def mix_fetch(dx):
        return pltpu.make_async_copy(mix_rows(dx, core), mix_own.at[dx], mix_sem.at[dx])

    def mix_core_copy(dx):
        return remote(
            mix_rows(dx, 1 - core), mix_core.at[dx], mc_send.at[dx], mc_recv.at[dx], sibling
        )

    def mix_x_copy(j):
        rows_j = pl.ds(pl.multiple_of(j * piece, piece), piece)
        return remote(
            mix_out.at[rows_j], mix_in.at[rows_j], mx_send.at[j], mx_recv.at[j], x_next
        )

    def mix_piece(j, carry):
        rows_j = pl.ds(pl.multiple_of(j * piece, piece), piece)
        mix_out[rows_j, :] = (
            mix_own[1, rows_j, :].astype(jnp.float32) + mix_core[1, rows_j, :].astype(jnp.float32)
        ).astype(jnp.bfloat16)
        mix_own[0, rows_j, :] = (
            mix_own[0, rows_j, :].astype(jnp.float32) + mix_core[0, rows_j, :].astype(jnp.float32)
        ).astype(jnp.bfloat16)
        return carry

    def mix_send(j, carry):
        mix_x_copy(j).start()
        return carry

    def mix_finish(j, carry):
        rows_j = pl.ds(pl.multiple_of(j * piece, piece), piece)
        mix_x_copy(j).wait_recv()
        mixed_ref[rows_j, :] = (
            mix_own[0, rows_j, :].astype(jnp.float32) + mix_in[rows_j, :].astype(jnp.float32)
        ).astype(jnp.bfloat16)
        return carry

    def mix_sent(j, carry):
        mix_x_copy(j).wait_send()
        return carry

    fetch(0).start()
    for dx in (1, 0):
        mix_fetch(dx).start()
    barrier = pltpu.get_barrier_semaphore()
    partners = [sibling, x_next, y_next] + [z_next(k) for k in range(1, depth)]
    for partner in partners:
        pl.semaphore_signal(barrier, inc=1, device_id=partner, device_id_type=mesh_id)
    pl.semaphore_wait(barrier, len(partners))

    for dx in (1, 0):
        mix_core_copy(dx).start()

    lane = lax.broadcasted_iota(jnp.int32, (rows, LANES), 1)
    lane_value = lane.astype(jnp.float32)
    slot_lane = lax.broadcasted_iota(jnp.int32, (capacity, LANES), 1)

    def chosen_slots(table, expert):
        column = jnp.sum(jnp.where(lane == expert, table, 0.0), axis=1, keepdims=True)
        return jnp.where(column == lane_value, 1.0, 0.0)

    def compute(s):
        weights = []
        for dx in (0, 1):
            for q in (0, 1):
                c = core if q == 0 else 1 - core
                block = ((x + dx) % 2) * 2 + c
                start = pl.multiple_of(block * rows, rows)
                arrived = tokens[s % 2, pl.ds(start, rows), :]
                table = arrived[:, features:].astype(jnp.float32)
                picked = chosen_slots(table, ep)
                if q == 0:
                    place[s, dx] = picked.astype(jnp.bfloat16)
                    place_next[s, dx] = chosen_slots(table, next_ep).astype(jnp.bfloat16)
                select = picked.T[:capacity].astype(jnp.bfloat16)
                taken = jnp.dot(select, arrived, preferred_element_type=jnp.float32)
                first = (dx * 2 + q) * capacity
                slots[first : first + capacity, :] = taken[:, :features].astype(jnp.bfloat16)
                mine = (slot_lane == experts + ep) | (slot_lane == 2 * experts + ep)
                weights.append(
                    jnp.sum(jnp.where(mine, taken[:, features:], 0.0), axis=1, keepdims=True)
                )
        value = slots[...]
        gate_h = jnp.dot(value, gate_ref[...], preferred_element_type=jnp.float32)
        up_h = jnp.dot(value, up_ref[...], preferred_element_type=jnp.float32)
        clipped = jnp.minimum(gate_h, clamp_top)
        act = (
            clipped
            * jax.nn.sigmoid(sigmoid_sharp * clipped)
            * (jnp.clip(up_h, -clamp_top, clamp_top) + 1.0)
        ).astype(jnp.bfloat16)
        for side in (0, 1):
            columns = slice(side * half, (side + 1) * half)
            part = jnp.dot(act, down_ref[:, columns], preferred_element_type=jnp.float32)
            for dx in (0, 1):
                for q in (0, 1):
                    first = (dx * 2 + q) * capacity
                    scaled = (part[first : first + capacity] * weights[dx * 2 + q]).astype(
                        jnp.bfloat16
                    )
                    if q == 0:
                        own[s, side, dx] = scaled
                    else:
                        outgoing[s, side, dx] = scaled

    def spread_out(where, value):
        return jnp.dot(where[:, :capacity], value, preferred_element_type=jnp.float32)

    last_x = 2 * depth + 2

    def step(s, carry):
        @pl.when(s < steps)
        def _():
            @pl.when(s + 1 < steps)
            def _():
                fetch(s + 1).start()

            fetch(s).wait()
            compute(s)

        @pl.when((s >= 1) & (s <= steps))
        def _():
            t = s - 1
            core_copy(t).wait_recv()
            for side in (0, 1):
                for dx in (0, 1):
                    own[t, side, dx] = (
                        own[t, side, dx].astype(jnp.float32)
                        + incoming[t, side, dx].astype(jnp.float32)
                    ).astype(jnp.bfloat16)

        @pl.when(s < steps)
        def _():
            core_copy(s).start()

        @pl.when(s == 0)
        def _():
            for dx in (1, 0):
                mix_fetch(dx).wait()
                mix_core_copy(dx).wait_recv()
            lax.fori_loop(0, chunks, mix_piece, 0)

        i = (s - 4) // 2

        @pl.when((s >= 4) & (s % 2 == 0) & (i < depth))
        def _():
            far, near = 2 * i, 2 * i + 1
            x_copy(far).wait_recv()
            where = place[far, 0]
            to_y[i] = (spread_out(where, own[far, 0, 0]) + spread_out(where, from_x[far])).astype(
                jnp.bfloat16
            )
            y_copy(i).wait_recv()
            to_x[i] = (
                spread_out(place[near, 1], own[near, 1, 1])
                + spread_out(place_next[near, 1], from_y[i, 1])
            ).astype(jnp.bfloat16)
            x_copy(near).wait_recv()
            where = place[near, 0]
            keep_a[i] = spread_out(where, own[near, 0, 0]) + spread_out(where, from_x[near])
            keep_b[i] = spread_out(where, own[near, 1, 0]) + spread_out(
                place_next[near, 0], from_y[i, 0]
            )
            a_copy(i).start()
            b_copy(i).start()

        @pl.when((s >= 1) & (s <= steps))
        def _():
            t = s - 1
            x_copy(t).start()

            @pl.when(t % 2 == 0)
            def _():
                y_copy(t // 2).start()

        early, late = chunks // 4, chunks // 2
        begin = jnp.where(s == 0, 0, jnp.where(s < last_x, early + s - 3, late))
        end = jnp.where(s == 0, early, jnp.where(s < last_x, early + s - 2, chunks))
        lax.fori_loop(
            jnp.where((s == 0) | (s == last_x), begin, jnp.clip(begin, early, late)),
            jnp.where((s == 0) | (s == last_x), end,
                      jnp.where(s > last_x, 0, jnp.clip(end, early, late))),
            mix_send, 0,
        )

        j = (s - 6) // 2

        @pl.when((s >= 6) & (s % 2 == 0) & (j < depth))
        def _():
            a_copy(j).wait_recv()
            b_copy(j).wait_recv()
            sum_a = keep_a[j] + came_y[j].astype(jnp.float32)
            sum_b = keep_b[j] + came_x[j].astype(jnp.float32)

            @pl.when(j < depth - 1)
            def _():
                to_z[j, :, :half] = sum_a.astype(jnp.bfloat16)
                to_z[j, :, half:] = sum_b.astype(jnp.bfloat16)
                z_copy(j).start()

            @pl.when(j == depth - 1)
            def _():
                keep_a[j] = sum_a
                keep_b[j] = sum_b

        return carry

    lax.fori_loop(0, 2 * depth + 5, step, 0)
    for i in range(depth - 1):
        z_copy(i).wait_recv()
    for side, keep in ((0, keep_a), (1, keep_b)):
        columns = slice(side * half, (side + 1) * half)
        total = keep[depth - 1]
        for i in range(depth - 1):
            total = total + from_z[i, :, columns].astype(jnp.float32)
        out_ref[:, columns] = total.astype(jnp.bfloat16)
    lax.fori_loop(0, chunks, mix_finish, 0)
    lax.fori_loop(0, chunks, mix_sent, 0)
    for dx in (0, 1):
        mix_core_copy(dx).wait_send()
    for s in range(steps):
        core_copy(s).wait_send()
        x_copy(s).wait_send()
    for i in range(depth):
        y_copy(i).wait_send()
        a_copy(i).wait_send()
        b_copy(i).wait_send()
    for i in range(depth - 1):
        z_copy(i).wait_send()


def mixer_gather_kernel(
    per_group, groups, blocks, depth,
    x_ref, xr_ref, xt_ref, b_ref, br_ref, bt_ref, c_ref, cr_ref, ct_ref, z_ref, lw_ref, cum_ref,
    row_ref, end_ref, decay_ref, skip_ref, scale_ref, exit_ref, marked_ref,
    part_ref, tokens_ref,
    xbuf, bbuf, cbuf, state, ybuf, nbuf, pair_out, pair_in, line_out, line_in, line_sum, swap_out,
    swap_in, local_sem, z_send, z_recv, xa_s, xa_r, xb_s, xb_r, xf_s, xf_r, ya_s, ya_r, yb_s, yb_r,
    yf_s, yf_r, d_s, d_r, pair_s, pair_r, line_s, line_r, swap_s, swap_r,
):
    step = pl.program_id(0)
    ep, tp = lax.axis_index("ep"), lax.axis_index("tp")
    z, y, x, core = ep // 2, ep % 2, tp // 2, tp % 2
    sibling = {"tp": x * 2 + 1 - core}
    x_next = {"tp": (1 - x) * 2 + core}
    y_next = {"ep": z * 2 + 1 - y}
    mesh_id = pl.DeviceIdType.MESH
    rows = marked_ref.shape[0]
    part_rows = rows // 2
    inner = state.shape[1]
    wide = inner // 2

    def z_next(k):
        return {"ep": ((z + k) % depth) * 2 + y}

    def remote(source, target, send, recv, device):
        return pltpu.make_async_remote_copy(
            src_ref=source, dst_ref=target, send_sem=send, recv_sem=recv,
            device_id=device, device_id_type=mesh_id,
        )

    def region(dx, dy, k, half, c=core):
        block = (((z + depth - k) % depth) * 2 + (y + dy) % 2) * 4 + ((x + dx) % 2) * 2 + c
        size = rows if half is None else part_rows
        start = block * rows + (0 if half is None else half * part_rows)
        return tokens_ref.at[pl.ds(pl.multiple_of(start, part_rows), size)]

    def source(dx, dy, k, half):
        if (dx, dy, k) == (0, 0, 0):
            if half is None:
                return marked_ref
            return marked_ref.at[pl.ds(half * part_rows, part_rows)]
        return region(dx, dy, k, half)

    def z_copy(k):
        return remote(
            marked_ref, region(0, 0, 0, None), z_send.at[k - 1], z_recv.at[k - 1], z_next(k)
        )

    def z_came(k):
        here = region(0, 0, k, None)
        return remote(here, here, z_send.at[k - 1], z_recv.at[k - 1], z_next(k))

    moves = {
        "xa": ((0, 0, 0), (1, 0, 0), xa_s, xa_r, x_next),
        "xb": ((0, 0, 1), (1, 0, 1), xb_s, xb_r, x_next),
        "xf": ((0, 1, 1), (1, 1, 1), xf_s, xf_r, x_next),
        "yb": ((0, 0, 1), (0, 1, 1), yb_s, yb_r, y_next),
        "ya": ((0, 0, 0), (0, 1, 0), ya_s, ya_r, y_next),
        "yf": ((1, 0, 0), (1, 1, 0), yf_s, yf_r, y_next),
    }

    def sent(name, k):
        (dx, dy, half), _, send, recv, device = moves[name]
        return remote(
            source(dx, dy, k, half), region(dx, dy, k, half), send.at[k], recv.at[k], device
        )

    def came(name, k):
        _, (dx, dy, half), send, recv, device = moves[name]
        here = region(dx, dy, k, half)
        return remote(here, here, send.at[k], recv.at[k], device)

    shared = [(0, 0, None), (1, 0, 0), (1, 0, 1), (0, 1, 1), (0, 1, 0), (1, 1, 0), (1, 1, 1)]

    def d_sent(k, n):
        dx, dy, half = shared[n]
        m = len(shared) * k + n
        return remote(
            source(dx, dy, k, half), region(dx, dy, k, half), d_s.at[m], d_r.at[m], sibling
        )

    def d_came(k, n):
        dx, dy, half = shared[n]
        m = len(shared) * k + n
        here = region(dx, dy, k, half, 1 - core)
        return remote(here, here, d_s.at[m], d_r.at[m], sibling)

    def first_hop(k):
        if k > 0:
            z_came(k).wait_recv()
        for name in ("xa", "yb", "xb", "ya"):
            sent(name, k).start()
        d_sent(k, 0).start()

    def second_hop(k):
        came("xa", k).wait_recv()
        sent("yf", k).start()
        d_sent(k, 1).start()
        came("yb", k).wait_recv()
        sent("xf", k).start()
        d_sent(k, 3).start()

    def last_hop(k, parts=(("xb", 2), ("ya", 4), ("yf", 5), ("xf", 6))):
        for name, n in parts:
            came(name, k).wait_recv()
            d_sent(k, n).start()

    def own_copy():
        return pltpu.make_async_copy(marked_ref, region(0, 0, 0, None), local_sem.at[0])

    @pl.when(step == 0)
    def _():
        barrier = pltpu.get_barrier_semaphore()
        partners = [sibling, x_next, y_next] + [z_next(k) for k in range(1, depth)]
        for partner in partners:
            pl.semaphore_signal(barrier, inc=1, device_id=partner, device_id_type=mesh_id)
        pl.semaphore_wait(barrier, len(partners))
        z_copy(1).start()
        first_hop(0)
        for k in range(2, depth - 1):
            z_copy(k).start()
        own_copy().start()

    low = lax.broadcasted_iota(jnp.int32, (SPAN, 2 * HEAD), 1) < HEAD
    state_pass = step < blocks
    output_pass = step > blocks

    @pl.when(state_pass)
    def _():
        first = step == 0
        xv = conv_block(xbuf, first, x_ref, xr_ref, xt_ref)
        bv = conv_block(bbuf, first, b_ref, br_ref, bt_ref)

        @pl.when(first)
        def _():
            state[...] = jnp.zeros_like(state)

        lw = lw_ref[...]
        for g in range(groups):
            bt = bv[:, g * STATE : (g + 1) * STATE].T.astype(jnp.bfloat16)
            for pair in range(per_group // 2):
                h = g * per_group + 2 * pair
                cols = slice(h * HEAD, (h + 2) * HEAD)
                factor = jnp.exp(
                    jnp.where(low, spread(lw, h, 2 * HEAD), spread(lw, h + 1, 2 * HEAD))
                )
                xw = (xv[:, cols] * factor).astype(jnp.bfloat16)
                added = jnp.dot(bt, xw, preferred_element_type=jnp.float32)
                state[:, cols] = state[:, cols] * end_ref[0, :, cols] + added

    @pl.when(step == blocks // 2)
    def _():
        second_hop(0)

    @pl.when(step == blocks)
    def _():
        pair = remote(pair_out, pair_in, pair_s.at[0], pair_r.at[0], y_next)
        swap = remote(swap_out, swap_in, swap_s.at[0], swap_r.at[0], y_next)

        def line(k):
            return remote(
                line_out, line_in.at[k - 1], line_s.at[k - 1], line_r.at[k - 1], z_next(k)
            )

        decay = decay_ref[...]
        pair_out[:STATE, :] = state[...].astype(jnp.bfloat16)
        pair_out[STATE:, :] = jnp.broadcast_to(decay, (2 * RIM, inner)).astype(jnp.bfloat16)
        last_hop(0, (("xb", 2), ("ya", 4)))
        pair.start()
        first_hop(1)
        last_hop(0, (("yf", 5), ("xf", 6)))
        pair.wait_recv()
        mine = pl.ds(pl.multiple_of(y * wide, wide), wide)
        theirs = pl.ds(pl.multiple_of((1 - y) * wide, wide), wide)
        own_state, own_decay = state[:, mine], decay_ref[:, mine]
        other_state = pair_in[:STATE, mine].astype(jnp.float32)
        other_decay = pair_in[STATE : STATE + 1, mine].astype(jnp.float32)
        later = y == 1
        both = jnp.where(
            later, other_state * own_decay + own_state, own_state * other_decay + other_state
        )
        line_out[:STATE, :] = both.astype(jnp.bfloat16)
        line_out[STATE:, :] = jnp.broadcast_to(own_decay * other_decay, (2 * RIM, wide)).astype(
            jnp.bfloat16
        )
        line_sum[...] = jnp.zeros_like(line_sum)
        for k in range(1, depth):
            @pl.when(z + k < depth)
            def _():
                line(k).start()

        z_copy(depth - 1).start()
        for k in range(depth - 1, 0, -1):
            @pl.when(z >= k)
            def _():
                line(k).wait_recv()
                line_sum[...] = line_sum[...] * line_in[k - 1, STATE : STATE + 1, :].astype(
                    jnp.float32
                ) + line_in[k - 1, :STATE, :].astype(jnp.float32)

        swap_out[...] = line_sum[...].astype(jnp.bfloat16)
        state[:, mine] = line_sum[...]
        second_hop(1)
        swap.start()
        swap.wait_recv()
        state[:, theirs] = swap_in[...].astype(jnp.float32)

        @pl.when(later)
        def _():
            state[...] = state[...] * pair_in[STATE : STATE + 1, :].astype(jnp.float32) + pair_in[
                :STATE, :
            ].astype(jnp.float32)

        pair.wait_send()
        swap.wait_send()
        for k in range(1, depth):
            @pl.when(z + k < depth)
            def _():
                line(k).wait_send()

    @pl.when(output_pass)
    def _():
        first = step == blocks + 1
        xv = conv_block(xbuf, first, x_ref, xr_ref, xt_ref)
        bv = conv_block(bbuf, first, b_ref, br_ref, bt_ref)
        cv = conv_block(cbuf, first, c_ref, cr_ref, ct_ref)
        lw = lw_ref[...]
        cum = cum_ref[...]
        causal = lax.broadcasted_iota(jnp.int32, (SPAN, SPAN), 0) >= lax.broadcasted_iota(
            jnp.int32, (SPAN, SPAN), 1
        )
        group_cols = per_group * HEAD
        for g in range(groups):
            bt = bv[:, g * STATE : (g + 1) * STATE].T.astype(jnp.bfloat16)
            cg = cv[:, g * STATE : (g + 1) * STATE].astype(jnp.bfloat16)
            scores = jnp.dot(cg, bt, preferred_element_type=jnp.float32)
            squares = jnp.zeros((SPAN, 2 * HEAD), jnp.float32)
            for pair in range(per_group // 2):
                h = g * per_group + 2 * pair
                cols = slice(h * HEAD, (h + 2) * HEAD)
                xp = xv[:, cols]
                cum_0, cum_1 = spread(cum, h, SPAN), spread(cum, h + 1, SPAN)
                row_0, row_1 = row_ref[0, h : h + 1, :], row_ref[0, h + 1 : h + 2, :]
                m_0 = scores * jnp.exp(jnp.where(causal, cum_0 + row_0, -jnp.inf))
                m_1 = scores * jnp.exp(jnp.where(causal, cum_1 + row_1, -jnp.inf))
                mixing = jnp.concatenate([m_0.astype(jnp.bfloat16), m_1.astype(jnp.bfloat16)], axis=1)
                x_0 = jnp.where(low, xp, 0.0).astype(jnp.bfloat16)
                x_1 = jnp.where(low, 0.0, xp).astype(jnp.bfloat16)
                value = jnp.dot(
                    mixing, jnp.concatenate([x_0, x_1], axis=0), preferred_element_type=jnp.float32
                )
                before = state[:, cols]
                carried = jnp.dot(cg, before.astype(jnp.bfloat16), preferred_element_type=jnp.float32)
                value = value + carried * jnp.exp(jnp.where(low, cum_0, cum_1)) + xp * skip_ref[:, cols]
                factor = jnp.exp(
                    jnp.where(low, spread(lw, h, 2 * HEAD), spread(lw, h + 1, 2 * HEAD))
                )
                xw = (xp * factor).astype(jnp.bfloat16)
                added = jnp.dot(bt, xw, preferred_element_type=jnp.float32)
                state[:, cols] = before * end_ref[0, :, cols] + added
                gate = z_ref[:, cols].astype(jnp.float32)
                gated = value * (gate * jax.nn.sigmoid(gate))
                squares = squares + gated * gated
                ybuf[:, cols] = gated
            mean = jnp.sum(squares, axis=1, keepdims=True) / group_cols
            inverse = lax.rsqrt(mean + norm_eps)
            cols = slice(g * group_cols, (g + 1) * group_cols)
            nbuf[:, cols] = (ybuf[:, cols] * inverse * scale_ref[:, cols]).astype(jnp.bfloat16)
        part_ref[...] = jnp.dot(
            nbuf[...], exit_ref[...], preferred_element_type=jnp.float32
        ).astype(jnp.bfloat16)

    pace = blocks // (2 * depth - 2)
    for k in range(2, depth):
        at = blocks + 1 + (2 * k - 3) * pace

        @pl.when(step == at)
        def _():
            first_hop(k)

        @pl.when(step == at + pace)
        def _():
            second_hop(k)
            last_hop(k - 1)

    @pl.when(step == 2 * blocks)
    def _():
        last_hop(depth - 1)
        for k in range(depth):
            for n in range(len(shared)):
                d_came(k, n).wait_recv()
        own_copy().wait()
        for k in range(1, depth):
            z_copy(k).wait_send()
        for k in range(depth):
            for name in moves:
                sent(name, k).wait_send()
            for n in range(len(shared)):
                d_sent(k, n).wait_send()


def dense_experts_fit(tok_rows, top_count, capacity, mix_rows):
    experts = lax.axis_size("ep")
    fits = experts % 2 == 0 and experts >= 4 and 3 * experts <= LANES and lax.axis_size("tp") == 4
    return fits and 2 * top_count >= experts and mix_rows % (4 * MIX_ROWS) == 0 and tok_rows == LANES and capacity % 16 == 0


def marked_tokens(
    specialist_sample_slice, specialist_scaling_vector, chosen_specialists, dispatcher_affinity_matrix
):
    rows, features = specialist_sample_slice.shape
    return pl.pallas_call(
        functools.partial(routing_kernel, lax.axis_size("ep")),
        out_shape=jax.ShapeDtypeStruct((rows, features + LANES), jnp.bfloat16),
        name="routing",
    )(
        specialist_sample_slice, specialist_scaling_vector[None], chosen_specialists,
        dispatcher_affinity_matrix,
    )


def experts_dense(
    tokens, mix_part, rows, capacity, gating_projection, expand_projection, shrink_projection
):
    experts = lax.axis_size("ep")
    features = gating_projection.shape[1]
    half, depth, steps = features // 2, experts // 2, experts
    hidden = gating_projection.shape[2]
    narrow = jnp.bfloat16
    dma = pltpu.SemaphoreType.DMA
    share = mix_part.shape[0] // 4
    pieces = share // MIX_ROWS
    work = 2 * experts * 4 * capacity * features * hidden * 3
    return pl.pallas_call(
        functools.partial(experts_kernel, experts, capacity),
        in_specs=[pl.BlockSpec(memory_space=pl.ANY)] * 2
        + [pl.BlockSpec(memory_space=pltpu.VMEM)] * 3,
        out_specs=[pl.BlockSpec(memory_space=pltpu.VMEM)] * 2,
        out_shape=[
            jax.ShapeDtypeStruct((rows, features), narrow),
            jax.ShapeDtypeStruct((share, features), narrow),
        ],
        scratch_shapes=[
            pltpu.VMEM((2, 4 * rows, features + LANES), narrow),
            pltpu.VMEM((4 * capacity, features), narrow),
            pltpu.VMEM((steps, 2, 2, capacity, half), narrow),
            pltpu.VMEM((steps, 2, 2, capacity, half), narrow),
            pltpu.VMEM((steps, 2, 2, capacity, half), narrow),
            pltpu.VMEM((steps, 2, rows, LANES), narrow),
            pltpu.VMEM((steps, 2, rows, LANES), narrow),
            pltpu.VMEM((steps, capacity, half), narrow),
            pltpu.VMEM((depth, 2, capacity, half), narrow),
            pltpu.VMEM((depth, rows, half), narrow),
            pltpu.VMEM((depth, rows, half), narrow),
            pltpu.VMEM((depth, rows, half), narrow),
            pltpu.VMEM((depth, rows, half), narrow),
            pltpu.VMEM((depth, rows, half), jnp.float32),
            pltpu.VMEM((depth, rows, half), jnp.float32),
            pltpu.VMEM((depth - 1, rows, features), narrow),
            pltpu.VMEM((depth - 1, rows, features), narrow),
            pltpu.VMEM((2, share, features), narrow),
            pltpu.VMEM((2, share, features), narrow),
            pltpu.VMEM((share, features), narrow),
            pltpu.VMEM((share, features), narrow),
            dma((2,)), dma((2,)), dma((2,)), dma((pieces,)), dma((pieces,)),
            dma((2,)), dma((steps,)), dma((steps,)), dma((steps,)), dma((steps,)),
            dma((depth,)), dma((depth,)), dma((depth,)), dma((depth,)), dma((depth,)),
            dma((depth,)), dma((depth - 1,)), dma((depth - 1,)),
        ],
        compiler_params=pltpu.CompilerParams(
            collective_id=0, has_side_effects=True, vmem_limit_bytes=63 * 1024 * 1024
        ),
        cost_estimate=pl.CostEstimate(
            flops=8 * work, bytes_accessed=4 * tokens.size, transcendentals=0
        ),
        name="experts",
    )(tokens, mix_part, gating_projection[0], expand_projection[0], shrink_projection[0])


def body(
    sequence_entry_features,
    sequence_exit_gating,
    memory_insert_clusters,
    memory_query_clusters,
    interval_presoftplus,
    entry_filter_taps,
    insert_filter_taps,
    query_filter_taps,
    interval_offset,
    head_fading_exponent,
    skip_connection_factor,
    spike_fading_exponent,
    cluster_scaling_vector,
    sequence_exit_projection,
    specialist_sample_slice,
    specialist_scaling_vector,
    chosen_specialists,
    dispatcher_affinity_matrix,
    gating_projection,
    expand_projection,
    shrink_projection,
):
    tok_rows, top_count = chosen_specialists.shape
    capacity = tok_rows * top_count * 5 // (4 * lax.axis_size("ep"))
    dense = dense_experts_fit(tok_rows, top_count, capacity, sequence_entry_features.shape[0])
    marked = None
    if dense:
        marked = marked_tokens(
            specialist_sample_slice,
            specialist_scaling_vector,
            chosen_specialists,
            dispatcher_affinity_matrix,
        )
    mix_part = mixer_half(
        sequence_entry_features,
        sequence_exit_gating,
        memory_insert_clusters,
        memory_query_clusters,
        interval_presoftplus,
        entry_filter_taps,
        insert_filter_taps,
        query_filter_taps,
        interval_offset,
        head_fading_exponent,
        skip_connection_factor,
        spike_fading_exponent,
        cluster_scaling_vector,
        sequence_exit_projection,
        marked,
    )
    if dense:
        mix_part, tokens = mix_part
        moe_out, mixed = experts_dense(
            tokens, mix_part, tok_rows, capacity, gating_projection, expand_projection, shrink_projection
        )
        return (mixed, moe_out)
    mixed = lax.psum_scatter(mix_part, "tp", scatter_dimension=0, tiled=True)
    moe_out = experts_half(
        specialist_sample_slice,
        specialist_scaling_vector,
        chosen_specialists,
        dispatcher_affinity_matrix,
        gating_projection,
        expand_projection,
        shrink_projection,
    )
    return (mixed, moe_out)


def solution(mesh):
    in_specs = (
        P("ep", "tp"),
        P("ep", "tp"),
        P("ep", "tp"),
        P("ep", "tp"),
        P("ep", "tp"),
        P(None, "tp"),
        P(None, "tp"),
        P(None, "tp"),
        P("tp"),
        P("tp"),
        P("tp"),
        P("ep", "tp"),
        P("tp"),
        P("tp", None),
        P(("ep", "tp"), None),
        P(),
        P(("ep", "tp"), None),
        P(("ep", "tp"), None),
        P("ep", None, "tp"),
        P("ep", None, "tp"),
        P("ep", "tp", None),
    )
    out_specs = (P(("ep", "tp"), None), P(("ep", "tp"), None))
    return jax.shard_map(body, mesh=mesh, in_specs=in_specs, out_specs=out_specs, check_vma=False)
```

```python
import functools
import jax
import jax.numpy as jnp
from jax import lax
from jax.experimental import pallas as pl
from jax.experimental.pallas import tpu as pltpu
from jax.sharding import PartitionSpec as P

HEAD = 64
STATE = 128
SPAN = 128
RIM = 8
LANES = 128
MIX_ROWS = 32
CUT_EIGHTHS = 5

norm_eps = 1e-05
clamp_top = 7.0
sigmoid_sharp = 1.702
highest = lax.Precision.HIGHEST


def passed_along(block, axis, distance):
    devices = range(lax.axis_size(axis))
    route = [(i - distance, i) for i in devices if i - distance in devices]
    return lax.ppermute(block, axis, route)


def conv_block(buf, first, value_ref, rim_ref, taps_ref):
    @pl.when(first)
    def _():
        buf[0:RIM, :] = rim_ref[...].astype(jnp.float32)

    @pl.when(jnp.logical_not(first))
    def _():
        buf[0:RIM, :] = buf[SPAN : SPAN + RIM, :]

    buf[RIM : RIM + SPAN, :] = value_ref[...].astype(jnp.float32)
    taps = taps_ref[...].astype(jnp.float32)
    count = taps.shape[0]
    total = buf[RIM : RIM + SPAN, :] * taps[count - 1 : count]
    for j in range(count - 1):
        start = RIM - (count - 1) + j
        total = total + buf[start : start + SPAN, :] * taps[j : j + 1]
    return total * jax.nn.sigmoid(total)


def conv_after(buf, first, value_ref, rim_ref, has_rim, taps_ref):
    @pl.when(first)
    def _():
        rim = rim_ref[...].astype(jnp.float32)[RIM:]
        buf[0:RIM, :] = jnp.where(has_rim, rim, 0.0)

    @pl.when(jnp.logical_not(first))
    def _():
        buf[0:RIM, :] = buf[SPAN : SPAN + RIM, :]

    buf[RIM : RIM + SPAN, :] = value_ref[...].astype(jnp.float32)
    taps = taps_ref[...].astype(jnp.float32)
    count = taps.shape[0]
    total = buf[RIM : RIM + SPAN, :] * taps[count - 1 : count]
    for j in range(count - 1):
        start = RIM - (count - 1) + j
        total = total + buf[start : start + SPAN, :] * taps[j : j + 1]
    return total * jax.nn.sigmoid(total)


def spread(cols, h, width):
    return jnp.broadcast_to(cols[:, h : h + 1], (SPAN, width))


def state_kernel(per_group, groups, x_ref, xr_ref, xt_ref, b_ref, br_ref, bt_ref, lw_ref, end_ref,
                 state_ref, xbuf, bbuf):
    first = pl.program_id(0) == 0
    x = conv_block(xbuf, first, x_ref, xr_ref, xt_ref)
    b = conv_block(bbuf, first, b_ref, br_ref, bt_ref)

    @pl.when(first)
    def _():
        state_ref[...] = jnp.zeros_like(state_ref)

    lw = lw_ref[...]
    low = lax.broadcasted_iota(jnp.int32, (SPAN, 2 * HEAD), 1) < HEAD
    for g in range(groups):
        bt = b[:, g * STATE : (g + 1) * STATE].T.astype(jnp.bfloat16)
        for pair in range(per_group // 2):
            h = g * per_group + 2 * pair
            cols = slice(h * HEAD, (h + 2) * HEAD)
            factor = jnp.exp(jnp.where(low, spread(lw, h, 2 * HEAD), spread(lw, h + 1, 2 * HEAD)))
            xw = (x[:, cols] * factor).astype(jnp.bfloat16)
            added = jnp.dot(bt, xw, preferred_element_type=jnp.float32)
            state_ref[:, cols] = state_ref[:, cols] * end_ref[0, :, cols] + added


def output_kernel(per_group, groups, x_ref, xr_ref, xt_ref, b_ref, br_ref, bt_ref, c_ref, cr_ref,
                  ct_ref, z_ref, lw_ref, cum_ref, row_ref, end_ref, enter_ref, skip_ref, scale_ref,
                  out_ref, xbuf, bbuf, cbuf, state, ybuf):
    first = pl.program_id(0) == 0
    x = conv_block(xbuf, first, x_ref, xr_ref, xt_ref)
    b = conv_block(bbuf, first, b_ref, br_ref, bt_ref)
    c = conv_block(cbuf, first, c_ref, cr_ref, ct_ref)

    @pl.when(first)
    def _():
        state[...] = enter_ref[...]

    lw = lw_ref[...]
    cum = cum_ref[...]
    low = lax.broadcasted_iota(jnp.int32, (SPAN, 2 * HEAD), 1) < HEAD
    causal = lax.broadcasted_iota(jnp.int32, (SPAN, SPAN), 0) >= lax.broadcasted_iota(
        jnp.int32, (SPAN, SPAN), 1
    )
    group_cols = per_group * HEAD
    for g in range(groups):
        bg = b[:, g * STATE : (g + 1) * STATE]
        bt = bg.T.astype(jnp.bfloat16)
        cg = c[:, g * STATE : (g + 1) * STATE].astype(jnp.bfloat16)
        scores = jnp.dot(cg, bt, preferred_element_type=jnp.float32)
        squares = jnp.zeros((SPAN, 2 * HEAD), jnp.float32)
        for pair in range(per_group // 2):
            h = g * per_group + 2 * pair
            cols = slice(h * HEAD, (h + 2) * HEAD)
            xp = x[:, cols]
            cum_0, cum_1 = spread(cum, h, SPAN), spread(cum, h + 1, SPAN)
            m_0 = scores * jnp.exp(jnp.where(causal, cum_0 + row_ref[0, h : h + 1, :], -jnp.inf))
            m_1 = scores * jnp.exp(jnp.where(causal, cum_1 + row_ref[0, h + 1 : h + 2, :], -jnp.inf))
            mixing = jnp.concatenate([m_0.astype(jnp.bfloat16), m_1.astype(jnp.bfloat16)], axis=1)
            x_0 = jnp.where(low, xp, 0.0).astype(jnp.bfloat16)
            x_1 = jnp.where(low, 0.0, xp).astype(jnp.bfloat16)
            y = jnp.dot(
                mixing, jnp.concatenate([x_0, x_1], axis=0), preferred_element_type=jnp.float32
            )
            before = state[:, cols]
            carried = jnp.dot(cg, before.astype(jnp.bfloat16), preferred_element_type=jnp.float32)
            y = y + carried * jnp.exp(jnp.where(low, cum_0, cum_1)) + xp * skip_ref[:, cols]
            factor = jnp.exp(jnp.where(low, spread(lw, h, 2 * HEAD), spread(lw, h + 1, 2 * HEAD)))
            xw = (xp * factor).astype(jnp.bfloat16)
            added = jnp.dot(bt, xw, preferred_element_type=jnp.float32)
            state[:, cols] = before * end_ref[0, :, cols] + added
            gate = z_ref[:, cols].astype(jnp.float32)
            gated = y * (gate * jax.nn.sigmoid(gate))
            squares = squares + gated * gated
            ybuf[:, cols] = gated
        mean = jnp.sum(squares, axis=1, keepdims=True) / group_cols
        inverse = lax.rsqrt(mean + norm_eps)
        cols = slice(g * group_cols, (g + 1) * group_cols)
        out_ref[:, cols] = (ybuf[:, cols] * inverse * scale_ref[:, cols]).astype(jnp.bfloat16)


def entering_state(own_state, own_decay):
    size, mine = (lax.axis_size("ep"), lax.axis_index("ep"))
    rows = own_state.shape[0]
    total = own_state
    decay = own_decay

    def joined():
        return jnp.concatenate(
            [total, jnp.broadcast_to(decay, (RIM, decay.shape[1]))], axis=0
        ).astype(jnp.bfloat16)

    distance = 1
    while distance < size:
        came = passed_along(joined(), "ep", distance)
        there = mine >= distance
        earlier = came[:rows].astype(jnp.float32)
        earlier_decay = jnp.where(there, came[rows : rows + 1].astype(jnp.float32), 1.0)
        total = earlier * decay + total
        decay = earlier_decay * decay
        distance *= 2
    return passed_along(total.astype(jnp.bfloat16), "ep", 1).astype(jnp.float32)


def mixer_half(
    sequence_entry_features,
    sequence_exit_gating,
    memory_insert_clusters,
    memory_query_clusters,
    interval_presoftplus,
    entry_filter_taps,
    insert_filter_taps,
    query_filter_taps,
    interval_offset,
    head_fading_exponent,
    skip_connection_factor,
    spike_fading_exponent,
    cluster_scaling_vector,
    sequence_exit_projection,
    marked,
):
    tok_rows = sequence_entry_features.shape[0]
    local_heads = interval_offset.shape[0]
    local_groups = memory_insert_clusters.shape[1] // STATE
    per_group = local_heads // local_groups
    if marked is not None:
        heads = jnp.stack([interval_offset, head_fading_exponent, skip_connection_factor], axis=1)
        return mixer_gather(
            per_group, local_groups, tok_rows // SPAN,
            (sequence_entry_features, memory_insert_clusters, memory_query_clusters),
            (entry_filter_taps, insert_filter_taps, query_filter_taps), sequence_exit_gating,
            interval_presoftplus.T, spike_fading_exponent.T,
            jnp.pad(heads, ((0, 0), (0, LANES - heads.shape[1]))), cluster_scaling_vector[None],
            sequence_exit_projection, marked,
        )
    inner_cols = sequence_entry_features.shape[1]
    state_cols = memory_insert_clusters.shape[1]
    last_rows = jnp.concatenate(
        [
            sequence_entry_features[tok_rows - RIM :],
            memory_insert_clusters[tok_rows - RIM :],
            memory_query_clusters[tok_rows - RIM :],
        ],
        axis=1,
    )
    rims = passed_along(last_rows, "ep", 1)
    rim_x = rims[:, :inner_cols]
    rim_b = rims[:, inner_cols : inner_cols + state_cols]
    rim_c = rims[:, inner_cols + state_cols :]
    blocks = tok_rows // SPAN
    interval = jax.nn.softplus(interval_presoftplus.astype(jnp.float32) + interval_offset)
    fading = spike_fading_exponent - jnp.exp(head_fading_exponent) * interval
    lower = jnp.tril(jnp.ones((SPAN, SPAN), jnp.float32))
    cumulative = jnp.einsum(
        "ts,csh->cth", lower, fading.reshape(blocks, SPAN, local_heads), precision=highest
    )
    log_step = jnp.log(interval).reshape(blocks, SPAN, local_heads)
    block_end = cumulative[:, -1:]
    key_log = (log_step - cumulative + block_end).reshape(tok_rows, local_heads)
    row_log = jnp.swapaxes(log_step - cumulative, 1, 2)
    end_factor = jnp.repeat(jnp.exp(block_end), HEAD, axis=2)
    own_decay = jnp.repeat(jnp.exp(jnp.sum(block_end, axis=0)), HEAD, axis=1)
    cumulative = cumulative.reshape(tok_rows, local_heads)

    def rows_of(width):
        return pl.BlockSpec((SPAN, width), lambda i: (i, 0))

    def fixed(shape):
        return pl.BlockSpec(shape, lambda i: (0, 0))

    def block_of(rows, width):
        return pl.BlockSpec((1, rows, width), lambda i: (i, 0, 0))

    def cost(dots):
        return pl.CostEstimate(
            flops=dots * tok_rows * inner_cols * STATE * 8,
            bytes_accessed=dots * tok_rows * inner_cols * 8,
            transcendentals=0,
        )

    taps = entry_filter_taps.shape[0]
    x_specs = [rows_of(inner_cols), fixed((RIM, inner_cols)), fixed((taps, inner_cols))]
    s_specs = [rows_of(state_cols), fixed((RIM, state_cols)), fixed((taps, state_cols))]
    x_args = (sequence_entry_features, rim_x, entry_filter_taps)
    b_args = (memory_insert_clusters, rim_b, insert_filter_taps)
    c_args = (memory_query_clusters, rim_c, query_filter_taps)
    own_state = pl.pallas_call(
        functools.partial(state_kernel, per_group, local_groups),
        grid=(blocks,),
        in_specs=x_specs + s_specs + [rows_of(local_heads), block_of(1, inner_cols)],
        out_specs=fixed((STATE, inner_cols)),
        out_shape=jax.ShapeDtypeStruct((STATE, inner_cols), jnp.float32),
        scratch_shapes=[
            pltpu.VMEM((SPAN + RIM, inner_cols), jnp.float32),
            pltpu.VMEM((SPAN + RIM, state_cols), jnp.float32),
        ],
        cost_estimate=cost(1),
        name="own_state",
    )(*x_args, *b_args, key_log, end_factor)
    entering = entering_state(own_state, own_decay)
    normed = pl.pallas_call(
        functools.partial(output_kernel, per_group, local_groups),
        grid=(blocks,),
        in_specs=x_specs + s_specs + s_specs + [
            rows_of(inner_cols),
            rows_of(local_heads),
            rows_of(local_heads),
            block_of(local_heads, SPAN),
            block_of(1, inner_cols),
            fixed((STATE, inner_cols)),
            fixed((1, inner_cols)),
            fixed((1, inner_cols)),
        ],
        out_specs=rows_of(inner_cols),
        out_shape=jax.ShapeDtypeStruct((tok_rows, inner_cols), jnp.bfloat16),
        scratch_shapes=[
            pltpu.VMEM((SPAN + RIM, inner_cols), jnp.float32),
            pltpu.VMEM((SPAN + RIM, state_cols), jnp.float32),
            pltpu.VMEM((SPAN + RIM, state_cols), jnp.float32),
            pltpu.VMEM((STATE, inner_cols), jnp.float32),
            pltpu.VMEM((SPAN, inner_cols), jnp.float32),
        ],
        cost_estimate=cost(3),
        name="mixer_output",
    )(
        *x_args, *b_args, *c_args, sequence_exit_gating, key_log, cumulative, row_log, end_factor,
        entering, jnp.repeat(skip_connection_factor, HEAD)[None], cluster_scaling_vector[None],
    )
    return jnp.dot(normed, sequence_exit_projection, preferred_element_type=jnp.float32).astype(
        jnp.bfloat16
    )


def mixer_gather(
    per_group, groups, blocks, streams, filters, gating, raw, spikes, heads, scale,
    exit_projection, marked,
):
    tok_rows, inner_cols = gating.shape
    state_cols = streams[1].shape[1]
    head_count = raw.shape[0]
    features = exit_projection.shape[1]
    rows, marked_cols = marked.shape
    taps = filters[0].shape[0]
    devices = lax.axis_size("ep") * lax.axis_size("tp")
    depth = lax.axis_size("ep") // 2
    narrow, wide = jnp.bfloat16, inner_cols // 2
    pieces = 7 * depth

    def either(i):
        return jnp.where(i < blocks, i, jnp.maximum(i - blocks - 1, 0))

    def late(i):
        return jnp.maximum(i - blocks - 1, 0)

    def by_rows(width, at):
        return pl.BlockSpec((SPAN, width), lambda i: (at(i), 0))

    def by_lanes(at):
        return pl.BlockSpec((head_count, SPAN), lambda i: (0, at(i)))

    def early(i):
        return jnp.minimum(i, blocks - 1)

    def fixed(shape):
        return pl.BlockSpec(shape, lambda i: (0, 0))

    def conv_specs(width, at):
        return [by_rows(width, at), fixed((taps, width))]

    dma = pltpu.SemaphoreType.DMA
    hops = [dma((depth,)) for _ in range(12)]
    return pl.pallas_call(
        functools.partial(mixer_gather_kernel, per_group, groups, blocks, depth),
        grid=(2 * blocks + 1,),
        in_specs=conv_specs(inner_cols, either)
        + conv_specs(state_cols, either)
        + conv_specs(state_cols, late)
        + [
            by_rows(inner_cols, late),
            by_lanes(early),
            by_lanes(early),
            fixed((head_count, LANES)),
            fixed((1, inner_cols)),
            fixed((inner_cols, features)),
            fixed((rows, marked_cols)),
        ]
        + [pl.BlockSpec(memory_space=pl.ANY)] * 3,
        out_specs=[by_rows(features, late), pl.BlockSpec(memory_space=pl.ANY)],
        out_shape=[
            jax.ShapeDtypeStruct((tok_rows, features), narrow),
            jax.ShapeDtypeStruct((devices * rows, marked_cols), narrow),
        ],
        scratch_shapes=[
            pltpu.VMEM((blocks, SPAN, head_count), jnp.float32),
            pltpu.VMEM((blocks, SPAN, head_count), jnp.float32),
            pltpu.VMEM((blocks, head_count, SPAN), jnp.float32),
            pltpu.VMEM((blocks, 1, head_count), jnp.float32),
            pltpu.VMEM((1, head_count), jnp.float32),
            pltpu.VMEM((1, head_count), jnp.float32),
            pltpu.VMEM((1, inner_cols), jnp.float32),
            pltpu.VMEM((2 * RIM, inner_cols), narrow),
            pltpu.VMEM((2 * RIM, state_cols), narrow),
            pltpu.VMEM((2 * RIM, state_cols), narrow),
            dma((3,)), dma((3,)),
            pltpu.VMEM((SPAN + RIM, inner_cols), jnp.float32),
            pltpu.VMEM((SPAN + RIM, state_cols), jnp.float32),
            pltpu.VMEM((SPAN + RIM, state_cols), jnp.float32),
            pltpu.VMEM((STATE, inner_cols), jnp.float32),
            pltpu.VMEM((SPAN, inner_cols), jnp.float32),
            pltpu.VMEM((SPAN, inner_cols), narrow),
            pltpu.VMEM((STATE + 2 * RIM, inner_cols), narrow),
            pltpu.VMEM((STATE + 2 * RIM, inner_cols), narrow),
            pltpu.VMEM((STATE + 2 * RIM, wide), narrow),
            pltpu.VMEM((depth - 1, STATE + 2 * RIM, wide), narrow),
            pltpu.VMEM((STATE, wide), jnp.float32),
            pltpu.VMEM((STATE, wide), narrow),
            pltpu.VMEM((STATE, wide), narrow),
            dma((1,)), dma((depth - 1,)), dma((depth - 1,)),
            *hops,
            dma((pieces,)), dma((pieces,)), dma((1,)), dma((1,)), dma((depth - 1,)),
            dma((depth - 1,)), dma((1,)), dma((1,)),
        ],
        compiler_params=pltpu.CompilerParams(
            collective_id=1, has_side_effects=True, vmem_limit_bytes=56 * 1024 * 1024,
            dimension_semantics=("arbitrary",),
        ),
        cost_estimate=pl.CostEstimate(
            flops=tok_rows * inner_cols * (features * 2 + STATE * 16),
            bytes_accessed=tok_rows * inner_cols * 16,
            transcendentals=0,
        ),
        name="mixer_gather",
    )(
        streams[0], filters[0], streams[1], filters[1], streams[2], filters[2], gating, raw, spikes,
        heads, scale, exit_projection, marked, *streams,
    )


def experts_half(
    specialist_sample_slice,
    specialist_scaling_vector,
    chosen_specialists,
    dispatcher_affinity_matrix,
    gating_projection,
    expand_projection,
    shrink_projection,
):
    tok_rows = specialist_sample_slice.shape[0]
    feature_count = specialist_sample_slice.shape[1]
    top_count = chosen_specialists.shape[1]
    experts = lax.axis_size("ep")
    groups_tp = lax.axis_size("tp")
    capacity = tok_rows * top_count * 5 // (4 * experts)
    as_float = specialist_sample_slice.astype(jnp.float32)
    centred = as_float - jnp.mean(as_float, axis=1, keepdims=True)
    normed = (
        centred
        * lax.rsqrt(jnp.mean(centred * centred, axis=1, keepdims=True) + norm_eps)
        * specialist_scaling_vector
    ).astype(jnp.bfloat16)
    route_weight = jnp.exp(dispatcher_affinity_matrix) / jnp.sum(
        jnp.exp(dispatcher_affinity_matrix), axis=1, keepdims=True
    )
    flat_routes = chosen_specialists.reshape(-1)
    onehot = (flat_routes[:, None] == jnp.arange(experts, dtype=jnp.int32)[None, :]).astype(
        jnp.int32
    )
    position = jnp.sum(onehot * (jnp.cumsum(onehot, axis=0) - 1), axis=1)
    target = flat_routes * capacity + position
    token_ids = jnp.arange(tok_rows * top_count, dtype=jnp.int32) // top_count
    source_table = jnp.full((experts * capacity,), tok_rows, jnp.int32).at[target].set(token_ids)
    padded = jnp.concatenate([normed, jnp.zeros((1, feature_count), jnp.bfloat16)], axis=0)
    outgoing = padded[source_table].reshape(experts, capacity, feature_count)
    arrived = lax.all_to_all(outgoing, "ep", split_axis=0, concat_axis=0, tiled=True)
    shard_rows = lax.all_gather(arrived, "tp", axis=0, tiled=True)
    rows_in = shard_rows.reshape(-1, feature_count)
    gate_h = jnp.dot(rows_in, gating_projection[0], preferred_element_type=jnp.float32)
    up_h = jnp.dot(rows_in, expand_projection[0], preferred_element_type=jnp.float32)
    clipped = jnp.minimum(gate_h, clamp_top)
    hidden_act = (
        (
            clipped
            * jax.nn.sigmoid(sigmoid_sharp * clipped)
            * (jnp.clip(up_h, -clamp_top, clamp_top) + 1.0)
        )
        .astype(jnp.bfloat16)
        .reshape(shard_rows.shape[0], capacity, -1)
    )
    hidden_act = hidden_act.reshape(groups_tp * experts * capacity, -1)
    summed = lax.psum_scatter(
        jnp.dot(hidden_act, shrink_projection[0], preferred_element_type=jnp.float32).astype(
            jnp.bfloat16
        ),
        "tp",
        scatter_dimension=0,
        tiled=True,
    )
    returned = lax.all_to_all(
        summed.reshape(experts, capacity, feature_count),
        "ep",
        split_axis=0,
        concat_axis=0,
        tiled=True,
    )
    slot_out = returned.reshape(experts * capacity, feature_count)[target].reshape(
        tok_rows, top_count, feature_count
    )
    combined = jnp.einsum("tk,tkd->td", route_weight, slot_out.astype(jnp.float32))
    return combined.astype(jnp.bfloat16)


def routing_kernel(experts, x_ref, scale_ref, chosen_ref, score_ref, out_ref, turned):
    features = x_ref.shape[1]
    top_count, rows = chosen_ref.shape
    value = x_ref[...].astype(jnp.float32)
    centred = value - jnp.mean(value, axis=1, keepdims=True)
    spread_of = jnp.mean(centred * centred, axis=1, keepdims=True)
    normed = centred * lax.rsqrt(spread_of + norm_eps) * scale_ref[...]
    out_ref[:, :features] = normed.astype(jnp.bfloat16)
    raised = jnp.exp(score_ref[...])
    turned[...] = jnp.zeros_like(turned)
    turned[0:top_count, :] = chosen_ref[...].astype(jnp.float32)
    turned[8 : 8 + top_count, :] = raised / jnp.sum(raised, axis=0, keepdims=True)
    columns = turned[...].T
    lane = lax.broadcasted_iota(jnp.int32, (rows, LANES), 1)
    named = lax.rem(lane, experts).astype(jnp.float32)
    held = jnp.zeros((rows, LANES), jnp.float32)
    share = jnp.zeros((rows, LANES), jnp.float32)
    for k in range(top_count):
        same = columns[:, k : k + 1] == named
        held = held + jnp.where(same, 1.0, 0.0)
        share = share + jnp.where(same, columns[:, 8 + k : 9 + k], 0.0)
    earlier = lax.broadcasted_iota(jnp.int32, (rows, rows), 0) > lax.broadcasted_iota(
        jnp.int32, (rows, rows), 1
    )
    place = jnp.dot(
        jnp.where(earlier, 1.0, 0.0).astype(jnp.bfloat16),
        held.astype(jnp.bfloat16),
        preferred_element_type=jnp.float32,
    )
    place = jnp.where(held > 0.0, place, 255.0)
    coarse = share.astype(jnp.bfloat16).astype(jnp.float32)
    table = jnp.where(lane < experts, place, jnp.where(lane < 2 * experts, coarse, share - coarse))
    out_ref[:, features:] = table.astype(jnp.bfloat16)


def experts_kernel(
    experts, capacity, tokens_ref, mix_ref, gate_ref, up_ref, down_ref, out_ref, mixed_ref,
    tokens, slots, own_a, own_b, outgoing_a, outgoing_b, incoming_a, incoming_b, place, place_next,
    from_x, from_y, to_y, came_y, to_x, came_x, keep_a, keep_b, to_za, from_za, to_zb, from_zb,
    mix_own, mix_core, mix_out, mix_in, mix_sem, mc_send, mc_recv, mx_send, mx_recv,
    token_sem, core_send, core_recv, x_send, x_recv, y_send, y_recv,
    a_send, a_recv, b_send, b_recv, za_send, za_recv, zb_send, zb_recv,
):
    depth = experts // 2
    steps = experts
    ep, tp = lax.axis_index("ep"), lax.axis_index("tp")
    z, y, x, core = ep // 2, ep % 2, tp // 2, tp % 2
    next_ep = z * 2 + 1 - y
    sibling = {"tp": x * 2 + 1 - core}
    x_next = {"tp": (1 - x) * 2 + core}
    y_next = {"ep": next_ep}
    rows = out_ref.shape[0]
    features = out_ref.shape[1]
    cut = own_a.shape[3]
    own, outgoing, incoming = (own_a, own_b), (outgoing_a, outgoing_b), (incoming_a, incoming_b)
    mesh_id = pl.DeviceIdType.MESH

    def z_next(k):
        return {"ep": ((z + k) % depth) * 2 + y}

    def turn(i):
        middle = depth // 2
        others = jnp.where(i == 0, middle, jnp.where(i < middle, i, i + 1))
        return jnp.where(i == depth - 1, 0, others)

    def fetch(s):
        k, dy = turn(s // 2), 1 - s % 2
        block = ((z + k) % depth) * 2 + (y + dy) % 2
        span = 4 * rows
        return pltpu.make_async_copy(
            tokens_ref.at[pl.ds(pl.multiple_of(block * span, span), span)],
            tokens.at[s % 2],
            token_sem.at[s % 2],
        )

    def remote(source, target, send, recv, device):
        return pltpu.make_async_remote_copy(
            src_ref=source, dst_ref=target, send_sem=send, recv_sem=recv,
            device_id=device, device_id_type=mesh_id,
        )

    def core_copy(s, side):
        send, recv = core_send.at[2 * s + side], core_recv.at[2 * s + side]
        return remote(outgoing[side].at[s], incoming[side].at[s], send, recv, sibling)

    def x_copy(s):
        return remote(own_a.at[s, 1], from_x.at[s], x_send.at[s], x_recv.at[s], x_next)

    def y_copy(i):
        return remote(own_b.at[2 * i], from_y.at[i], y_send.at[i], y_recv.at[i], y_next)

    def a_copy(i):
        return remote(to_y.at[i], came_y.at[i], a_send.at[i], a_recv.at[i], y_next)

    def b_copy():
        return remote(to_x, came_x, b_send.at[0], b_recv.at[0], x_next)

    def za_copy(i):
        return remote(to_za.at[i], from_za.at[i], za_send.at[i], za_recv.at[i], z_next(turn(i)))

    def zb_copy(i):
        return remote(to_zb.at[i], from_zb.at[i], zb_send.at[i], zb_recv.at[i], z_next(turn(i)))

    chunks, piece = mixed_ref.shape[0] // MIX_ROWS, MIX_ROWS
    share = mixed_ref.shape[0]

    def mix_rows(dx, c):
        block = ((x + dx) % 2) * 2 + c
        return mix_ref.at[pl.ds(pl.multiple_of(block * share, share), share)]

    def mix_fetch(dx):
        return pltpu.make_async_copy(mix_rows(dx, core), mix_own.at[dx], mix_sem.at[dx])

    def mix_core_copy(dx):
        return remote(
            mix_rows(dx, 1 - core), mix_core.at[dx], mc_send.at[dx], mc_recv.at[dx], sibling
        )

    def mix_x_copy(j):
        rows_j = pl.ds(pl.multiple_of(j * piece, piece), piece)
        return remote(
            mix_out.at[rows_j], mix_in.at[rows_j], mx_send.at[j], mx_recv.at[j], x_next
        )

    def mix_piece(j, carry):
        rows_j = pl.ds(pl.multiple_of(j * piece, piece), piece)
        mix_out[rows_j, :] = (
            mix_own[1, rows_j, :].astype(jnp.float32) + mix_core[1, rows_j, :].astype(jnp.float32)
        ).astype(jnp.bfloat16)
        mix_own[0, rows_j, :] = (
            mix_own[0, rows_j, :].astype(jnp.float32) + mix_core[0, rows_j, :].astype(jnp.float32)
        ).astype(jnp.bfloat16)
        return carry

    def mix_send(j, carry):
        mix_x_copy(j).start()
        return carry

    def mix_finish(j, carry):
        rows_j = pl.ds(pl.multiple_of(j * piece, piece), piece)
        mix_x_copy(j).wait_recv()
        mixed_ref[rows_j, :] = (
            mix_own[0, rows_j, :].astype(jnp.float32) + mix_in[rows_j, :].astype(jnp.float32)
        ).astype(jnp.bfloat16)
        return carry

    def mix_sent(j, carry):
        mix_x_copy(j).wait_send()
        return carry

    fetch(0).start()
    for dx in (1, 0):
        mix_fetch(dx).start()
    barrier = pltpu.get_barrier_semaphore()
    partners = [sibling, x_next, y_next] + [z_next(k) for k in range(1, depth)]
    for partner in partners:
        pl.semaphore_signal(barrier, inc=1, device_id=partner, device_id_type=mesh_id)
    pl.semaphore_wait(barrier, len(partners))

    for dx in (1, 0):
        mix_core_copy(dx).start()

    lane = lax.broadcasted_iota(jnp.int32, (rows, LANES), 1)
    lane_value = lane.astype(jnp.float32)
    slot_lane = lax.broadcasted_iota(jnp.int32, (capacity, LANES), 1)

    def chosen_slots(table, expert):
        column = jnp.sum(jnp.where(lane == expert, table, 0.0), axis=1, keepdims=True)
        return jnp.where(column == lane_value, 1.0, 0.0)

    def compute(s):
        weights = []
        for dx in (0, 1):
            for q in (0, 1):
                c = core if q == 0 else 1 - core
                block = ((x + dx) % 2) * 2 + c
                start = pl.multiple_of(block * rows, rows)
                arrived = tokens[s % 2, pl.ds(start, rows), :]
                table = arrived[:, features:].astype(jnp.float32)
                picked = chosen_slots(table, ep)
                if q == 0:
                    place[s, dx] = picked.astype(jnp.bfloat16)
                    place_next[s, dx] = chosen_slots(table, next_ep).astype(jnp.bfloat16)
                select = picked.T[:capacity].astype(jnp.bfloat16)
                taken = jnp.dot(select, arrived, preferred_element_type=jnp.float32)
                first = (dx * 2 + q) * capacity
                slots[first : first + capacity, :] = taken[:, :features].astype(jnp.bfloat16)
                mine = (slot_lane == experts + ep) | (slot_lane == 2 * experts + ep)
                weights.append(
                    jnp.sum(jnp.where(mine, taken[:, features:], 0.0), axis=1, keepdims=True)
                )
        value = slots[...]
        gate_h = jnp.dot(value, gate_ref[...], preferred_element_type=jnp.float32)
        up_h = jnp.dot(value, up_ref[...], preferred_element_type=jnp.float32)
        clipped = jnp.minimum(gate_h, clamp_top)
        act = (
            clipped
            * jax.nn.sigmoid(sigmoid_sharp * clipped)
            * (jnp.clip(up_h, -clamp_top, clamp_top) + 1.0)
        ).astype(jnp.bfloat16)
        for side in (0, 1):
            columns = slice(0, cut) if side == 0 else slice(cut, features)
            part = jnp.dot(act, down_ref[:, columns], preferred_element_type=jnp.float32)
            for dx in (0, 1):
                for q in (0, 1):
                    first = (dx * 2 + q) * capacity
                    scaled = (part[first : first + capacity] * weights[dx * 2 + q]).astype(
                        jnp.bfloat16
                    )
                    if q == 0:
                        own[side][s, dx] = scaled
                    else:
                        outgoing[side][s, dx] = scaled

    def spread_out(where, value):
        return jnp.dot(where[:, :capacity], value, preferred_element_type=jnp.float32)

    last_x = 2 * depth + 2

    def step(s, carry):
        @pl.when(s < steps)
        def _():
            @pl.when(s + 1 < steps)
            def _():
                fetch(s + 1).start()

            fetch(s).wait()
            compute(s)

        @pl.when((s >= 1) & (s <= steps))
        def _():
            t = s - 1
            for side in (0, 1):
                core_copy(t, side).wait_recv()
                for dx in (0, 1):
                    own[side][t, dx] = (
                        own[side][t, dx].astype(jnp.float32)
                        + incoming[side][t, dx].astype(jnp.float32)
                    ).astype(jnp.bfloat16)

        @pl.when(s < steps)
        def _():
            for side in (0, 1):
                core_copy(s, side).start()

        @pl.when(s == 0)
        def _():
            for dx in (1, 0):
                mix_fetch(dx).wait()
                mix_core_copy(dx).wait_recv()
            lax.fori_loop(0, chunks, mix_piece, 0)

        i = (s - 4) // 2

        @pl.when((s >= 4) & (s % 2 == 0) & (i < depth))
        def _():
            far, near = 2 * i, 2 * i + 1
            y_copy(i).wait_recv()
            for dx in (0, 1):
                sum_b = spread_out(place[near, dx], own_b[near, dx]) + spread_out(
                    place_next[near, dx], from_y[i, dx]
                )

                @pl.when(i < depth - 1)
                def _():
                    to_zb[i, dx] = sum_b.astype(jnp.bfloat16)

                @pl.when(i == depth - 1)
                def _():
                    keep_b[dx] = sum_b

            x_copy(far).wait_recv()
            where = place[far, 0]
            to_y[i] = (spread_out(where, own_a[far, 0]) + spread_out(where, from_x[far])).astype(
                jnp.bfloat16
            )

            @pl.when(i < depth - 1)
            def _():
                zb_copy(i).start()

            x_copy(near).wait_recv()
            where = place[near, 0]
            keep_a[i] = spread_out(where, own_a[near, 0]) + spread_out(where, from_x[near])
            a_copy(i).start()

        @pl.when((s >= 1) & (s <= steps))
        def _():
            t = s - 1
            x_copy(t).start()

            @pl.when(t % 2 == 0)
            def _():
                y_copy(t // 2).start()

        early, late = chunks // 4, chunks // 2
        begin = jnp.where(s == 0, 0, jnp.where(s < last_x, early + s - 3, late))
        end = jnp.where(s == 0, early, jnp.where(s < last_x, early + s - 2, chunks))
        lax.fori_loop(
            jnp.where((s == 0) | (s == last_x), begin, jnp.clip(begin, early, late)),
            jnp.where((s == 0) | (s == last_x), end,
                      jnp.where(s > last_x, 0, jnp.clip(end, early, late))),
            mix_send, 0,
        )

        j = (s - 6) // 2

        @pl.when((s >= 6) & (s % 2 == 0) & (j < depth))
        def _():
            a_copy(j).wait_recv()
            sum_a = keep_a[j] + came_y[j].astype(jnp.float32)

            @pl.when(j < depth - 1)
            def _():
                to_za[j] = sum_a.astype(jnp.bfloat16)
                za_copy(j).start()

            @pl.when(j == depth - 1)
            def _():
                keep_a[j] = sum_a

        return carry

    lax.fori_loop(0, 2 * depth + 5, step, 0)
    for i in range(depth - 1):
        zb_copy(i).wait_recv()
    total = [keep_b[0], keep_b[1]]
    for i in range(depth - 1):
        total = [total[dx] + from_zb[i, dx].astype(jnp.float32) for dx in (0, 1)]
    to_x[...] = total[1].astype(jnp.bfloat16)
    keep_b[0] = total[0]
    total = keep_a[depth - 1]
    for i in range(depth - 1):
        za_copy(i).wait_recv()
        total = total + from_za[i].astype(jnp.float32)
    out_ref[:, :cut] = total.astype(jnp.bfloat16)
    b_copy().start()
    lax.fori_loop(0, chunks, mix_finish, 0)
    lax.fori_loop(0, chunks, mix_sent, 0)
    b_copy().wait_recv()
    out_ref[:, cut:] = (keep_b[0] + came_x[...].astype(jnp.float32)).astype(jnp.bfloat16)
    for dx in (0, 1):
        mix_core_copy(dx).wait_send()
    for s in range(steps):
        for side in (0, 1):
            core_copy(s, side).wait_send()
        x_copy(s).wait_send()
    for i in range(depth):
        y_copy(i).wait_send()
        a_copy(i).wait_send()
    b_copy().wait_send()
    for i in range(depth - 1):
        za_copy(i).wait_send()
        zb_copy(i).wait_send()


def mixer_gather_kernel(
    per_group, groups, blocks, depth,
    x_ref, xt_ref, b_ref, bt_ref, c_ref, ct_ref, z_ref, pre_ref, spike_ref, head_ref, scale_ref,
    exit_ref, marked_ref, x_all, b_all, c_all,
    part_ref, tokens_ref,
    lw_of, cum_of, row_of, end_of, skip_of, decay_of, decay_row, xr_ref, br_ref, cr_ref, rim_s,
    rim_r, xbuf, bbuf, cbuf, state, ybuf, nbuf, pair_out, pair_in, line_out, line_in, line_sum, swap_out,
    swap_in, local_sem, z_send, z_recv, xa_s, xa_r, xb_s, xb_r, xf_s, xf_r, ya_s, ya_r, yb_s, yb_r,
    yf_s, yf_r, d_s, d_r, pair_s, pair_r, line_s, line_r, swap_s, swap_r,
):
    step = pl.program_id(0)
    ep, tp = lax.axis_index("ep"), lax.axis_index("tp")
    z, y, x, core = ep // 2, ep % 2, tp // 2, tp % 2
    sibling = {"tp": x * 2 + 1 - core}
    x_next = {"tp": (1 - x) * 2 + core}
    y_next = {"ep": z * 2 + 1 - y}
    mesh_id = pl.DeviceIdType.MESH
    rows = marked_ref.shape[0]
    part_rows = rows // 2
    inner = state.shape[1]
    wide = inner // 2

    def z_next(k):
        return {"ep": ((z + k) % depth) * 2 + y}

    def remote(source, target, send, recv, device):
        return pltpu.make_async_remote_copy(
            src_ref=source, dst_ref=target, send_sem=send, recv_sem=recv,
            device_id=device, device_id_type=mesh_id,
        )

    def region(dx, dy, k, half, c=core):
        block = (((z + depth - k) % depth) * 2 + (y + dy) % 2) * 4 + ((x + dx) % 2) * 2 + c
        size = rows if half is None else part_rows
        start = block * rows + (0 if half is None else half * part_rows)
        return tokens_ref.at[pl.ds(pl.multiple_of(start, part_rows), size)]

    def source(dx, dy, k, half):
        if (dx, dy, k) == (0, 0, 0):
            if half is None:
                return marked_ref
            return marked_ref.at[pl.ds(half * part_rows, part_rows)]
        return region(dx, dy, k, half)

    def z_copy(k):
        return remote(
            marked_ref, region(0, 0, 0, None), z_send.at[k - 1], z_recv.at[k - 1], z_next(k)
        )

    def z_came(k):
        here = region(0, 0, k, None)
        return remote(here, here, z_send.at[k - 1], z_recv.at[k - 1], z_next(k))

    moves = {
        "xa": ((0, 0, 0), (1, 0, 0), xa_s, xa_r, x_next),
        "xb": ((0, 0, 1), (1, 0, 1), xb_s, xb_r, x_next),
        "xf": ((0, 1, 1), (1, 1, 1), xf_s, xf_r, x_next),
        "yb": ((0, 0, 1), (0, 1, 1), yb_s, yb_r, y_next),
        "ya": ((0, 0, 0), (0, 1, 0), ya_s, ya_r, y_next),
        "yf": ((1, 0, 0), (1, 1, 0), yf_s, yf_r, y_next),
    }

    def sent(name, k):
        (dx, dy, half), _, send, recv, device = moves[name]
        return remote(
            source(dx, dy, k, half), region(dx, dy, k, half), send.at[k], recv.at[k], device
        )

    def came(name, k):
        _, (dx, dy, half), send, recv, device = moves[name]
        here = region(dx, dy, k, half)
        return remote(here, here, send.at[k], recv.at[k], device)

    shared = [(0, 0, None), (1, 0, 0), (1, 0, 1), (0, 1, 1), (0, 1, 0), (1, 1, 0), (1, 1, 1)]

    def d_sent(k, n):
        dx, dy, half = shared[n]
        m = len(shared) * k + n
        return remote(
            source(dx, dy, k, half), region(dx, dy, k, half), d_s.at[m], d_r.at[m], sibling
        )

    def d_came(k, n):
        dx, dy, half = shared[n]
        m = len(shared) * k + n
        here = region(dx, dy, k, half, 1 - core)
        return remote(here, here, d_s.at[m], d_r.at[m], sibling)

    def first_hop(k):
        if k > 0:
            z_came(k).wait_recv()
        for name in ("xa", "yb", "xb", "ya"):
            sent(name, k).start()
        d_sent(k, 0).start()

    def second_hop(k):
        came("xa", k).wait_recv()
        sent("yf", k).start()
        d_sent(k, 1).start()
        came("yb", k).wait_recv()
        sent("xf", k).start()
        d_sent(k, 3).start()

    def last_hop(k, parts=(("xb", 2), ("ya", 4), ("yf", 5), ("xf", 6))):
        for name, n in parts:
            came(name, k).wait_recv()
            d_sent(k, n).start()

    devices = 2 * depth
    after, before = {"ep": (ep + 1) % devices}, {"ep": (ep + devices - 1) % devices}
    last_rows = pl.ds(x_all.shape[0] - 2 * RIM, 2 * RIM)

    def rim_copy(n):
        whole, rim = ((x_all, xr_ref), (b_all, br_ref), (c_all, cr_ref))[n]
        return remote(whole.at[last_rows], rim, rim_s.at[n], rim_r.at[n], after)

    def own_copy():
        return pltpu.make_async_copy(marked_ref, region(0, 0, 0, None), local_sem.at[0])

    @pl.when(step == 0)
    def _():
        barrier = pltpu.get_barrier_semaphore()
        partners = [sibling, x_next, y_next, after, before]
        partners = partners + [z_next(k) for k in range(1, depth)]
        for partner in partners:
            pl.semaphore_signal(barrier, inc=1, device_id=partner, device_id_type=mesh_id)
        pl.semaphore_wait(barrier, len(partners))
        for n in range(3):
            rim_copy(n).start()
        z_copy(1).start()
        first_hop(0)
        for k in range(2, depth - 1):
            z_copy(k).start()
        own_copy().start()
        turned = head_ref[...].T
        skip_of[...] = turned[2:3]
        decay_of[...] = jnp.ones_like(decay_of)
        for n in range(3):
            rim_copy(n).wait_recv()

    def per_head(row, h):
        first_head = jnp.broadcast_to(row[:, h : h + 1], (1, 2 * HEAD))
        second_head = jnp.broadcast_to(row[:, h + 1 : h + 2], (1, 2 * HEAD))
        return jnp.where(low[0:1], first_head, second_head)

    has_rim = ep > 0
    low = lax.broadcasted_iota(jnp.int32, (SPAN, 2 * HEAD), 1) < HEAD
    state_pass = step < blocks
    output_pass = step > blocks

    @pl.when(state_pass)
    def _():
        first = step == 0
        xv = conv_after(xbuf, first, x_ref, xr_ref, has_rim, xt_ref)
        bv = conv_after(bbuf, first, b_ref, br_ref, has_rim, bt_ref)

        @pl.when(first)
        def _():
            state[...] = jnp.zeros_like(state)

        raw = pre_ref[...].astype(jnp.float32) + head_ref[:, 0:1]
        interval = jnp.maximum(raw, 0.0) + jnp.log1p(jnp.exp(-jnp.abs(raw)))
        fading = spike_ref[...] - jnp.exp(head_ref[:, 1:2]) * interval
        upto = lax.broadcasted_iota(jnp.int32, (SPAN, SPAN), 0) <= lax.broadcasted_iota(
            jnp.int32, (SPAN, SPAN), 1
        )
        cumulative = jnp.dot(
            fading, jnp.where(upto, 1.0, 0.0), precision=highest, preferred_element_type=jnp.float32
        )
        row_log = jnp.log(interval) - cumulative
        lw = (row_log + cumulative[:, SPAN - 1 :]).T
        cum = cumulative.T
        end = jnp.exp(cum[SPAN - 1 :])
        row_of[step] = row_log
        lw_of[step] = lw
        cum_of[step] = cum
        end_of[step] = end
        decay_of[...] = decay_of[...] * end
        for g in range(groups):
            bt = bv[:, g * STATE : (g + 1) * STATE].T.astype(jnp.bfloat16)
            for pair in range(per_group // 2):
                h = g * per_group + 2 * pair
                cols = slice(h * HEAD, (h + 2) * HEAD)
                factor = jnp.exp(
                    jnp.where(low, spread(lw, h, 2 * HEAD), spread(lw, h + 1, 2 * HEAD))
                )
                xw = (xv[:, cols] * factor).astype(jnp.bfloat16)
                added = jnp.dot(bt, xw, preferred_element_type=jnp.float32)
                state[:, cols] = state[:, cols] * per_head(end, h) + added

    @pl.when(step == blocks // 2)
    def _():
        second_hop(0)

    @pl.when(step == blocks)
    def _():
        pair = remote(pair_out, pair_in, pair_s.at[0], pair_r.at[0], y_next)
        swap = remote(swap_out, swap_in, swap_s.at[0], swap_r.at[0], y_next)

        def line(k):
            return remote(
                line_out, line_in.at[k - 1], line_s.at[k - 1], line_r.at[k - 1], z_next(k)
            )

        for h in range(0, groups * per_group, 2):
            decay_row[:, h * HEAD : (h + 2) * HEAD] = per_head(decay_of[...], h)
        decay = decay_row[...]
        pair_out[:STATE, :] = state[...].astype(jnp.bfloat16)
        pair_out[STATE:, :] = jnp.broadcast_to(decay, (2 * RIM, inner)).astype(jnp.bfloat16)
        last_hop(0, (("xb", 2), ("ya", 4)))
        pair.start()
        first_hop(1)
        last_hop(0, (("yf", 5), ("xf", 6)))
        pair.wait_recv()
        mine = pl.ds(pl.multiple_of(y * wide, wide), wide)
        theirs = pl.ds(pl.multiple_of((1 - y) * wide, wide), wide)
        own_state, own_decay = state[:, mine], decay_row[:, mine]
        other_state = pair_in[:STATE, mine].astype(jnp.float32)
        other_decay = pair_in[STATE : STATE + 1, mine].astype(jnp.float32)
        later = y == 1
        both = jnp.where(
            later, other_state * own_decay + own_state, own_state * other_decay + other_state
        )
        line_out[:STATE, :] = both.astype(jnp.bfloat16)
        line_out[STATE:, :] = jnp.broadcast_to(own_decay * other_decay, (2 * RIM, wide)).astype(
            jnp.bfloat16
        )
        line_sum[...] = jnp.zeros_like(line_sum)
        for k in range(1, depth):
            @pl.when(z + k < depth)
            def _():
                line(k).start()

        z_copy(depth - 1).start()
        for k in range(depth - 1, 0, -1):
            @pl.when(z >= k)
            def _():
                line(k).wait_recv()
                line_sum[...] = line_sum[...] * line_in[k - 1, STATE : STATE + 1, :].astype(
                    jnp.float32
                ) + line_in[k - 1, :STATE, :].astype(jnp.float32)

        swap_out[...] = line_sum[...].astype(jnp.bfloat16)
        state[:, mine] = line_sum[...]
        second_hop(1)
        swap.start()
        swap.wait_recv()
        state[:, theirs] = swap_in[...].astype(jnp.float32)

        @pl.when(later)
        def _():
            state[...] = state[...] * pair_in[STATE : STATE + 1, :].astype(jnp.float32) + pair_in[
                :STATE, :
            ].astype(jnp.float32)

        pair.wait_send()
        swap.wait_send()
        for k in range(1, depth):
            @pl.when(z + k < depth)
            def _():
                line(k).wait_send()

    @pl.when(output_pass)
    def _():
        first = step == blocks + 1
        xv = conv_after(xbuf, first, x_ref, xr_ref, has_rim, xt_ref)
        bv = conv_after(bbuf, first, b_ref, br_ref, has_rim, bt_ref)
        cv = conv_after(cbuf, first, c_ref, cr_ref, has_rim, ct_ref)
        at = step - blocks - 1
        lw = lw_of[at]
        cum = cum_of[at]
        end = end_of[at]
        causal = lax.broadcasted_iota(jnp.int32, (SPAN, SPAN), 0) >= lax.broadcasted_iota(
            jnp.int32, (SPAN, SPAN), 1
        )
        group_cols = per_group * HEAD
        for g in range(groups):
            bt = bv[:, g * STATE : (g + 1) * STATE].T.astype(jnp.bfloat16)
            cg = cv[:, g * STATE : (g + 1) * STATE].astype(jnp.bfloat16)
            scores = jnp.dot(cg, bt, preferred_element_type=jnp.float32)
            squares = jnp.zeros((SPAN, 2 * HEAD), jnp.float32)
            for pair in range(per_group // 2):
                h = g * per_group + 2 * pair
                cols = slice(h * HEAD, (h + 2) * HEAD)
                xp = xv[:, cols]
                cum_0, cum_1 = spread(cum, h, SPAN), spread(cum, h + 1, SPAN)
                row_0, row_1 = row_of[at, h : h + 1, :], row_of[at, h + 1 : h + 2, :]
                m_0 = scores * jnp.exp(jnp.where(causal, cum_0 + row_0, -jnp.inf))
                m_1 = scores * jnp.exp(jnp.where(causal, cum_1 + row_1, -jnp.inf))
                mixing = jnp.concatenate([m_0.astype(jnp.bfloat16), m_1.astype(jnp.bfloat16)], axis=1)
                x_0 = jnp.where(low, xp, 0.0).astype(jnp.bfloat16)
                x_1 = jnp.where(low, 0.0, xp).astype(jnp.bfloat16)
                value = jnp.dot(
                    mixing, jnp.concatenate([x_0, x_1], axis=0), preferred_element_type=jnp.float32
                )
                before = state[:, cols]
                carried = jnp.dot(cg, before.astype(jnp.bfloat16), preferred_element_type=jnp.float32)
                value = value + carried * jnp.exp(jnp.where(low, cum_0, cum_1)) + xp * per_head(skip_of[...], h)
                factor = jnp.exp(
                    jnp.where(low, spread(lw, h, 2 * HEAD), spread(lw, h + 1, 2 * HEAD))
                )
                xw = (xp * factor).astype(jnp.bfloat16)
                added = jnp.dot(bt, xw, preferred_element_type=jnp.float32)
                state[:, cols] = before * per_head(end, h) + added
                gate = z_ref[:, cols].astype(jnp.float32)
                gated = value * (gate * jax.nn.sigmoid(gate))
                squares = squares + gated * gated
                ybuf[:, cols] = gated
            mean = jnp.sum(squares, axis=1, keepdims=True) / group_cols
            inverse = lax.rsqrt(mean + norm_eps)
            cols = slice(g * group_cols, (g + 1) * group_cols)
            nbuf[:, cols] = (ybuf[:, cols] * inverse * scale_ref[:, cols]).astype(jnp.bfloat16)
        part_ref[...] = jnp.dot(
            nbuf[...], exit_ref[...], preferred_element_type=jnp.float32
        ).astype(jnp.bfloat16)

    pace = blocks // (2 * depth - 2)
    for k in range(2, depth):
        at = blocks + 1 + (2 * k - 3) * pace

        @pl.when(step == at)
        def _():
            first_hop(k)

        @pl.when(step == at + pace)
        def _():
            second_hop(k)
            last_hop(k - 1)

    @pl.when(step == 2 * blocks)
    def _():
        last_hop(depth - 1)
        for k in range(depth):
            for n in range(len(shared)):
                d_came(k, n).wait_recv()
        own_copy().wait()
        for n in range(3):
            rim_copy(n).wait_send()
        for k in range(1, depth):
            z_copy(k).wait_send()
        for k in range(depth):
            for name in moves:
                sent(name, k).wait_send()
            for n in range(len(shared)):
                d_sent(k, n).wait_send()


def dense_experts_fit(tok_rows, top_count, capacity, mix_rows):
    experts = lax.axis_size("ep")
    fits = experts % 2 == 0 and experts >= 4 and 3 * experts <= LANES and lax.axis_size("tp") == 4
    return fits and 2 * top_count >= experts and mix_rows % (4 * MIX_ROWS) == 0 and tok_rows == LANES and capacity % 16 == 0 and top_count <= 8


def marked_tokens(
    specialist_sample_slice, specialist_scaling_vector, chosen_specialists, dispatcher_affinity_matrix
):
    rows, features = specialist_sample_slice.shape
    return pl.pallas_call(
        functools.partial(routing_kernel, lax.axis_size("ep")),
        out_shape=jax.ShapeDtypeStruct((rows, features + LANES), jnp.bfloat16),
        scratch_shapes=[pltpu.VMEM((LANES, rows), jnp.float32)],
        name="routing",
    )(
        specialist_sample_slice, specialist_scaling_vector[None], chosen_specialists.T,
        dispatcher_affinity_matrix.T,
    )


def experts_dense(
    tokens, mix_part, rows, capacity, gating_projection, expand_projection, shrink_projection
):
    experts = lax.axis_size("ep")
    features = gating_projection.shape[1]
    depth, steps = experts // 2, experts
    cut = features * CUT_EIGHTHS // 8 // LANES * LANES
    rest = features - cut
    hidden = gating_projection.shape[2]
    narrow = jnp.bfloat16
    dma = pltpu.SemaphoreType.DMA
    share = mix_part.shape[0] // 4
    pieces = share // MIX_ROWS
    work = 2 * experts * 4 * capacity * features * hidden * 3
    return pl.pallas_call(
        functools.partial(experts_kernel, experts, capacity),
        in_specs=[pl.BlockSpec(memory_space=pl.ANY)] * 2
        + [pl.BlockSpec(memory_space=pltpu.VMEM)] * 3,
        out_specs=[pl.BlockSpec(memory_space=pltpu.VMEM)] * 2,
        out_shape=[
            jax.ShapeDtypeStruct((rows, features), narrow),
            jax.ShapeDtypeStruct((share, features), narrow),
        ],
        scratch_shapes=[
            pltpu.VMEM((2, 4 * rows, features + LANES), narrow),
            pltpu.VMEM((4 * capacity, features), narrow),
            pltpu.VMEM((steps, 2, capacity, cut), narrow),
            pltpu.VMEM((steps, 2, capacity, rest), narrow),
            pltpu.VMEM((steps, 2, capacity, cut), narrow),
            pltpu.VMEM((steps, 2, capacity, rest), narrow),
            pltpu.VMEM((steps, 2, capacity, cut), narrow),
            pltpu.VMEM((steps, 2, capacity, rest), narrow),
            pltpu.VMEM((steps, 2, rows, LANES), narrow),
            pltpu.VMEM((steps, 2, rows, LANES), narrow),
            pltpu.VMEM((steps, capacity, cut), narrow),
            pltpu.VMEM((depth, 2, capacity, rest), narrow),
            pltpu.VMEM((depth, rows, cut), narrow),
            pltpu.VMEM((depth, rows, cut), narrow),
            pltpu.VMEM((rows, rest), narrow),
            pltpu.VMEM((rows, rest), narrow),
            pltpu.VMEM((depth, rows, cut), jnp.float32),
            pltpu.VMEM((2, rows, rest), jnp.float32),
            pltpu.VMEM((depth - 1, rows, cut), narrow),
            pltpu.VMEM((depth - 1, rows, cut), narrow),
            pltpu.VMEM((depth - 1, 2, rows, rest), narrow),
            pltpu.VMEM((depth - 1, 2, rows, rest), narrow),
            pltpu.VMEM((2, share, features), narrow),
            pltpu.VMEM((2, share, features), narrow),
            pltpu.VMEM((share, features), narrow),
            pltpu.VMEM((share, features), narrow),
            dma((2,)), dma((2,)), dma((2,)), dma((pieces,)), dma((pieces,)),
            dma((2,)), dma((2 * steps,)), dma((2 * steps,)), dma((steps,)), dma((steps,)),
            dma((depth,)), dma((depth,)), dma((depth,)), dma((depth,)), dma((1,)), dma((1,)),
            dma((depth - 1,)), dma((depth - 1,)), dma((depth - 1,)), dma((depth - 1,)),
        ],
        compiler_params=pltpu.CompilerParams(
            collective_id=0, has_side_effects=True, vmem_limit_bytes=63 * 1024 * 1024
        ),
        cost_estimate=pl.CostEstimate(
            flops=8 * work, bytes_accessed=4 * tokens.size, transcendentals=0
        ),
        name="experts",
    )(tokens, mix_part, gating_projection[0], expand_projection[0], shrink_projection[0])


def body(
    sequence_entry_features,
    sequence_exit_gating,
    memory_insert_clusters,
    memory_query_clusters,
    interval_presoftplus,
    entry_filter_taps,
    insert_filter_taps,
    query_filter_taps,
    interval_offset,
    head_fading_exponent,
    skip_connection_factor,
    spike_fading_exponent,
    cluster_scaling_vector,
    sequence_exit_projection,
    specialist_sample_slice,
    specialist_scaling_vector,
    chosen_specialists,
    dispatcher_affinity_matrix,
    gating_projection,
    expand_projection,
    shrink_projection,
):
    tok_rows, top_count = chosen_specialists.shape
    capacity = tok_rows * top_count * 5 // (4 * lax.axis_size("ep"))
    dense = dense_experts_fit(tok_rows, top_count, capacity, sequence_entry_features.shape[0])
    marked = None
    if dense:
        marked = marked_tokens(
            specialist_sample_slice,
            specialist_scaling_vector,
            chosen_specialists,
            dispatcher_affinity_matrix,
        )
    mix_part = mixer_half(
        sequence_entry_features,
        sequence_exit_gating,
        memory_insert_clusters,
        memory_query_clusters,
        interval_presoftplus,
        entry_filter_taps,
        insert_filter_taps,
        query_filter_taps,
        interval_offset,
        head_fading_exponent,
        skip_connection_factor,
        spike_fading_exponent,
        cluster_scaling_vector,
        sequence_exit_projection,
        marked,
    )
    if dense:
        mix_part, tokens = mix_part
        moe_out, mixed = experts_dense(
            tokens, mix_part, tok_rows, capacity, gating_projection, expand_projection, shrink_projection
        )
        return (mixed, moe_out)
    mixed = lax.psum_scatter(mix_part, "tp", scatter_dimension=0, tiled=True)
    moe_out = experts_half(
        specialist_sample_slice,
        specialist_scaling_vector,
        chosen_specialists,
        dispatcher_affinity_matrix,
        gating_projection,
        expand_projection,
        shrink_projection,
    )
    return (mixed, moe_out)


def solution(mesh):
    in_specs = (
        P("ep", "tp"),
        P("ep", "tp"),
        P("ep", "tp"),
        P("ep", "tp"),
        P("ep", "tp"),
        P(None, "tp"),
        P(None, "tp"),
        P(None, "tp"),
        P("tp"),
        P("tp"),
        P("tp"),
        P("ep", "tp"),
        P("tp"),
        P("tp", None),
        P(("ep", "tp"), None),
        P(),
        P(("ep", "tp"), None),
        P(("ep", "tp"), None),
        P("ep", None, "tp"),
        P("ep", None, "tp"),
        P("ep", "tp", None),
    )
    out_specs = (P(("ep", "tp"), None), P(("ep", "tp"), None))
    return jax.shard_map(body, mesh=mesh, in_specs=in_specs, out_specs=out_specs, check_vma=False)
```

```python
import functools
import jax
import jax.numpy as jnp
from jax import lax
from jax.experimental import pallas as pl
from jax.experimental.pallas import tpu as pltpu
from jax.sharding import PartitionSpec as P

HEAD = 64
STATE = 128
SPAN = 128
RIM = 8
LANES = 128
MIX_ROWS = 32
CUT_EIGHTHS = 5

norm_eps = 1e-05
clamp_top = 7.0
sigmoid_sharp = 1.702
highest = lax.Precision.HIGHEST


def passed_along(block, axis, distance):
    devices = range(lax.axis_size(axis))
    route = [(i - distance, i) for i in devices if i - distance in devices]
    return lax.ppermute(block, axis, route)


def conv_block(buf, first, value_ref, rim_ref, taps_ref):
    @pl.when(first)
    def _():
        buf[0:RIM, :] = rim_ref[...].astype(jnp.float32)

    @pl.when(jnp.logical_not(first))
    def _():
        buf[0:RIM, :] = buf[SPAN : SPAN + RIM, :]

    buf[RIM : RIM + SPAN, :] = value_ref[...].astype(jnp.float32)
    taps = taps_ref[...].astype(jnp.float32)
    count = taps.shape[0]
    total = buf[RIM : RIM + SPAN, :] * taps[count - 1 : count]
    for j in range(count - 1):
        start = RIM - (count - 1) + j
        total = total + buf[start : start + SPAN, :] * taps[j : j + 1]
    return total * jax.nn.sigmoid(total)


def conv_after(buf, first, value_ref, rim_ref, has_rim, taps_ref):
    @pl.when(first)
    def _():
        rim = rim_ref[...].astype(jnp.float32)[RIM:]
        buf[0:RIM, :] = jnp.where(has_rim, rim, 0.0)

    @pl.when(jnp.logical_not(first))
    def _():
        buf[0:RIM, :] = buf[SPAN : SPAN + RIM, :]

    buf[RIM : RIM + SPAN, :] = value_ref[...].astype(jnp.float32)
    taps = taps_ref[...].astype(jnp.float32)
    count = taps.shape[0]
    total = buf[RIM : RIM + SPAN, :] * taps[count - 1 : count]
    for j in range(count - 1):
        start = RIM - (count - 1) + j
        total = total + buf[start : start + SPAN, :] * taps[j : j + 1]
    return total * jax.nn.sigmoid(total)


def spread(cols, h, width):
    return jnp.broadcast_to(cols[:, h : h + 1], (SPAN, width))


def state_kernel(per_group, groups, x_ref, xr_ref, xt_ref, b_ref, br_ref, bt_ref, lw_ref, end_ref,
                 state_ref, xbuf, bbuf):
    first = pl.program_id(0) == 0
    x = conv_block(xbuf, first, x_ref, xr_ref, xt_ref)
    b = conv_block(bbuf, first, b_ref, br_ref, bt_ref)

    @pl.when(first)
    def _():
        state_ref[...] = jnp.zeros_like(state_ref)

    lw = lw_ref[...]
    low = lax.broadcasted_iota(jnp.int32, (SPAN, 2 * HEAD), 1) < HEAD
    for g in range(groups):
        bt = b[:, g * STATE : (g + 1) * STATE].T.astype(jnp.bfloat16)
        for pair in range(per_group // 2):
            h = g * per_group + 2 * pair
            cols = slice(h * HEAD, (h + 2) * HEAD)
            factor = jnp.exp(jnp.where(low, spread(lw, h, 2 * HEAD), spread(lw, h + 1, 2 * HEAD)))
            xw = (x[:, cols] * factor).astype(jnp.bfloat16)
            added = jnp.dot(bt, xw, preferred_element_type=jnp.float32)
            state_ref[:, cols] = state_ref[:, cols] * end_ref[0, :, cols] + added


def output_kernel(per_group, groups, x_ref, xr_ref, xt_ref, b_ref, br_ref, bt_ref, c_ref, cr_ref,
                  ct_ref, z_ref, lw_ref, cum_ref, row_ref, end_ref, enter_ref, skip_ref, scale_ref,
                  out_ref, xbuf, bbuf, cbuf, state, ybuf):
    first = pl.program_id(0) == 0
    x = conv_block(xbuf, first, x_ref, xr_ref, xt_ref)
    b = conv_block(bbuf, first, b_ref, br_ref, bt_ref)
    c = conv_block(cbuf, first, c_ref, cr_ref, ct_ref)

    @pl.when(first)
    def _():
        state[...] = enter_ref[...]

    lw = lw_ref[...]
    cum = cum_ref[...]
    low = lax.broadcasted_iota(jnp.int32, (SPAN, 2 * HEAD), 1) < HEAD
    causal = lax.broadcasted_iota(jnp.int32, (SPAN, SPAN), 0) >= lax.broadcasted_iota(
        jnp.int32, (SPAN, SPAN), 1
    )
    group_cols = per_group * HEAD
    for g in range(groups):
        bg = b[:, g * STATE : (g + 1) * STATE]
        bt = bg.T.astype(jnp.bfloat16)
        cg = c[:, g * STATE : (g + 1) * STATE].astype(jnp.bfloat16)
        scores = jnp.dot(cg, bt, preferred_element_type=jnp.float32)
        squares = jnp.zeros((SPAN, 2 * HEAD), jnp.float32)
        for pair in range(per_group // 2):
            h = g * per_group + 2 * pair
            cols = slice(h * HEAD, (h + 2) * HEAD)
            xp = x[:, cols]
            cum_0, cum_1 = spread(cum, h, SPAN), spread(cum, h + 1, SPAN)
            m_0 = scores * jnp.exp(jnp.where(causal, cum_0 + row_ref[0, h : h + 1, :], -jnp.inf))
            m_1 = scores * jnp.exp(jnp.where(causal, cum_1 + row_ref[0, h + 1 : h + 2, :], -jnp.inf))
            mixing = jnp.concatenate([m_0.astype(jnp.bfloat16), m_1.astype(jnp.bfloat16)], axis=1)
            x_0 = jnp.where(low, xp, 0.0).astype(jnp.bfloat16)
            x_1 = jnp.where(low, 0.0, xp).astype(jnp.bfloat16)
            y = jnp.dot(
                mixing, jnp.concatenate([x_0, x_1], axis=0), preferred_element_type=jnp.float32
            )
            before = state[:, cols]
            carried = jnp.dot(cg, before.astype(jnp.bfloat16), preferred_element_type=jnp.float32)
            y = y + carried * jnp.exp(jnp.where(low, cum_0, cum_1)) + xp * skip_ref[:, cols]
            factor = jnp.exp(jnp.where(low, spread(lw, h, 2 * HEAD), spread(lw, h + 1, 2 * HEAD)))
            xw = (xp * factor).astype(jnp.bfloat16)
            added = jnp.dot(bt, xw, preferred_element_type=jnp.float32)
            state[:, cols] = before * end_ref[0, :, cols] + added
            gate = z_ref[:, cols].astype(jnp.float32)
            gated = y * (gate * jax.nn.sigmoid(gate))
            squares = squares + gated * gated
            ybuf[:, cols] = gated
        mean = jnp.sum(squares, axis=1, keepdims=True) / group_cols
        inverse = lax.rsqrt(mean + norm_eps)
        cols = slice(g * group_cols, (g + 1) * group_cols)
        out_ref[:, cols] = (ybuf[:, cols] * inverse * scale_ref[:, cols]).astype(jnp.bfloat16)


def entering_state(own_state, own_decay):
    size, mine = (lax.axis_size("ep"), lax.axis_index("ep"))
    rows = own_state.shape[0]
    total = own_state
    decay = own_decay

    def joined():
        return jnp.concatenate(
            [total, jnp.broadcast_to(decay, (RIM, decay.shape[1]))], axis=0
        ).astype(jnp.bfloat16)

    distance = 1
    while distance < size:
        came = passed_along(joined(), "ep", distance)
        there = mine >= distance
        earlier = came[:rows].astype(jnp.float32)
        earlier_decay = jnp.where(there, came[rows : rows + 1].astype(jnp.float32), 1.0)
        total = earlier * decay + total
        decay = earlier_decay * decay
        distance *= 2
    return passed_along(total.astype(jnp.bfloat16), "ep", 1).astype(jnp.float32)


def mixer_half(
    sequence_entry_features,
    sequence_exit_gating,
    memory_insert_clusters,
    memory_query_clusters,
    interval_presoftplus,
    entry_filter_taps,
    insert_filter_taps,
    query_filter_taps,
    interval_offset,
    head_fading_exponent,
    skip_connection_factor,
    spike_fading_exponent,
    cluster_scaling_vector,
    sequence_exit_projection,
    marked,
):
    tok_rows = sequence_entry_features.shape[0]
    local_heads = interval_offset.shape[0]
    local_groups = memory_insert_clusters.shape[1] // STATE
    per_group = local_heads // local_groups
    if marked is not None:
        heads = jnp.stack([interval_offset, head_fading_exponent, skip_connection_factor], axis=1)
        return mixer_gather(
            per_group, local_groups, tok_rows // SPAN,
            (sequence_entry_features, memory_insert_clusters, memory_query_clusters),
            (entry_filter_taps, insert_filter_taps, query_filter_taps), sequence_exit_gating,
            interval_presoftplus.T, spike_fading_exponent.T,
            jnp.pad(heads, ((0, 0), (0, LANES - heads.shape[1]))), cluster_scaling_vector[None],
            sequence_exit_projection, marked,
        )
    inner_cols = sequence_entry_features.shape[1]
    state_cols = memory_insert_clusters.shape[1]
    last_rows = jnp.concatenate(
        [
            sequence_entry_features[tok_rows - RIM :],
            memory_insert_clusters[tok_rows - RIM :],
            memory_query_clusters[tok_rows - RIM :],
        ],
        axis=1,
    )
    rims = passed_along(last_rows, "ep", 1)
    rim_x = rims[:, :inner_cols]
    rim_b = rims[:, inner_cols : inner_cols + state_cols]
    rim_c = rims[:, inner_cols + state_cols :]
    blocks = tok_rows // SPAN
    interval = jax.nn.softplus(interval_presoftplus.astype(jnp.float32) + interval_offset)
    fading = spike_fading_exponent - jnp.exp(head_fading_exponent) * interval
    lower = jnp.tril(jnp.ones((SPAN, SPAN), jnp.float32))
    cumulative = jnp.einsum(
        "ts,csh->cth", lower, fading.reshape(blocks, SPAN, local_heads), precision=highest
    )
    log_step = jnp.log(interval).reshape(blocks, SPAN, local_heads)
    block_end = cumulative[:, -1:]
    key_log = (log_step - cumulative + block_end).reshape(tok_rows, local_heads)
    row_log = jnp.swapaxes(log_step - cumulative, 1, 2)
    end_factor = jnp.repeat(jnp.exp(block_end), HEAD, axis=2)
    own_decay = jnp.repeat(jnp.exp(jnp.sum(block_end, axis=0)), HEAD, axis=1)
    cumulative = cumulative.reshape(tok_rows, local_heads)

    def rows_of(width):
        return pl.BlockSpec((SPAN, width), lambda i: (i, 0))

    def fixed(shape):
        return pl.BlockSpec(shape, lambda i: (0, 0))

    def block_of(rows, width):
        return pl.BlockSpec((1, rows, width), lambda i: (i, 0, 0))

    def cost(dots):
        return pl.CostEstimate(
            flops=dots * tok_rows * inner_cols * STATE * 8,
            bytes_accessed=dots * tok_rows * inner_cols * 8,
            transcendentals=0,
        )

    taps = entry_filter_taps.shape[0]
    x_specs = [rows_of(inner_cols), fixed((RIM, inner_cols)), fixed((taps, inner_cols))]
    s_specs = [rows_of(state_cols), fixed((RIM, state_cols)), fixed((taps, state_cols))]
    x_args = (sequence_entry_features, rim_x, entry_filter_taps)
    b_args = (memory_insert_clusters, rim_b, insert_filter_taps)
    c_args = (memory_query_clusters, rim_c, query_filter_taps)
    own_state = pl.pallas_call(
        functools.partial(state_kernel, per_group, local_groups),
        grid=(blocks,),
        in_specs=x_specs + s_specs + [rows_of(local_heads), block_of(1, inner_cols)],
        out_specs=fixed((STATE, inner_cols)),
        out_shape=jax.ShapeDtypeStruct((STATE, inner_cols), jnp.float32),
        scratch_shapes=[
            pltpu.VMEM((SPAN + RIM, inner_cols), jnp.float32),
            pltpu.VMEM((SPAN + RIM, state_cols), jnp.float32),
        ],
        cost_estimate=cost(1),
        name="own_state",
    )(*x_args, *b_args, key_log, end_factor)
    entering = entering_state(own_state, own_decay)
    normed = pl.pallas_call(
        functools.partial(output_kernel, per_group, local_groups),
        grid=(blocks,),
        in_specs=x_specs + s_specs + s_specs + [
            rows_of(inner_cols),
            rows_of(local_heads),
            rows_of(local_heads),
            block_of(local_heads, SPAN),
            block_of(1, inner_cols),
            fixed((STATE, inner_cols)),
            fixed((1, inner_cols)),
            fixed((1, inner_cols)),
        ],
        out_specs=rows_of(inner_cols),
        out_shape=jax.ShapeDtypeStruct((tok_rows, inner_cols), jnp.bfloat16),
        scratch_shapes=[
            pltpu.VMEM((SPAN + RIM, inner_cols), jnp.float32),
            pltpu.VMEM((SPAN + RIM, state_cols), jnp.float32),
            pltpu.VMEM((SPAN + RIM, state_cols), jnp.float32),
            pltpu.VMEM((STATE, inner_cols), jnp.float32),
            pltpu.VMEM((SPAN, inner_cols), jnp.float32),
        ],
        cost_estimate=cost(3),
        name="mixer_output",
    )(
        *x_args, *b_args, *c_args, sequence_exit_gating, key_log, cumulative, row_log, end_factor,
        entering, jnp.repeat(skip_connection_factor, HEAD)[None], cluster_scaling_vector[None],
    )
    return jnp.dot(normed, sequence_exit_projection, preferred_element_type=jnp.float32).astype(
        jnp.bfloat16
    )


def mixer_gather(
    per_group, groups, blocks, streams, filters, gating, raw, spikes, heads, scale,
    exit_projection, marked,
):
    tok_rows, inner_cols = gating.shape
    state_cols = streams[1].shape[1]
    head_count = raw.shape[0]
    features = exit_projection.shape[1]
    rows, marked_cols = marked.shape
    taps = filters[0].shape[0]
    devices = lax.axis_size("ep") * lax.axis_size("tp")
    depth = lax.axis_size("ep") // 2
    narrow, wide = jnp.bfloat16, inner_cols // 2
    pieces = 7 * depth

    def either(i):
        return jnp.where(i < blocks, i, jnp.maximum(i - blocks - 1, 0))

    def late(i):
        return jnp.maximum(i - blocks - 1, 0)

    def by_rows(width, at):
        return pl.BlockSpec((SPAN, width), lambda i: (at(i), 0))

    def fixed(shape):
        return pl.BlockSpec(shape, lambda i: (0, 0))

    def conv_specs(width, at):
        return [by_rows(width, at), fixed((taps, width))]

    dma = pltpu.SemaphoreType.DMA
    hops = [dma((depth,)) for _ in range(12)]
    return pl.pallas_call(
        functools.partial(mixer_gather_kernel, per_group, groups, blocks, depth),
        grid=(2 * blocks + 1,),
        in_specs=conv_specs(inner_cols, either)
        + conv_specs(state_cols, either)
        + conv_specs(state_cols, late)
        + [
            by_rows(inner_cols, late),
            fixed((head_count, tok_rows)),
            fixed((head_count, tok_rows)),
            fixed((head_count, LANES)),
            fixed((1, inner_cols)),
            fixed((inner_cols, features)),
            fixed((rows, marked_cols)),
        ]
        + [pl.BlockSpec(memory_space=pl.ANY)] * 3,
        out_specs=[by_rows(features, late), pl.BlockSpec(memory_space=pl.ANY)],
        out_shape=[
            jax.ShapeDtypeStruct((tok_rows, features), narrow),
            jax.ShapeDtypeStruct((devices * rows, marked_cols), narrow),
        ],
        scratch_shapes=[
            pltpu.VMEM((blocks, SPAN, head_count), jnp.float32),
            pltpu.VMEM((blocks, SPAN, head_count), jnp.float32),
            pltpu.VMEM((blocks, head_count, SPAN), jnp.float32),
            pltpu.VMEM((blocks, 1, head_count), jnp.float32),
            pltpu.VMEM((1, head_count), jnp.float32),
            pltpu.VMEM((1, head_count), jnp.float32),
            pltpu.VMEM((1, inner_cols), jnp.float32),
            pltpu.VMEM((2 * RIM, inner_cols), narrow),
            pltpu.VMEM((2 * RIM, state_cols), narrow),
            pltpu.VMEM((2 * RIM, state_cols), narrow),
            dma((3,)), dma((3,)),
            pltpu.VMEM((SPAN + RIM, inner_cols), jnp.float32),
            pltpu.VMEM((SPAN + RIM, state_cols), jnp.float32),
            pltpu.VMEM((SPAN + RIM, state_cols), jnp.float32),
            pltpu.VMEM((STATE, inner_cols), jnp.float32),
            pltpu.VMEM((SPAN, inner_cols), jnp.float32),
            pltpu.VMEM((SPAN, inner_cols), narrow),
            pltpu.VMEM((STATE + 2 * RIM, inner_cols), narrow),
            pltpu.VMEM((STATE + 2 * RIM, inner_cols), narrow),
            pltpu.VMEM((STATE + 2 * RIM, wide), narrow),
            pltpu.VMEM((depth - 1, STATE + 2 * RIM, wide), narrow),
            pltpu.VMEM((STATE, wide), jnp.float32),
            pltpu.VMEM((STATE, wide), narrow),
            pltpu.VMEM((STATE, wide), narrow),
            dma((1,)), dma((depth - 1,)), dma((depth - 1,)),
            *hops,
            dma((pieces,)), dma((pieces,)), dma((1,)), dma((1,)), dma((depth - 1,)),
            dma((depth - 1,)), dma((1,)), dma((1,)),
        ],
        compiler_params=pltpu.CompilerParams(
            collective_id=1, has_side_effects=True, vmem_limit_bytes=56 * 1024 * 1024,
            dimension_semantics=("arbitrary",),
        ),
        cost_estimate=pl.CostEstimate(
            flops=tok_rows * inner_cols * (features * 2 + STATE * 16),
            bytes_accessed=tok_rows * inner_cols * 16,
            transcendentals=0,
        ),
        name="mixer_gather",
    )(
        streams[0], filters[0], streams[1], filters[1], streams[2], filters[2], gating, raw, spikes,
        heads, scale, exit_projection, marked, *streams,
    )


def experts_half(
    specialist_sample_slice,
    specialist_scaling_vector,
    chosen_specialists,
    dispatcher_affinity_matrix,
    gating_projection,
    expand_projection,
    shrink_projection,
):
    tok_rows = specialist_sample_slice.shape[0]
    feature_count = specialist_sample_slice.shape[1]
    top_count = chosen_specialists.shape[1]
    experts = lax.axis_size("ep")
    groups_tp = lax.axis_size("tp")
    capacity = tok_rows * top_count * 5 // (4 * experts)
    as_float = specialist_sample_slice.astype(jnp.float32)
    centred = as_float - jnp.mean(as_float, axis=1, keepdims=True)
    normed = (
        centred
        * lax.rsqrt(jnp.mean(centred * centred, axis=1, keepdims=True) + norm_eps)
        * specialist_scaling_vector
    ).astype(jnp.bfloat16)
    route_weight = jnp.exp(dispatcher_affinity_matrix) / jnp.sum(
        jnp.exp(dispatcher_affinity_matrix), axis=1, keepdims=True
    )
    flat_routes = chosen_specialists.reshape(-1)
    onehot = (flat_routes[:, None] == jnp.arange(experts, dtype=jnp.int32)[None, :]).astype(
        jnp.int32
    )
    position = jnp.sum(onehot * (jnp.cumsum(onehot, axis=0) - 1), axis=1)
    target = flat_routes * capacity + position
    token_ids = jnp.arange(tok_rows * top_count, dtype=jnp.int32) // top_count
    source_table = jnp.full((experts * capacity,), tok_rows, jnp.int32).at[target].set(token_ids)
    padded = jnp.concatenate([normed, jnp.zeros((1, feature_count), jnp.bfloat16)], axis=0)
    outgoing = padded[source_table].reshape(experts, capacity, feature_count)
    arrived = lax.all_to_all(outgoing, "ep", split_axis=0, concat_axis=0, tiled=True)
    shard_rows = lax.all_gather(arrived, "tp", axis=0, tiled=True)
    rows_in = shard_rows.reshape(-1, feature_count)
    gate_h = jnp.dot(rows_in, gating_projection[0], preferred_element_type=jnp.float32)
    up_h = jnp.dot(rows_in, expand_projection[0], preferred_element_type=jnp.float32)
    clipped = jnp.minimum(gate_h, clamp_top)
    hidden_act = (
        (
            clipped
            * jax.nn.sigmoid(sigmoid_sharp * clipped)
            * (jnp.clip(up_h, -clamp_top, clamp_top) + 1.0)
        )
        .astype(jnp.bfloat16)
        .reshape(shard_rows.shape[0], capacity, -1)
    )
    hidden_act = hidden_act.reshape(groups_tp * experts * capacity, -1)
    summed = lax.psum_scatter(
        jnp.dot(hidden_act, shrink_projection[0], preferred_element_type=jnp.float32).astype(
            jnp.bfloat16
        ),
        "tp",
        scatter_dimension=0,
        tiled=True,
    )
    returned = lax.all_to_all(
        summed.reshape(experts, capacity, feature_count),
        "ep",
        split_axis=0,
        concat_axis=0,
        tiled=True,
    )
    slot_out = returned.reshape(experts * capacity, feature_count)[target].reshape(
        tok_rows, top_count, feature_count
    )
    combined = jnp.einsum("tk,tkd->td", route_weight, slot_out.astype(jnp.float32))
    return combined.astype(jnp.bfloat16)


def routing_kernel(experts, x_ref, scale_ref, chosen_ref, score_ref, out_ref, turned):
    features = x_ref.shape[1]
    top_count, rows = chosen_ref.shape
    value = x_ref[...].astype(jnp.float32)
    centred = value - jnp.mean(value, axis=1, keepdims=True)
    spread_of = jnp.mean(centred * centred, axis=1, keepdims=True)
    normed = centred * lax.rsqrt(spread_of + norm_eps) * scale_ref[...]
    out_ref[:, :features] = normed.astype(jnp.bfloat16)
    raised = jnp.exp(score_ref[...])
    turned[...] = jnp.zeros_like(turned)
    turned[0:top_count, :] = chosen_ref[...].astype(jnp.float32)
    turned[8 : 8 + top_count, :] = raised / jnp.sum(raised, axis=0, keepdims=True)
    columns = turned[...].T
    lane = lax.broadcasted_iota(jnp.int32, (rows, LANES), 1)
    named = lax.rem(lane, experts).astype(jnp.float32)
    held = jnp.zeros((rows, LANES), jnp.float32)
    share = jnp.zeros((rows, LANES), jnp.float32)
    for k in range(top_count):
        same = columns[:, k : k + 1] == named
        held = held + jnp.where(same, 1.0, 0.0)
        share = share + jnp.where(same, columns[:, 8 + k : 9 + k], 0.0)
    earlier = lax.broadcasted_iota(jnp.int32, (rows, rows), 0) > lax.broadcasted_iota(
        jnp.int32, (rows, rows), 1
    )
    place = jnp.dot(
        jnp.where(earlier, 1.0, 0.0).astype(jnp.bfloat16),
        held.astype(jnp.bfloat16),
        preferred_element_type=jnp.float32,
    )
    place = jnp.where(held > 0.0, place, 255.0)
    coarse = share.astype(jnp.bfloat16).astype(jnp.float32)
    table = jnp.where(lane < experts, place, jnp.where(lane < 2 * experts, coarse, share - coarse))
    out_ref[:, features:] = table.astype(jnp.bfloat16)


def experts_kernel(
    experts, capacity, tokens_ref, mix_ref, gate_ref, up_ref, down_ref, out_ref, mixed_ref,
    tokens, slots, own_a, own_b, outgoing_a, outgoing_b, incoming_a, incoming_b, place, place_next,
    from_x, from_y, to_y, came_y, to_x, came_x, keep_a, keep_b, to_za, from_za, to_zb, from_zb,
    mix_own, mix_core, mix_out, mix_in, mix_sem, mc_send, mc_recv, mx_send, mx_recv,
    token_sem, core_send, core_recv, x_send, x_recv, y_send, y_recv,
    a_send, a_recv, b_send, b_recv, za_send, za_recv, zb_send, zb_recv,
):
    depth = experts // 2
    steps = experts
    ep, tp = lax.axis_index("ep"), lax.axis_index("tp")
    z, y, x, core = ep // 2, ep % 2, tp // 2, tp % 2
    next_ep = z * 2 + 1 - y
    sibling = {"tp": x * 2 + 1 - core}
    x_next = {"tp": (1 - x) * 2 + core}
    y_next = {"ep": next_ep}
    rows = out_ref.shape[0]
    features = out_ref.shape[1]
    cut = own_a.shape[3]
    own, outgoing, incoming = (own_a, own_b), (outgoing_a, outgoing_b), (incoming_a, incoming_b)
    mesh_id = pl.DeviceIdType.MESH

    def z_next(k):
        return {"ep": ((z + k) % depth) * 2 + y}

    def turn(i):
        middle = depth // 2
        others = jnp.where(i == 0, middle, jnp.where(i < middle, i, i + 1))
        return jnp.where(i == depth - 1, 0, others)

    def fetch(s):
        k, dy = turn(s // 2), 1 - s % 2
        block = ((z + k) % depth) * 2 + (y + dy) % 2
        span = 4 * rows
        return pltpu.make_async_copy(
            tokens_ref.at[pl.ds(pl.multiple_of(block * span, span), span)],
            tokens.at[s % 2],
            token_sem.at[s % 2],
        )

    def remote(source, target, send, recv, device):
        return pltpu.make_async_remote_copy(
            src_ref=source, dst_ref=target, send_sem=send, recv_sem=recv,
            device_id=device, device_id_type=mesh_id,
        )

    def core_copy(s, side):
        send, recv = core_send.at[2 * s + side], core_recv.at[2 * s + side]
        return remote(outgoing[side].at[s], incoming[side].at[s], send, recv, sibling)

    def x_copy(s):
        return remote(own_a.at[s, 1], from_x.at[s], x_send.at[s], x_recv.at[s], x_next)

    def y_copy(i):
        return remote(own_b.at[2 * i], from_y.at[i], y_send.at[i], y_recv.at[i], y_next)

    def a_copy(i):
        return remote(to_y.at[i], came_y.at[i], a_send.at[i], a_recv.at[i], y_next)

    def b_copy():
        return remote(to_x, came_x, b_send.at[0], b_recv.at[0], x_next)

    def za_copy(i):
        return remote(to_za.at[i], from_za.at[i], za_send.at[i], za_recv.at[i], z_next(turn(i)))

    def zb_copy(i):
        return remote(to_zb.at[i], from_zb.at[i], zb_send.at[i], zb_recv.at[i], z_next(turn(i)))

    chunks, piece = mixed_ref.shape[0] // MIX_ROWS, MIX_ROWS
    share = mixed_ref.shape[0]

    early, late = chunks // 4, chunks // 2

    def mix_part(n, c):
        dx, start, stop = ((0, 0, share), (1, early * piece, share), (1, 0, early * piece))[n]
        block = ((x + dx) % 2) * 2 + c
        rows_n = pl.ds(pl.multiple_of(block * share + start, piece), stop - start)
        return dx, pl.ds(start, stop - start), mix_ref.at[rows_n]

    def mix_fetch(n):
        dx, there, source = mix_part(n, core)
        return pltpu.make_async_copy(source, mix_own.at[dx, there], mix_sem.at[n])

    def mix_core_copy(n):
        dx, there, source = mix_part(n, 1 - core)
        return remote(source, mix_core.at[dx, there], mc_send.at[n], mc_recv.at[n], sibling)

    def mix_x_copy(j):
        rows_j = pl.ds(pl.multiple_of(j * piece, piece), piece)
        return remote(
            mix_out.at[rows_j], mix_in.at[rows_j], mx_send.at[j], mx_recv.at[j], x_next
        )

    def mix_away(j, carry):
        rows_j = pl.ds(pl.multiple_of(j * piece, piece), piece)
        mix_out[rows_j, :] = (
            mix_own[1, rows_j, :].astype(jnp.float32) + mix_core[1, rows_j, :].astype(jnp.float32)
        ).astype(jnp.bfloat16)
        return carry

    def mix_home(j, carry):
        rows_j = pl.ds(pl.multiple_of(j * piece, piece), piece)
        mix_own[0, rows_j, :] = (
            mix_own[0, rows_j, :].astype(jnp.float32) + mix_core[0, rows_j, :].astype(jnp.float32)
        ).astype(jnp.bfloat16)
        return carry

    def mix_send(j, carry):
        mix_x_copy(j).start()
        return carry

    def mix_finish(j, carry):
        rows_j = pl.ds(pl.multiple_of(j * piece, piece), piece)
        mix_x_copy(j).wait_recv()
        mixed_ref[rows_j, :] = (
            mix_own[0, rows_j, :].astype(jnp.float32) + mix_in[rows_j, :].astype(jnp.float32)
        ).astype(jnp.bfloat16)
        return carry

    def mix_sent(j, carry):
        mix_x_copy(j).wait_send()
        return carry

    fetch(0).start()
    for n in (2, 1, 0):
        mix_fetch(n).start()
    barrier = pltpu.get_barrier_semaphore()
    partners = [sibling, x_next, y_next] + [z_next(k) for k in range(1, depth)]
    for partner in partners:
        pl.semaphore_signal(barrier, inc=1, device_id=partner, device_id_type=mesh_id)
    pl.semaphore_wait(barrier, len(partners))

    for n in (2, 1, 0):
        mix_core_copy(n).start()

    lane = lax.broadcasted_iota(jnp.int32, (rows, LANES), 1)
    lane_value = lane.astype(jnp.float32)
    slot_lane = lax.broadcasted_iota(jnp.int32, (capacity, LANES), 1)

    def chosen_slots(table, expert):
        column = jnp.sum(jnp.where(lane == expert, table, 0.0), axis=1, keepdims=True)
        return jnp.where(column == lane_value, 1.0, 0.0)

    def compute(s):
        weights = []
        for dx in (0, 1):
            for q in (0, 1):
                c = core if q == 0 else 1 - core
                block = ((x + dx) % 2) * 2 + c
                start = pl.multiple_of(block * rows, rows)
                arrived = tokens[s % 2, pl.ds(start, rows), :]
                table = arrived[:, features:].astype(jnp.float32)
                picked = chosen_slots(table, ep)
                if q == 0:
                    place[s, dx] = picked.astype(jnp.bfloat16)
                    place_next[s, dx] = chosen_slots(table, next_ep).astype(jnp.bfloat16)
                select = picked.T[:capacity].astype(jnp.bfloat16)
                taken = jnp.dot(select, arrived, preferred_element_type=jnp.float32)
                first = (dx * 2 + q) * capacity
                slots[first : first + capacity, :] = taken[:, :features].astype(jnp.bfloat16)
                mine = (slot_lane == experts + ep) | (slot_lane == 2 * experts + ep)
                weights.append(
                    jnp.sum(jnp.where(mine, taken[:, features:], 0.0), axis=1, keepdims=True)
                )
        value = slots[...]
        gate_h = jnp.dot(value, gate_ref[...], preferred_element_type=jnp.float32)
        up_h = jnp.dot(value, up_ref[...], preferred_element_type=jnp.float32)
        clipped = jnp.minimum(gate_h, clamp_top)
        act = (
            clipped
            * jax.nn.sigmoid(sigmoid_sharp * clipped)
            * (jnp.clip(up_h, -clamp_top, clamp_top) + 1.0)
        ).astype(jnp.bfloat16)
        for side in (0, 1):
            columns = slice(0, cut) if side == 0 else slice(cut, features)
            part = jnp.dot(act, down_ref[:, columns], preferred_element_type=jnp.float32)
            for dx in (0, 1):
                for q in (0, 1):
                    first = (dx * 2 + q) * capacity
                    scaled = (part[first : first + capacity] * weights[dx * 2 + q]).astype(
                        jnp.bfloat16
                    )
                    if q == 0:
                        own[side][s, dx] = scaled
                    else:
                        outgoing[side][s, dx] = scaled

    def spread_out(where, value):
        return jnp.dot(where[:, :capacity], value, preferred_element_type=jnp.float32)

    last_x = 2 * depth + 2
    mix_fetch(2).wait()
    mix_core_copy(2).wait_recv()
    lax.fori_loop(0, early, mix_away, 0)
    lax.fori_loop(0, early, mix_send, 0)

    def step(s, carry):
        @pl.when(s < steps)
        def _():
            @pl.when(s + 1 < steps)
            def _():
                fetch(s + 1).start()

            fetch(s).wait()
            compute(s)

        @pl.when((s >= 1) & (s <= steps))
        def _():
            t = s - 1
            for side in (0, 1):
                core_copy(t, side).wait_recv()
                for dx in (0, 1):
                    own[side][t, dx] = (
                        own[side][t, dx].astype(jnp.float32)
                        + incoming[side][t, dx].astype(jnp.float32)
                    ).astype(jnp.bfloat16)

        @pl.when(s < steps)
        def _():
            for side in (0, 1):
                core_copy(s, side).start()

        @pl.when(s == 1)
        def _():
            for n in (1, 0):
                mix_fetch(n).wait()
                mix_core_copy(n).wait_recv()
            lax.fori_loop(early, chunks, mix_away, 0)
            lax.fori_loop(0, chunks, mix_home, 0)

        i = (s - 4) // 2

        @pl.when((s >= 4) & (s % 2 == 0) & (i < depth))
        def _():
            far, near = 2 * i, 2 * i + 1
            y_copy(i).wait_recv()
            for dx in (0, 1):
                sum_b = spread_out(place[near, dx], own_b[near, dx]) + spread_out(
                    place_next[near, dx], from_y[i, dx]
                )

                @pl.when(i < depth - 1)
                def _():
                    to_zb[i, dx] = sum_b.astype(jnp.bfloat16)

                @pl.when(i == depth - 1)
                def _():
                    keep_b[dx] = sum_b

            x_copy(far).wait_recv()
            where = place[far, 0]
            to_y[i] = (spread_out(where, own_a[far, 0]) + spread_out(where, from_x[far])).astype(
                jnp.bfloat16
            )

            @pl.when(i < depth - 1)
            def _():
                zb_copy(i).start()

            x_copy(near).wait_recv()
            where = place[near, 0]
            keep_a[i] = spread_out(where, own_a[near, 0]) + spread_out(where, from_x[near])
            a_copy(i).start()

        @pl.when((s >= 1) & (s <= steps))
        def _():
            t = s - 1
            x_copy(t).start()

            @pl.when(t % 2 == 0)
            def _():
                y_copy(t // 2).start()

        start = jnp.where(s == last_x, late, jnp.clip(early + s - 3, early, late))
        stop = jnp.where(
            s == last_x, chunks, jnp.where(s > last_x, 0, jnp.clip(early + s - 2, early, late))
        )
        lax.fori_loop(start, stop, mix_send, 0)

        j = (s - 6) // 2

        @pl.when((s >= 6) & (s % 2 == 0) & (j < depth))
        def _():
            a_copy(j).wait_recv()
            sum_a = keep_a[j] + came_y[j].astype(jnp.float32)

            @pl.when(j < depth - 1)
            def _():
                to_za[j] = sum_a.astype(jnp.bfloat16)
                za_copy(j).start()

            @pl.when(j == depth - 1)
            def _():
                keep_a[j] = sum_a

        return carry

    lax.fori_loop(0, 2 * depth + 5, step, 0)
    for i in range(depth - 1):
        zb_copy(i).wait_recv()
    total = [keep_b[0], keep_b[1]]
    for i in range(depth - 1):
        total = [total[dx] + from_zb[i, dx].astype(jnp.float32) for dx in (0, 1)]
    to_x[...] = total[1].astype(jnp.bfloat16)
    keep_b[0] = total[0]
    total = keep_a[depth - 1]
    for i in range(depth - 1):
        za_copy(i).wait_recv()
        total = total + from_za[i].astype(jnp.float32)
    out_ref[:, :cut] = total.astype(jnp.bfloat16)
    b_copy().start()
    lax.fori_loop(0, chunks, mix_finish, 0)
    lax.fori_loop(0, chunks, mix_sent, 0)
    b_copy().wait_recv()
    out_ref[:, cut:] = (keep_b[0] + came_x[...].astype(jnp.float32)).astype(jnp.bfloat16)
    for n in range(3):
        mix_core_copy(n).wait_send()
    for s in range(steps):
        for side in (0, 1):
            core_copy(s, side).wait_send()
        x_copy(s).wait_send()
    for i in range(depth):
        y_copy(i).wait_send()
        a_copy(i).wait_send()
    b_copy().wait_send()
    for i in range(depth - 1):
        za_copy(i).wait_send()
        zb_copy(i).wait_send()


def mixer_gather_kernel(
    per_group, groups, blocks, depth,
    x_ref, xt_ref, b_ref, bt_ref, c_ref, ct_ref, z_ref, pre_ref, spike_ref, head_ref, scale_ref,
    exit_ref, marked_ref, x_all, b_all, c_all,
    part_ref, tokens_ref,
    lw_of, cum_of, row_of, end_of, skip_of, decay_of, decay_row, xr_ref, br_ref, cr_ref, rim_s,
    rim_r, xbuf, bbuf, cbuf, state, ybuf, nbuf, pair_out, pair_in, line_out, line_in, line_sum, swap_out,
    swap_in, local_sem, z_send, z_recv, xa_s, xa_r, xb_s, xb_r, xf_s, xf_r, ya_s, ya_r, yb_s, yb_r,
    yf_s, yf_r, d_s, d_r, pair_s, pair_r, line_s, line_r, swap_s, swap_r,
):
    step = pl.program_id(0)
    ep, tp = lax.axis_index("ep"), lax.axis_index("tp")
    z, y, x, core = ep // 2, ep % 2, tp // 2, tp % 2
    sibling = {"tp": x * 2 + 1 - core}
    x_next = {"tp": (1 - x) * 2 + core}
    y_next = {"ep": z * 2 + 1 - y}
    mesh_id = pl.DeviceIdType.MESH
    rows = marked_ref.shape[0]
    first_rows = rows * 3 // 8
    inner = state.shape[1]
    wide = inner // 2

    def z_next(k):
        return {"ep": ((z + k) % depth) * 2 + y}

    def remote(source, target, send, recv, device):
        return pltpu.make_async_remote_copy(
            src_ref=source, dst_ref=target, send_sem=send, recv_sem=recv,
            device_id=device, device_id_type=mesh_id,
        )

    def region(dx, dy, k, half, c=core):
        block = (((z + depth - k) % depth) * 2 + (y + dy) % 2) * 4 + ((x + dx) % 2) * 2 + c
        offset, size = ((0, rows), (0, first_rows), (first_rows, rows - first_rows))[
            0 if half is None else 1 + half
        ]
        return tokens_ref.at[pl.ds(pl.multiple_of(block * rows + offset, 16), size)]

    def source(dx, dy, k, half):
        if (dx, dy, k) == (0, 0, 0):
            if half is None:
                return marked_ref
            if half == 0:
                return marked_ref.at[pl.ds(0, first_rows)]
            return marked_ref.at[pl.ds(first_rows, rows - first_rows)]
        return region(dx, dy, k, half)

    def z_copy(k):
        return remote(
            marked_ref, region(0, 0, 0, None), z_send.at[k - 1], z_recv.at[k - 1], z_next(k)
        )

    def z_came(k):
        here = region(0, 0, k, None)
        return remote(here, here, z_send.at[k - 1], z_recv.at[k - 1], z_next(k))

    moves = {
        "xa": ((0, 0, 0), (1, 0, 0), xa_s, xa_r, x_next),
        "xb": ((0, 0, 1), (1, 0, 1), xb_s, xb_r, x_next),
        "xf": ((0, 1, 1), (1, 1, 1), xf_s, xf_r, x_next),
        "yb": ((0, 0, 1), (0, 1, 1), yb_s, yb_r, y_next),
        "ya": ((0, 0, 0), (0, 1, 0), ya_s, ya_r, y_next),
        "yf": ((1, 0, 0), (1, 1, 0), yf_s, yf_r, y_next),
    }

    def sent(name, k):
        (dx, dy, half), _, send, recv, device = moves[name]
        return remote(
            source(dx, dy, k, half), region(dx, dy, k, half), send.at[k], recv.at[k], device
        )

    def came(name, k):
        _, (dx, dy, half), send, recv, device = moves[name]
        here = region(dx, dy, k, half)
        return remote(here, here, send.at[k], recv.at[k], device)

    shared = [(0, 0, None), (1, 0, 0), (1, 0, 1), (0, 1, 1), (0, 1, 0), (1, 1, 0), (1, 1, 1)]

    def d_sent(k, n):
        dx, dy, half = shared[n]
        m = len(shared) * k + n
        return remote(
            source(dx, dy, k, half), region(dx, dy, k, half), d_s.at[m], d_r.at[m], sibling
        )

    def d_came(k, n):
        dx, dy, half = shared[n]
        m = len(shared) * k + n
        here = region(dx, dy, k, half, 1 - core)
        return remote(here, here, d_s.at[m], d_r.at[m], sibling)

    def first_hop(k):
        if k > 0:
            z_came(k).wait_recv()
        for name in ("xa", "yb", "xb", "ya"):
            sent(name, k).start()
        d_sent(k, 0).start()

    def second_hop(k):
        came("xa", k).wait_recv()
        sent("yf", k).start()
        d_sent(k, 1).start()
        came("yb", k).wait_recv()
        sent("xf", k).start()
        d_sent(k, 3).start()

    def last_hop(k, parts=(("xb", 2), ("ya", 4), ("yf", 5), ("xf", 6))):
        for name, n in parts:
            came(name, k).wait_recv()
            d_sent(k, n).start()

    devices = 2 * depth
    after, before = {"ep": (ep + 1) % devices}, {"ep": (ep + devices - 1) % devices}
    last_rows = pl.ds(x_all.shape[0] - 2 * RIM, 2 * RIM)

    def rim_copy(n):
        whole, rim = ((x_all, xr_ref), (b_all, br_ref), (c_all, cr_ref))[n]
        return remote(whole.at[last_rows], rim, rim_s.at[n], rim_r.at[n], after)

    def own_copy():
        return pltpu.make_async_copy(marked_ref, region(0, 0, 0, None), local_sem.at[0])

    @pl.when(step == 0)
    def _():
        barrier = pltpu.get_barrier_semaphore()
        partners = [sibling, x_next, y_next, after, before]
        partners = partners + [z_next(k) for k in range(1, depth)]
        for partner in partners:
            pl.semaphore_signal(barrier, inc=1, device_id=partner, device_id_type=mesh_id)
        pl.semaphore_wait(barrier, len(partners))
        for n in range(3):
            rim_copy(n).start()
        z_copy(1).start()
        first_hop(0)
        for k in range(2, depth - 1):
            z_copy(k).start()
        own_copy().start()
        turned = head_ref[...].T
        skip_of[...] = turned[2:3]
        heads = head_ref.shape[0]

        def stacked(piece):
            return jnp.concatenate([piece(n) for n in range(blocks)], axis=0)

        def tall(column):
            return stacked(lambda n: jnp.broadcast_to(column, (heads, SPAN)))

        raw = stacked(lambda n: pre_ref[:, n * SPAN : (n + 1) * SPAN].astype(jnp.float32))
        raw = raw + tall(head_ref[:, 0:1])
        interval = jnp.maximum(raw, 0.0) + jnp.log1p(jnp.exp(-jnp.abs(raw)))
        spikes = stacked(lambda n: spike_ref[:, n * SPAN : (n + 1) * SPAN])
        fading = spikes - tall(jnp.exp(head_ref[:, 1:2])) * interval
        upto = lax.broadcasted_iota(jnp.int32, (SPAN, SPAN), 0) <= lax.broadcasted_iota(
            jnp.int32, (SPAN, SPAN), 1
        )
        cumulative = jnp.dot(
            fading, jnp.where(upto, 1.0, 0.0), precision=highest, preferred_element_type=jnp.float32
        )
        row_log = jnp.log(interval) - cumulative
        key_log = row_log + cumulative[:, SPAN - 1 :]
        decay = jnp.ones((1, heads), jnp.float32)
        for n in range(blocks):
            rows_n = slice(n * heads, (n + 1) * heads)
            cum = cumulative[rows_n].T
            end = jnp.exp(cum[SPAN - 1 :])
            row_of[n] = row_log[rows_n]
            lw_of[n] = key_log[rows_n].T
            cum_of[n] = cum
            end_of[n] = end
            decay = decay * end
        decay_of[...] = decay
        for n in range(3):
            rim_copy(n).wait_recv()

    def per_head(row, h):
        first_head = jnp.broadcast_to(row[:, h : h + 1], (1, 2 * HEAD))
        second_head = jnp.broadcast_to(row[:, h + 1 : h + 2], (1, 2 * HEAD))
        return jnp.where(low[0:1], first_head, second_head)

    has_rim = ep > 0
    low = lax.broadcasted_iota(jnp.int32, (SPAN, 2 * HEAD), 1) < HEAD
    state_pass = step < blocks
    output_pass = step > blocks

    @pl.when(state_pass)
    def _():
        first = step == 0
        xv = conv_after(xbuf, first, x_ref, xr_ref, has_rim, xt_ref)
        bv = conv_after(bbuf, first, b_ref, br_ref, has_rim, bt_ref)

        @pl.when(first)
        def _():
            state[...] = jnp.zeros_like(state)

        lw = lw_of[step]
        end = end_of[step]
        for g in range(groups):
            bt = bv[:, g * STATE : (g + 1) * STATE].T.astype(jnp.bfloat16)
            for pair in range(per_group // 2):
                h = g * per_group + 2 * pair
                cols = slice(h * HEAD, (h + 2) * HEAD)
                factor = jnp.exp(
                    jnp.where(low, spread(lw, h, 2 * HEAD), spread(lw, h + 1, 2 * HEAD))
                )
                xw = (xv[:, cols] * factor).astype(jnp.bfloat16)
                added = jnp.dot(bt, xw, preferred_element_type=jnp.float32)
                state[:, cols] = state[:, cols] * per_head(end, h) + added

    @pl.when(step == blocks // 2)
    def _():
        second_hop(0)

    @pl.when(step == blocks)
    def _():
        pair = remote(pair_out, pair_in, pair_s.at[0], pair_r.at[0], y_next)
        swap = remote(swap_out, swap_in, swap_s.at[0], swap_r.at[0], y_next)

        def line(k):
            return remote(
                line_out, line_in.at[k - 1], line_s.at[k - 1], line_r.at[k - 1], z_next(k)
            )

        for h in range(0, groups * per_group, 2):
            decay_row[:, h * HEAD : (h + 2) * HEAD] = per_head(decay_of[...], h)
        decay = decay_row[...]
        pair_out[:STATE, :] = state[...].astype(jnp.bfloat16)
        pair_out[STATE:, :] = jnp.broadcast_to(decay, (2 * RIM, inner)).astype(jnp.bfloat16)
        last_hop(0, (("xb", 2), ("ya", 4)))
        pair.start()
        first_hop(1)
        last_hop(0, (("yf", 5), ("xf", 6)))
        pair.wait_recv()
        mine = pl.ds(pl.multiple_of(y * wide, wide), wide)
        theirs = pl.ds(pl.multiple_of((1 - y) * wide, wide), wide)
        own_state, own_decay = state[:, mine], decay_row[:, mine]
        other_state = pair_in[:STATE, mine].astype(jnp.float32)
        other_decay = pair_in[STATE : STATE + 1, mine].astype(jnp.float32)
        later = y == 1
        both = jnp.where(
            later, other_state * own_decay + own_state, own_state * other_decay + other_state
        )
        line_out[:STATE, :] = both.astype(jnp.bfloat16)
        line_out[STATE:, :] = jnp.broadcast_to(own_decay * other_decay, (2 * RIM, wide)).astype(
            jnp.bfloat16
        )
        line_sum[...] = jnp.zeros_like(line_sum)
        for k in range(1, depth):
            @pl.when(z + k < depth)
            def _():
                line(k).start()

        z_copy(depth - 1).start()
        for k in range(depth - 1, 0, -1):
            @pl.when(z >= k)
            def _():
                line(k).wait_recv()
                line_sum[...] = line_sum[...] * line_in[k - 1, STATE : STATE + 1, :].astype(
                    jnp.float32
                ) + line_in[k - 1, :STATE, :].astype(jnp.float32)

        swap_out[...] = line_sum[...].astype(jnp.bfloat16)
        state[:, mine] = line_sum[...]
        second_hop(1)
        swap.start()
        swap.wait_recv()
        state[:, theirs] = swap_in[...].astype(jnp.float32)

        @pl.when(later)
        def _():
            state[...] = state[...] * pair_in[STATE : STATE + 1, :].astype(jnp.float32) + pair_in[
                :STATE, :
            ].astype(jnp.float32)

        pair.wait_send()
        swap.wait_send()
        for k in range(1, depth):
            @pl.when(z + k < depth)
            def _():
                line(k).wait_send()

    @pl.when(output_pass)
    def _():
        first = step == blocks + 1
        xv = conv_after(xbuf, first, x_ref, xr_ref, has_rim, xt_ref)
        bv = conv_after(bbuf, first, b_ref, br_ref, has_rim, bt_ref)
        cv = conv_after(cbuf, first, c_ref, cr_ref, has_rim, ct_ref)
        at = step - blocks - 1
        lw = lw_of[at]
        cum = cum_of[at]
        end = end_of[at]
        causal = lax.broadcasted_iota(jnp.int32, (SPAN, SPAN), 0) >= lax.broadcasted_iota(
            jnp.int32, (SPAN, SPAN), 1
        )
        group_cols = per_group * HEAD
        for g in range(groups):
            bt = bv[:, g * STATE : (g + 1) * STATE].T.astype(jnp.bfloat16)
            cg = cv[:, g * STATE : (g + 1) * STATE].astype(jnp.bfloat16)
            scores = jnp.dot(cg, bt, preferred_element_type=jnp.float32)
            squares = jnp.zeros((SPAN, 2 * HEAD), jnp.float32)
            for pair in range(per_group // 2):
                h = g * per_group + 2 * pair
                cols = slice(h * HEAD, (h + 2) * HEAD)
                xp = xv[:, cols]
                cum_0, cum_1 = spread(cum, h, SPAN), spread(cum, h + 1, SPAN)
                row_0, row_1 = row_of[at, h : h + 1, :], row_of[at, h + 1 : h + 2, :]
                m_0 = scores * jnp.exp(jnp.where(causal, cum_0 + row_0, -jnp.inf))
                m_1 = scores * jnp.exp(jnp.where(causal, cum_1 + row_1, -jnp.inf))
                mixing = jnp.concatenate([m_0.astype(jnp.bfloat16), m_1.astype(jnp.bfloat16)], axis=1)
                x_0 = jnp.where(low, xp, 0.0).astype(jnp.bfloat16)
                x_1 = jnp.where(low, 0.0, xp).astype(jnp.bfloat16)
                value = jnp.dot(
                    mixing, jnp.concatenate([x_0, x_1], axis=0), preferred_element_type=jnp.float32
                )
                before = state[:, cols]
                carried = jnp.dot(cg, before.astype(jnp.bfloat16), preferred_element_type=jnp.float32)
                value = value + carried * jnp.exp(jnp.where(low, cum_0, cum_1)) + xp * per_head(skip_of[...], h)
                factor = jnp.exp(
                    jnp.where(low, spread(lw, h, 2 * HEAD), spread(lw, h + 1, 2 * HEAD))
                )
                xw = (xp * factor).astype(jnp.bfloat16)
                added = jnp.dot(bt, xw, preferred_element_type=jnp.float32)
                state[:, cols] = before * per_head(end, h) + added
                gate = z_ref[:, cols].astype(jnp.float32)
                gated = value * (gate * jax.nn.sigmoid(gate))
                squares = squares + gated * gated
                ybuf[:, cols] = gated
            mean = jnp.sum(squares, axis=1, keepdims=True) / group_cols
            inverse = lax.rsqrt(mean + norm_eps)
            cols = slice(g * group_cols, (g + 1) * group_cols)
            nbuf[:, cols] = (ybuf[:, cols] * inverse * scale_ref[:, cols]).astype(jnp.bfloat16)
        part_ref[...] = jnp.dot(
            nbuf[...], exit_ref[...], preferred_element_type=jnp.float32
        ).astype(jnp.bfloat16)

    pace = blocks // (2 * depth - 2)
    for k in range(2, depth):
        at = blocks + 1 + (2 * k - 4) * pace

        @pl.when(step == at - (1 if k == 2 else 0))
        def _():
            first_hop(k)

        @pl.when(step == at + pace)
        def _():
            second_hop(k)
            last_hop(k - 1)

    @pl.when(step == 2 * blocks)
    def _():
        last_hop(depth - 1)
        for k in range(depth):
            for n in range(len(shared)):
                d_came(k, n).wait_recv()
        own_copy().wait()
        for n in range(3):
            rim_copy(n).wait_send()
        for k in range(1, depth):
            z_copy(k).wait_send()
        for k in range(depth):
            for name in moves:
                sent(name, k).wait_send()
            for n in range(len(shared)):
                d_sent(k, n).wait_send()


def dense_experts_fit(tok_rows, top_count, capacity, mix_rows):
    experts = lax.axis_size("ep")
    fits = experts % 2 == 0 and experts >= 4 and 3 * experts <= LANES and lax.axis_size("tp") == 4
    return fits and 2 * top_count >= experts and mix_rows % (4 * MIX_ROWS) == 0 and tok_rows == LANES and capacity % 16 == 0 and top_count <= 8


def marked_tokens(
    specialist_sample_slice, specialist_scaling_vector, chosen_specialists, dispatcher_affinity_matrix
):
    rows, features = specialist_sample_slice.shape
    return pl.pallas_call(
        functools.partial(routing_kernel, lax.axis_size("ep")),
        out_shape=jax.ShapeDtypeStruct((rows, features + LANES), jnp.bfloat16),
        scratch_shapes=[pltpu.VMEM((LANES, rows), jnp.float32)],
        name="routing",
    )(
        specialist_sample_slice, specialist_scaling_vector[None], chosen_specialists.T,
        dispatcher_affinity_matrix.T,
    )


def experts_dense(
    tokens, mix_part, rows, capacity, gating_projection, expand_projection, shrink_projection
):
    experts = lax.axis_size("ep")
    features = gating_projection.shape[1]
    depth, steps = experts // 2, experts
    cut = features * CUT_EIGHTHS // 8 // LANES * LANES
    rest = features - cut
    hidden = gating_projection.shape[2]
    narrow = jnp.bfloat16
    dma = pltpu.SemaphoreType.DMA
    share = mix_part.shape[0] // 4
    pieces = share // MIX_ROWS
    work = 2 * experts * 4 * capacity * features * hidden * 3
    return pl.pallas_call(
        functools.partial(experts_kernel, experts, capacity),
        in_specs=[pl.BlockSpec(memory_space=pl.ANY)] * 2
        + [pl.BlockSpec(memory_space=pltpu.VMEM)] * 3,
        out_specs=[pl.BlockSpec(memory_space=pltpu.VMEM)] * 2,
        out_shape=[
            jax.ShapeDtypeStruct((rows, features), narrow),
            jax.ShapeDtypeStruct((share, features), narrow),
        ],
        scratch_shapes=[
            pltpu.VMEM((2, 4 * rows, features + LANES), narrow),
            pltpu.VMEM((4 * capacity, features), narrow),
            pltpu.VMEM((steps, 2, capacity, cut), narrow),
            pltpu.VMEM((steps, 2, capacity, rest), narrow),
            pltpu.VMEM((steps, 2, capacity, cut), narrow),
            pltpu.VMEM((steps, 2, capacity, rest), narrow),
            pltpu.VMEM((steps, 2, capacity, cut), narrow),
            pltpu.VMEM((steps, 2, capacity, rest), narrow),
            pltpu.VMEM((steps, 2, rows, LANES), narrow),
            pltpu.VMEM((steps, 2, rows, LANES), narrow),
            pltpu.VMEM((steps, capacity, cut), narrow),
            pltpu.VMEM((depth, 2, capacity, rest), narrow),
            pltpu.VMEM((depth, rows, cut), narrow),
            pltpu.VMEM((depth, rows, cut), narrow),
            pltpu.VMEM((rows, rest), narrow),
            pltpu.VMEM((rows, rest), narrow),
            pltpu.VMEM((depth, rows, cut), jnp.float32),
            pltpu.VMEM((2, rows, rest), jnp.float32),
            pltpu.VMEM((depth - 1, rows, cut), narrow),
            pltpu.VMEM((depth - 1, rows, cut), narrow),
            pltpu.VMEM((depth - 1, 2, rows, rest), narrow),
            pltpu.VMEM((depth - 1, 2, rows, rest), narrow),
            pltpu.VMEM((2, share, features), narrow),
            pltpu.VMEM((2, share, features), narrow),
            pltpu.VMEM((share, features), narrow),
            pltpu.VMEM((share, features), narrow),
            dma((3,)), dma((3,)), dma((3,)), dma((pieces,)), dma((pieces,)),
            dma((2,)), dma((2 * steps,)), dma((2 * steps,)), dma((steps,)), dma((steps,)),
            dma((depth,)), dma((depth,)), dma((depth,)), dma((depth,)), dma((1,)), dma((1,)),
            dma((depth - 1,)), dma((depth - 1,)), dma((depth - 1,)), dma((depth - 1,)),
        ],
        compiler_params=pltpu.CompilerParams(
            collective_id=0, has_side_effects=True, vmem_limit_bytes=63 * 1024 * 1024
        ),
        cost_estimate=pl.CostEstimate(
            flops=8 * work, bytes_accessed=4 * tokens.size, transcendentals=0
        ),
        name="experts",
    )(tokens, mix_part, gating_projection[0], expand_projection[0], shrink_projection[0])


def body(
    sequence_entry_features,
    sequence_exit_gating,
    memory_insert_clusters,
    memory_query_clusters,
    interval_presoftplus,
    entry_filter_taps,
    insert_filter_taps,
    query_filter_taps,
    interval_offset,
    head_fading_exponent,
    skip_connection_factor,
    spike_fading_exponent,
    cluster_scaling_vector,
    sequence_exit_projection,
    specialist_sample_slice,
    specialist_scaling_vector,
    chosen_specialists,
    dispatcher_affinity_matrix,
    gating_projection,
    expand_projection,
    shrink_projection,
):
    tok_rows, top_count = chosen_specialists.shape
    capacity = tok_rows * top_count * 5 // (4 * lax.axis_size("ep"))
    dense = dense_experts_fit(tok_rows, top_count, capacity, sequence_entry_features.shape[0])
    marked = None
    if dense:
        marked = marked_tokens(
            specialist_sample_slice,
            specialist_scaling_vector,
            chosen_specialists,
            dispatcher_affinity_matrix,
        )
    mix_part = mixer_half(
        sequence_entry_features,
        sequence_exit_gating,
        memory_insert_clusters,
        memory_query_clusters,
        interval_presoftplus,
        entry_filter_taps,
        insert_filter_taps,
        query_filter_taps,
        interval_offset,
        head_fading_exponent,
        skip_connection_factor,
        spike_fading_exponent,
        cluster_scaling_vector,
        sequence_exit_projection,
        marked,
    )
    if dense:
        mix_part, tokens = mix_part
        moe_out, mixed = experts_dense(
            tokens, mix_part, tok_rows, capacity, gating_projection, expand_projection, shrink_projection
        )
        return (mixed, moe_out)
    mixed = lax.psum_scatter(mix_part, "tp", scatter_dimension=0, tiled=True)
    moe_out = experts_half(
        specialist_sample_slice,
        specialist_scaling_vector,
        chosen_specialists,
        dispatcher_affinity_matrix,
        gating_projection,
        expand_projection,
        shrink_projection,
    )
    return (mixed, moe_out)


def solution(mesh):
    in_specs = (
        P("ep", "tp"),
        P("ep", "tp"),
        P("ep", "tp"),
        P("ep", "tp"),
        P("ep", "tp"),
        P(None, "tp"),
        P(None, "tp"),
        P(None, "tp"),
        P("tp"),
        P("tp"),
        P("tp"),
        P("ep", "tp"),
        P("tp"),
        P("tp", None),
        P(("ep", "tp"), None),
        P(),
        P(("ep", "tp"), None),
        P(("ep", "tp"), None),
        P("ep", None, "tp"),
        P("ep", None, "tp"),
        P("ep", "tp", None),
    )
    out_specs = (P(("ep", "tp"), None), P(("ep", "tp"), None))
    return jax.shard_map(body, mesh=mesh, in_specs=in_specs, out_specs=out_specs, check_vma=False)
```

```python
import functools
import jax
import jax.numpy as jnp
from jax import lax
from jax.experimental import pallas as pl
from jax.experimental.pallas import tpu as pltpu
from jax.sharding import PartitionSpec as P

HEAD = 64
STATE = 128
SPAN = 128
RIM = 8
LANES = 128
MIX_ROWS = 32
CUT_EIGHTHS = 5

norm_eps = 1e-05
clamp_top = 7.0
sigmoid_sharp = 1.702
highest = lax.Precision.HIGHEST


def passed_along(block, axis, distance):
    devices = range(lax.axis_size(axis))
    route = [(i - distance, i) for i in devices if i - distance in devices]
    return lax.ppermute(block, axis, route)


def conv_block(buf, first, value_ref, rim_ref, taps_ref):
    @pl.when(first)
    def _():
        buf[0:RIM, :] = rim_ref[...].astype(jnp.float32)

    @pl.when(jnp.logical_not(first))
    def _():
        buf[0:RIM, :] = buf[SPAN : SPAN + RIM, :]

    buf[RIM : RIM + SPAN, :] = value_ref[...].astype(jnp.float32)
    taps = taps_ref[...].astype(jnp.float32)
    count = taps.shape[0]
    total = buf[RIM : RIM + SPAN, :] * taps[count - 1 : count]
    for j in range(count - 1):
        start = RIM - (count - 1) + j
        total = total + buf[start : start + SPAN, :] * taps[j : j + 1]
    return total * jax.nn.sigmoid(total)


def conv_after(buf, first, value_ref, rim_ref, has_rim, taps_ref):
    @pl.when(first)
    def _():
        rim = rim_ref[...].astype(jnp.float32)[RIM:]
        buf[0:RIM, :] = jnp.where(has_rim, rim, 0.0)

    @pl.when(jnp.logical_not(first))
    def _():
        buf[0:RIM, :] = buf[SPAN : SPAN + RIM, :]

    buf[RIM : RIM + SPAN, :] = value_ref[...].astype(jnp.float32)
    taps = taps_ref[...].astype(jnp.float32)
    count = taps.shape[0]
    total = buf[RIM : RIM + SPAN, :] * taps[count - 1 : count]
    for j in range(count - 1):
        start = RIM - (count - 1) + j
        total = total + buf[start : start + SPAN, :] * taps[j : j + 1]
    return total * jax.nn.sigmoid(total)


def spread(cols, h, width):
    return jnp.broadcast_to(cols[:, h : h + 1], (SPAN, width))


def state_kernel(per_group, groups, x_ref, xr_ref, xt_ref, b_ref, br_ref, bt_ref, lw_ref, end_ref,
                 state_ref, xbuf, bbuf):
    first = pl.program_id(0) == 0
    x = conv_block(xbuf, first, x_ref, xr_ref, xt_ref)
    b = conv_block(bbuf, first, b_ref, br_ref, bt_ref)

    @pl.when(first)
    def _():
        state_ref[...] = jnp.zeros_like(state_ref)

    lw = lw_ref[...]
    low = lax.broadcasted_iota(jnp.int32, (SPAN, 2 * HEAD), 1) < HEAD
    for g in range(groups):
        bt = b[:, g * STATE : (g + 1) * STATE].T.astype(jnp.bfloat16)
        for pair in range(per_group // 2):
            h = g * per_group + 2 * pair
            cols = slice(h * HEAD, (h + 2) * HEAD)
            factor = jnp.exp(jnp.where(low, spread(lw, h, 2 * HEAD), spread(lw, h + 1, 2 * HEAD)))
            xw = (x[:, cols] * factor).astype(jnp.bfloat16)
            added = jnp.dot(bt, xw, preferred_element_type=jnp.float32)
            state_ref[:, cols] = state_ref[:, cols] * end_ref[0, :, cols] + added


def output_kernel(per_group, groups, x_ref, xr_ref, xt_ref, b_ref, br_ref, bt_ref, c_ref, cr_ref,
                  ct_ref, z_ref, lw_ref, cum_ref, row_ref, end_ref, enter_ref, skip_ref, scale_ref,
                  out_ref, xbuf, bbuf, cbuf, state, ybuf):
    first = pl.program_id(0) == 0
    x = conv_block(xbuf, first, x_ref, xr_ref, xt_ref)
    b = conv_block(bbuf, first, b_ref, br_ref, bt_ref)
    c = conv_block(cbuf, first, c_ref, cr_ref, ct_ref)

    @pl.when(first)
    def _():
        state[...] = enter_ref[...]

    lw = lw_ref[...]
    cum = cum_ref[...]
    low = lax.broadcasted_iota(jnp.int32, (SPAN, 2 * HEAD), 1) < HEAD
    causal = lax.broadcasted_iota(jnp.int32, (SPAN, SPAN), 0) >= lax.broadcasted_iota(
        jnp.int32, (SPAN, SPAN), 1
    )
    group_cols = per_group * HEAD
    for g in range(groups):
        bg = b[:, g * STATE : (g + 1) * STATE]
        bt = bg.T.astype(jnp.bfloat16)
        cg = c[:, g * STATE : (g + 1) * STATE].astype(jnp.bfloat16)
        scores = jnp.dot(cg, bt, preferred_element_type=jnp.float32)
        squares = jnp.zeros((SPAN, 2 * HEAD), jnp.float32)
        for pair in range(per_group // 2):
            h = g * per_group + 2 * pair
            cols = slice(h * HEAD, (h + 2) * HEAD)
            xp = x[:, cols]
            cum_0, cum_1 = spread(cum, h, SPAN), spread(cum, h + 1, SPAN)
            m_0 = scores * jnp.exp(jnp.where(causal, cum_0 + row_ref[0, h : h + 1, :], -jnp.inf))
            m_1 = scores * jnp.exp(jnp.where(causal, cum_1 + row_ref[0, h + 1 : h + 2, :], -jnp.inf))
            mixing = jnp.concatenate([m_0.astype(jnp.bfloat16), m_1.astype(jnp.bfloat16)], axis=1)
            x_0 = jnp.where(low, xp, 0.0).astype(jnp.bfloat16)
            x_1 = jnp.where(low, 0.0, xp).astype(jnp.bfloat16)
            y = jnp.dot(
                mixing, jnp.concatenate([x_0, x_1], axis=0), preferred_element_type=jnp.float32
            )
            before = state[:, cols]
            carried = jnp.dot(cg, before.astype(jnp.bfloat16), preferred_element_type=jnp.float32)
            y = y + carried * jnp.exp(jnp.where(low, cum_0, cum_1)) + xp * skip_ref[:, cols]
            factor = jnp.exp(jnp.where(low, spread(lw, h, 2 * HEAD), spread(lw, h + 1, 2 * HEAD)))
            xw = (xp * factor).astype(jnp.bfloat16)
            added = jnp.dot(bt, xw, preferred_element_type=jnp.float32)
            state[:, cols] = before * end_ref[0, :, cols] + added
            gate = z_ref[:, cols].astype(jnp.float32)
            gated = y * (gate * jax.nn.sigmoid(gate))
            squares = squares + gated * gated
            ybuf[:, cols] = gated
        mean = jnp.sum(squares, axis=1, keepdims=True) / group_cols
        inverse = lax.rsqrt(mean + norm_eps)
        cols = slice(g * group_cols, (g + 1) * group_cols)
        out_ref[:, cols] = (ybuf[:, cols] * inverse * scale_ref[:, cols]).astype(jnp.bfloat16)


def entering_state(own_state, own_decay):
    size, mine = (lax.axis_size("ep"), lax.axis_index("ep"))
    rows = own_state.shape[0]
    total = own_state
    decay = own_decay

    def joined():
        return jnp.concatenate(
            [total, jnp.broadcast_to(decay, (RIM, decay.shape[1]))], axis=0
        ).astype(jnp.bfloat16)

    distance = 1
    while distance < size:
        came = passed_along(joined(), "ep", distance)
        there = mine >= distance
        earlier = came[:rows].astype(jnp.float32)
        earlier_decay = jnp.where(there, came[rows : rows + 1].astype(jnp.float32), 1.0)
        total = earlier * decay + total
        decay = earlier_decay * decay
        distance *= 2
    return passed_along(total.astype(jnp.bfloat16), "ep", 1).astype(jnp.float32)


def mixer_half(
    sequence_entry_features,
    sequence_exit_gating,
    memory_insert_clusters,
    memory_query_clusters,
    interval_presoftplus,
    entry_filter_taps,
    insert_filter_taps,
    query_filter_taps,
    interval_offset,
    head_fading_exponent,
    skip_connection_factor,
    spike_fading_exponent,
    cluster_scaling_vector,
    sequence_exit_projection,
    marked,
):
    tok_rows = sequence_entry_features.shape[0]
    local_heads = interval_offset.shape[0]
    local_groups = memory_insert_clusters.shape[1] // STATE
    per_group = local_heads // local_groups
    if marked is not None:
        return mixer_gather(
            per_group, local_groups, tok_rows // SPAN,
            (sequence_entry_features, memory_insert_clusters, memory_query_clusters),
            (entry_filter_taps, insert_filter_taps, query_filter_taps), sequence_exit_gating,
            interval_presoftplus.T, spike_fading_exponent.T,
            (interval_offset[None], head_fading_exponent[None], skip_connection_factor[None]),
            cluster_scaling_vector[None],
            sequence_exit_projection, marked,
        )
    inner_cols = sequence_entry_features.shape[1]
    state_cols = memory_insert_clusters.shape[1]
    last_rows = jnp.concatenate(
        [
            sequence_entry_features[tok_rows - RIM :],
            memory_insert_clusters[tok_rows - RIM :],
            memory_query_clusters[tok_rows - RIM :],
        ],
        axis=1,
    )
    rims = passed_along(last_rows, "ep", 1)
    rim_x = rims[:, :inner_cols]
    rim_b = rims[:, inner_cols : inner_cols + state_cols]
    rim_c = rims[:, inner_cols + state_cols :]
    blocks = tok_rows // SPAN
    interval = jax.nn.softplus(interval_presoftplus.astype(jnp.float32) + interval_offset)
    fading = spike_fading_exponent - jnp.exp(head_fading_exponent) * interval
    lower = jnp.tril(jnp.ones((SPAN, SPAN), jnp.float32))
    cumulative = jnp.einsum(
        "ts,csh->cth", lower, fading.reshape(blocks, SPAN, local_heads), precision=highest
    )
    log_step = jnp.log(interval).reshape(blocks, SPAN, local_heads)
    block_end = cumulative[:, -1:]
    key_log = (log_step - cumulative + block_end).reshape(tok_rows, local_heads)
    row_log = jnp.swapaxes(log_step - cumulative, 1, 2)
    end_factor = jnp.repeat(jnp.exp(block_end), HEAD, axis=2)
    own_decay = jnp.repeat(jnp.exp(jnp.sum(block_end, axis=0)), HEAD, axis=1)
    cumulative = cumulative.reshape(tok_rows, local_heads)

    def rows_of(width):
        return pl.BlockSpec((SPAN, width), lambda i: (i, 0))

    def fixed(shape):
        return pl.BlockSpec(shape, lambda i: (0, 0))

    def block_of(rows, width):
        return pl.BlockSpec((1, rows, width), lambda i: (i, 0, 0))

    def cost(dots):
        return pl.CostEstimate(
            flops=dots * tok_rows * inner_cols * STATE * 8,
            bytes_accessed=dots * tok_rows * inner_cols * 8,
            transcendentals=0,
        )

    taps = entry_filter_taps.shape[0]
    x_specs = [rows_of(inner_cols), fixed((RIM, inner_cols)), fixed((taps, inner_cols))]
    s_specs = [rows_of(state_cols), fixed((RIM, state_cols)), fixed((taps, state_cols))]
    x_args = (sequence_entry_features, rim_x, entry_filter_taps)
    b_args = (memory_insert_clusters, rim_b, insert_filter_taps)
    c_args = (memory_query_clusters, rim_c, query_filter_taps)
    own_state = pl.pallas_call(
        functools.partial(state_kernel, per_group, local_groups),
        grid=(blocks,),
        in_specs=x_specs + s_specs + [rows_of(local_heads), block_of(1, inner_cols)],
        out_specs=fixed((STATE, inner_cols)),
        out_shape=jax.ShapeDtypeStruct((STATE, inner_cols), jnp.float32),
        scratch_shapes=[
            pltpu.VMEM((SPAN + RIM, inner_cols), jnp.float32),
            pltpu.VMEM((SPAN + RIM, state_cols), jnp.float32),
        ],
        cost_estimate=cost(1),
        name="own_state",
    )(*x_args, *b_args, key_log, end_factor)
    entering = entering_state(own_state, own_decay)
    normed = pl.pallas_call(
        functools.partial(output_kernel, per_group, local_groups),
        grid=(blocks,),
        in_specs=x_specs + s_specs + s_specs + [
            rows_of(inner_cols),
            rows_of(local_heads),
            rows_of(local_heads),
            block_of(local_heads, SPAN),
            block_of(1, inner_cols),
            fixed((STATE, inner_cols)),
            fixed((1, inner_cols)),
            fixed((1, inner_cols)),
        ],
        out_specs=rows_of(inner_cols),
        out_shape=jax.ShapeDtypeStruct((tok_rows, inner_cols), jnp.bfloat16),
        scratch_shapes=[
            pltpu.VMEM((SPAN + RIM, inner_cols), jnp.float32),
            pltpu.VMEM((SPAN + RIM, state_cols), jnp.float32),
            pltpu.VMEM((SPAN + RIM, state_cols), jnp.float32),
            pltpu.VMEM((STATE, inner_cols), jnp.float32),
            pltpu.VMEM((SPAN, inner_cols), jnp.float32),
        ],
        cost_estimate=cost(3),
        name="mixer_output",
    )(
        *x_args, *b_args, *c_args, sequence_exit_gating, key_log, cumulative, row_log, end_factor,
        entering, jnp.repeat(skip_connection_factor, HEAD)[None], cluster_scaling_vector[None],
    )
    return jnp.dot(normed, sequence_exit_projection, preferred_element_type=jnp.float32).astype(
        jnp.bfloat16
    )


def mixer_gather(
    per_group, groups, blocks, streams, filters, gating, raw, spikes, heads, scale,
    exit_projection, marked,
):
    tok_rows, inner_cols = gating.shape
    state_cols = streams[1].shape[1]
    head_count = raw.shape[0]
    features = exit_projection.shape[1]
    rows, marked_cols = marked.shape
    taps = filters[0].shape[0]
    devices = lax.axis_size("ep") * lax.axis_size("tp")
    depth = lax.axis_size("ep") // 2
    narrow, wide = jnp.bfloat16, inner_cols // 2
    pieces = 7 * depth

    def either(i):
        return jnp.where(i < blocks, i, jnp.maximum(i - blocks - 1, 0))

    def late(i):
        return jnp.maximum(i - blocks - 1, 0)

    def by_rows(width, at):
        return pl.BlockSpec((SPAN, width), lambda i: (at(i), 0))

    def fixed(shape):
        return pl.BlockSpec(shape, lambda i: (0, 0))

    def conv_specs(width, at):
        return [by_rows(width, at), fixed((taps, width))]

    dma = pltpu.SemaphoreType.DMA
    hops = [dma((depth,)) for _ in range(12)]
    return pl.pallas_call(
        functools.partial(mixer_gather_kernel, per_group, groups, blocks, depth),
        grid=(2 * blocks + 1,),
        in_specs=conv_specs(inner_cols, either)
        + conv_specs(state_cols, either)
        + conv_specs(state_cols, late)
        + [
            by_rows(inner_cols, late),
            fixed((head_count, tok_rows)),
            fixed((head_count, tok_rows)),
            fixed((1, head_count)),
            fixed((1, head_count)),
            fixed((1, head_count)),
            fixed((1, inner_cols)),
            fixed((inner_cols, features)),
            fixed((rows, marked_cols)),
        ]
        + [pl.BlockSpec(memory_space=pl.ANY)] * 3,
        out_specs=[by_rows(features, late), pl.BlockSpec(memory_space=pl.ANY)],
        out_shape=[
            jax.ShapeDtypeStruct((tok_rows, features), narrow),
            jax.ShapeDtypeStruct((devices * rows, marked_cols), narrow),
        ],
        scratch_shapes=[
            pltpu.VMEM((LANES, LANES), jnp.float32),
            pltpu.VMEM((blocks, SPAN, head_count), jnp.float32),
            pltpu.VMEM((blocks, SPAN, head_count), jnp.float32),
            pltpu.VMEM((blocks, head_count, SPAN), jnp.float32),
            pltpu.VMEM((blocks, 1, head_count), jnp.float32),
            pltpu.VMEM((1, head_count), jnp.float32),
            pltpu.VMEM((1, head_count), jnp.float32),
            pltpu.VMEM((1, inner_cols), jnp.float32),
            pltpu.VMEM((2 * RIM, inner_cols), narrow),
            pltpu.VMEM((2 * RIM, state_cols), narrow),
            pltpu.VMEM((2 * RIM, state_cols), narrow),
            dma((3,)), dma((3,)),
            pltpu.VMEM((SPAN + RIM, inner_cols), jnp.float32),
            pltpu.VMEM((SPAN + RIM, state_cols), jnp.float32),
            pltpu.VMEM((SPAN + RIM, state_cols), jnp.float32),
            pltpu.VMEM((STATE, inner_cols), jnp.float32),
            pltpu.VMEM((SPAN, inner_cols), jnp.float32),
            pltpu.VMEM((SPAN, inner_cols), narrow),
            pltpu.VMEM((STATE + 2 * RIM, inner_cols), narrow),
            pltpu.VMEM((STATE + 2 * RIM, inner_cols), narrow),
            pltpu.VMEM((STATE + 2 * RIM, wide), narrow),
            pltpu.VMEM((depth - 1, STATE + 2 * RIM, wide), narrow),
            pltpu.VMEM((STATE, wide), jnp.float32),
            pltpu.VMEM((STATE, wide), narrow),
            pltpu.VMEM((STATE, wide), narrow),
            dma((1,)), dma((depth - 1,)), dma((depth - 1,)),
            *hops,
            dma((pieces,)), dma((pieces,)), dma((1,)), dma((1,)), dma((depth - 1,)),
            dma((depth - 1,)), dma((1,)), dma((1,)),
        ],
        compiler_params=pltpu.CompilerParams(
            collective_id=1, has_side_effects=True, vmem_limit_bytes=56 * 1024 * 1024,
            dimension_semantics=("arbitrary",),
        ),
        cost_estimate=pl.CostEstimate(
            flops=tok_rows * inner_cols * (features * 2 + STATE * 16),
            bytes_accessed=tok_rows * inner_cols * 16,
            transcendentals=0,
        ),
        name="mixer_gather",
    )(
        streams[0], filters[0], streams[1], filters[1], streams[2], filters[2], gating, raw, spikes,
        *heads, scale, exit_projection, marked, *streams,
    )


def experts_half(
    specialist_sample_slice,
    specialist_scaling_vector,
    chosen_specialists,
    dispatcher_affinity_matrix,
    gating_projection,
    expand_projection,
    shrink_projection,
):
    tok_rows = specialist_sample_slice.shape[0]
    feature_count = specialist_sample_slice.shape[1]
    top_count = chosen_specialists.shape[1]
    experts = lax.axis_size("ep")
    groups_tp = lax.axis_size("tp")
    capacity = tok_rows * top_count * 5 // (4 * experts)
    as_float = specialist_sample_slice.astype(jnp.float32)
    centred = as_float - jnp.mean(as_float, axis=1, keepdims=True)
    normed = (
        centred
        * lax.rsqrt(jnp.mean(centred * centred, axis=1, keepdims=True) + norm_eps)
        * specialist_scaling_vector
    ).astype(jnp.bfloat16)
    route_weight = jnp.exp(dispatcher_affinity_matrix) / jnp.sum(
        jnp.exp(dispatcher_affinity_matrix), axis=1, keepdims=True
    )
    flat_routes = chosen_specialists.reshape(-1)
    onehot = (flat_routes[:, None] == jnp.arange(experts, dtype=jnp.int32)[None, :]).astype(
        jnp.int32
    )
    position = jnp.sum(onehot * (jnp.cumsum(onehot, axis=0) - 1), axis=1)
    target = flat_routes * capacity + position
    token_ids = jnp.arange(tok_rows * top_count, dtype=jnp.int32) // top_count
    source_table = jnp.full((experts * capacity,), tok_rows, jnp.int32).at[target].set(token_ids)
    padded = jnp.concatenate([normed, jnp.zeros((1, feature_count), jnp.bfloat16)], axis=0)
    outgoing = padded[source_table].reshape(experts, capacity, feature_count)
    arrived = lax.all_to_all(outgoing, "ep", split_axis=0, concat_axis=0, tiled=True)
    shard_rows = lax.all_gather(arrived, "tp", axis=0, tiled=True)
    rows_in = shard_rows.reshape(-1, feature_count)
    gate_h = jnp.dot(rows_in, gating_projection[0], preferred_element_type=jnp.float32)
    up_h = jnp.dot(rows_in, expand_projection[0], preferred_element_type=jnp.float32)
    clipped = jnp.minimum(gate_h, clamp_top)
    hidden_act = (
        (
            clipped
            * jax.nn.sigmoid(sigmoid_sharp * clipped)
            * (jnp.clip(up_h, -clamp_top, clamp_top) + 1.0)
        )
        .astype(jnp.bfloat16)
        .reshape(shard_rows.shape[0], capacity, -1)
    )
    hidden_act = hidden_act.reshape(groups_tp * experts * capacity, -1)
    summed = lax.psum_scatter(
        jnp.dot(hidden_act, shrink_projection[0], preferred_element_type=jnp.float32).astype(
            jnp.bfloat16
        ),
        "tp",
        scatter_dimension=0,
        tiled=True,
    )
    returned = lax.all_to_all(
        summed.reshape(experts, capacity, feature_count),
        "ep",
        split_axis=0,
        concat_axis=0,
        tiled=True,
    )
    slot_out = returned.reshape(experts * capacity, feature_count)[target].reshape(
        tok_rows, top_count, feature_count
    )
    combined = jnp.einsum("tk,tkd->td", route_weight, slot_out.astype(jnp.float32))
    return combined.astype(jnp.bfloat16)


def routing_kernel(experts, x_ref, scale_ref, chosen_ref, score_ref, out_ref, turned):
    features = x_ref.shape[1]
    top_count, rows = chosen_ref.shape
    value = x_ref[...].astype(jnp.float32)
    centred = value - jnp.mean(value, axis=1, keepdims=True)
    spread_of = jnp.mean(centred * centred, axis=1, keepdims=True)
    normed = centred * lax.rsqrt(spread_of + norm_eps) * scale_ref[...]
    out_ref[:, :features] = normed.astype(jnp.bfloat16)
    raised = jnp.exp(score_ref[...])
    turned[...] = jnp.zeros_like(turned)
    turned[0:top_count, :] = chosen_ref[...].astype(jnp.float32)
    turned[8 : 8 + top_count, :] = raised / jnp.sum(raised, axis=0, keepdims=True)
    columns = turned[...].T
    lane = lax.broadcasted_iota(jnp.int32, (rows, LANES), 1)
    named = lax.rem(lane, experts).astype(jnp.float32)
    held = jnp.zeros((rows, LANES), jnp.float32)
    share = jnp.zeros((rows, LANES), jnp.float32)
    for k in range(top_count):
        same = columns[:, k : k + 1] == named
        held = held + jnp.where(same, 1.0, 0.0)
        share = share + jnp.where(same, columns[:, 8 + k : 9 + k], 0.0)
    earlier = lax.broadcasted_iota(jnp.int32, (rows, rows), 0) > lax.broadcasted_iota(
        jnp.int32, (rows, rows), 1
    )
    place = jnp.dot(
        jnp.where(earlier, 1.0, 0.0).astype(jnp.bfloat16),
        held.astype(jnp.bfloat16),
        preferred_element_type=jnp.float32,
    )
    place = jnp.where(held > 0.0, place, 255.0)
    coarse = share.astype(jnp.bfloat16).astype(jnp.float32)
    table = jnp.where(lane < experts, place, jnp.where(lane < 2 * experts, coarse, share - coarse))
    out_ref[:, features:] = table.astype(jnp.bfloat16)


def experts_kernel(
    experts, capacity, tokens_ref, mix_ref, gate_ref, up_ref, down_ref, out_ref, mixed_ref,
    tokens, slots, own_a, own_b, outgoing_a, outgoing_b, incoming_a, incoming_b, place, place_next,
    from_x, from_y, to_y, came_y, to_x, came_x, keep_a, keep_b, to_za, from_za, to_zb, from_zb,
    mix_own, mix_core, mix_out, mix_in, mix_sem, mc_send, mc_recv, mx_send, mx_recv,
    token_sem, core_send, core_recv, x_send, x_recv, y_send, y_recv,
    a_send, a_recv, b_send, b_recv, za_send, za_recv, zb_send, zb_recv,
):
    depth = experts // 2
    steps = experts
    ep, tp = lax.axis_index("ep"), lax.axis_index("tp")
    z, y, x, core = ep // 2, ep % 2, tp // 2, tp % 2
    next_ep = z * 2 + 1 - y
    sibling = {"tp": x * 2 + 1 - core}
    x_next = {"tp": (1 - x) * 2 + core}
    y_next = {"ep": next_ep}
    rows = out_ref.shape[0]
    features = out_ref.shape[1]
    cut = own_a.shape[3]
    own, outgoing, incoming = (own_a, own_b), (outgoing_a, outgoing_b), (incoming_a, incoming_b)
    mesh_id = pl.DeviceIdType.MESH

    def z_next(k):
        return {"ep": ((z + k) % depth) * 2 + y}

    def turn(i):
        middle = depth // 2
        others = jnp.where(i == 0, middle, jnp.where(i < middle, i, i + 1))
        return jnp.where(i == depth - 1, 0, others)

    def fetch(s):
        k, dy = turn(s // 2), 1 - s % 2
        block = ((z + k) % depth) * 2 + (y + dy) % 2
        span = 4 * rows
        return pltpu.make_async_copy(
            tokens_ref.at[pl.ds(pl.multiple_of(block * span, span), span)],
            tokens.at[s % 2],
            token_sem.at[s % 2],
        )

    def remote(source, target, send, recv, device):
        return pltpu.make_async_remote_copy(
            src_ref=source, dst_ref=target, send_sem=send, recv_sem=recv,
            device_id=device, device_id_type=mesh_id,
        )

    def core_copy(s, side):
        send, recv = core_send.at[2 * s + side], core_recv.at[2 * s + side]
        return remote(outgoing[side].at[s], incoming[side].at[s], send, recv, sibling)

    def x_copy(s):
        return remote(own_a.at[s, 1], from_x.at[s], x_send.at[s], x_recv.at[s], x_next)

    def y_copy(i):
        return remote(own_b.at[2 * i], from_y.at[i], y_send.at[i], y_recv.at[i], y_next)

    def a_copy(i):
        return remote(to_y.at[i], came_y.at[i], a_send.at[i], a_recv.at[i], y_next)

    def b_copy():
        return remote(to_x, came_x, b_send.at[0], b_recv.at[0], x_next)

    def za_copy(i):
        return remote(to_za.at[i], from_za.at[i], za_send.at[i], za_recv.at[i], z_next(turn(i)))

    def zb_copy(i):
        return remote(to_zb.at[i], from_zb.at[i], zb_send.at[i], zb_recv.at[i], z_next(turn(i)))

    chunks, piece = mixed_ref.shape[0] // MIX_ROWS, MIX_ROWS
    share = mixed_ref.shape[0]

    early, late = chunks // 4, chunks // 2

    def mix_part(n, c):
        dx, start, stop = ((0, 0, share), (1, early * piece, share), (1, 0, early * piece))[n]
        block = ((x + dx) % 2) * 2 + c
        rows_n = pl.ds(pl.multiple_of(block * share + start, piece), stop - start)
        return dx, pl.ds(start, stop - start), mix_ref.at[rows_n]

    def mix_fetch(n):
        dx, there, source = mix_part(n, core)
        return pltpu.make_async_copy(source, mix_own.at[dx, there], mix_sem.at[n])

    def mix_core_copy(n):
        dx, there, source = mix_part(n, 1 - core)
        return remote(source, mix_core.at[dx, there], mc_send.at[n], mc_recv.at[n], sibling)

    def mix_x_copy(j):
        rows_j = pl.ds(pl.multiple_of(j * piece, piece), piece)
        return remote(
            mix_out.at[rows_j], mix_in.at[rows_j], mx_send.at[j], mx_recv.at[j], x_next
        )

    def mix_away(j, carry):
        rows_j = pl.ds(pl.multiple_of(j * piece, piece), piece)
        mix_out[rows_j, :] = (
            mix_own[1, rows_j, :].astype(jnp.float32) + mix_core[1, rows_j, :].astype(jnp.float32)
        ).astype(jnp.bfloat16)
        return carry

    def mix_home(j, carry):
        rows_j = pl.ds(pl.multiple_of(j * piece, piece), piece)
        mix_own[0, rows_j, :] = (
            mix_own[0, rows_j, :].astype(jnp.float32) + mix_core[0, rows_j, :].astype(jnp.float32)
        ).astype(jnp.bfloat16)
        return carry

    def mix_send(j, carry):
        mix_x_copy(j).start()
        return carry

    def mix_finish(j, carry):
        rows_j = pl.ds(pl.multiple_of(j * piece, piece), piece)
        mix_x_copy(j).wait_recv()
        mixed_ref[rows_j, :] = (
            mix_own[0, rows_j, :].astype(jnp.float32) + mix_in[rows_j, :].astype(jnp.float32)
        ).astype(jnp.bfloat16)
        return carry

    def mix_sent(j, carry):
        mix_x_copy(j).wait_send()
        return carry

    fetch(0).start()
    for n in (2, 1, 0):
        mix_fetch(n).start()
    barrier = pltpu.get_barrier_semaphore()
    partners = [sibling, x_next, y_next] + [z_next(k) for k in range(1, depth)]
    for partner in partners:
        pl.semaphore_signal(barrier, inc=1, device_id=partner, device_id_type=mesh_id)
    pl.semaphore_wait(barrier, len(partners))

    for n in (2, 1, 0):
        mix_core_copy(n).start()

    lane = lax.broadcasted_iota(jnp.int32, (rows, LANES), 1)
    lane_value = lane.astype(jnp.float32)
    slot_lane = lax.broadcasted_iota(jnp.int32, (capacity, LANES), 1)

    def chosen_slots(table, expert):
        column = jnp.sum(jnp.where(lane == expert, table, 0.0), axis=1, keepdims=True)
        return jnp.where(column == lane_value, 1.0, 0.0)

    def compute(s):
        weights = []
        for dx in (0, 1):
            for q in (0, 1):
                c = core if q == 0 else 1 - core
                block = ((x + dx) % 2) * 2 + c
                start = pl.multiple_of(block * rows, rows)
                arrived = tokens[s % 2, pl.ds(start, rows), :]
                table = arrived[:, features:].astype(jnp.float32)
                picked = chosen_slots(table, ep)
                if q == 0:
                    place[s, dx] = picked.astype(jnp.bfloat16)
                    place_next[s, dx] = chosen_slots(table, next_ep).astype(jnp.bfloat16)
                select = picked.T[:capacity].astype(jnp.bfloat16)
                taken = jnp.dot(select, arrived, preferred_element_type=jnp.float32)
                first = (dx * 2 + q) * capacity
                slots[first : first + capacity, :] = taken[:, :features].astype(jnp.bfloat16)
                mine = (slot_lane == experts + ep) | (slot_lane == 2 * experts + ep)
                weights.append(
                    jnp.sum(jnp.where(mine, taken[:, features:], 0.0), axis=1, keepdims=True)
                )
        value = slots[...]
        gate_h = jnp.dot(value, gate_ref[...], preferred_element_type=jnp.float32)
        up_h = jnp.dot(value, up_ref[...], preferred_element_type=jnp.float32)
        clipped = jnp.minimum(gate_h, clamp_top)
        act = (
            clipped
            * jax.nn.sigmoid(sigmoid_sharp * clipped)
            * (jnp.clip(up_h, -clamp_top, clamp_top) + 1.0)
        ).astype(jnp.bfloat16)
        for side in (0, 1):
            columns = slice(0, cut) if side == 0 else slice(cut, features)
            part = jnp.dot(act, down_ref[:, columns], preferred_element_type=jnp.float32)
            for dx in (0, 1):
                for q in (0, 1):
                    first = (dx * 2 + q) * capacity
                    scaled = (part[first : first + capacity] * weights[dx * 2 + q]).astype(
                        jnp.bfloat16
                    )
                    if q == 0:
                        own[side][s, dx] = scaled
                    else:
                        outgoing[side][s, dx] = scaled

    def spread_out(where, value):
        return jnp.dot(where[:, :capacity], value, preferred_element_type=jnp.float32)

    last_x = 2 * depth + 2
    mix_fetch(2).wait()
    mix_core_copy(2).wait_recv()
    lax.fori_loop(0, early, mix_away, 0)
    lax.fori_loop(0, early, mix_send, 0)

    def step(s, carry):
        @pl.when(s < steps)
        def _():
            @pl.when(s + 1 < steps)
            def _():
                fetch(s + 1).start()

            fetch(s).wait()
            compute(s)

        @pl.when((s >= 1) & (s <= steps))
        def _():
            t = s - 1
            for side in (0, 1):
                core_copy(t, side).wait_recv()
                for dx in (0, 1):
                    own[side][t, dx] = (
                        own[side][t, dx].astype(jnp.float32)
                        + incoming[side][t, dx].astype(jnp.float32)
                    ).astype(jnp.bfloat16)

        @pl.when(s < steps)
        def _():
            for side in (0, 1):
                core_copy(s, side).start()

        @pl.when(s == 1)
        def _():
            for n in (1, 0):
                mix_fetch(n).wait()
                mix_core_copy(n).wait_recv()
            lax.fori_loop(early, chunks, mix_away, 0)
            lax.fori_loop(0, chunks, mix_home, 0)

        i = (s - 4) // 2

        @pl.when((s >= 4) & (s % 2 == 0) & (i < depth))
        def _():
            far, near = 2 * i, 2 * i + 1
            y_copy(i).wait_recv()
            for dx in (0, 1):
                sum_b = spread_out(place[near, dx], own_b[near, dx]) + spread_out(
                    place_next[near, dx], from_y[i, dx]
                )

                @pl.when(i < depth - 1)
                def _():
                    to_zb[i, dx] = sum_b.astype(jnp.bfloat16)

                @pl.when(i == depth - 1)
                def _():
                    keep_b[dx] = sum_b

            x_copy(far).wait_recv()
            where = place[far, 0]
            to_y[i] = (spread_out(where, own_a[far, 0]) + spread_out(where, from_x[far])).astype(
                jnp.bfloat16
            )

            @pl.when(i < depth - 1)
            def _():
                zb_copy(i).start()

            x_copy(near).wait_recv()
            where = place[near, 0]
            keep_a[i] = spread_out(where, own_a[near, 0]) + spread_out(where, from_x[near])
            a_copy(i).start()

        @pl.when((s >= 1) & (s <= steps))
        def _():
            t = s - 1
            x_copy(t).start()

            @pl.when(t % 2 == 0)
            def _():
                y_copy(t // 2).start()

        start = jnp.where(s == last_x, late, jnp.clip(early + s - 3, early, late))
        stop = jnp.where(
            s == last_x, chunks, jnp.where(s > last_x, 0, jnp.clip(early + s - 2, early, late))
        )
        lax.fori_loop(start, stop, mix_send, 0)

        j = (s - 6) // 2

        @pl.when((s >= 6) & (s % 2 == 0) & (j < depth))
        def _():
            a_copy(j).wait_recv()
            sum_a = keep_a[j] + came_y[j].astype(jnp.float32)

            @pl.when(j < depth - 1)
            def _():
                to_za[j] = sum_a.astype(jnp.bfloat16)
                za_copy(j).start()

            @pl.when(j == depth - 1)
            def _():
                keep_a[j] = sum_a

        return carry

    lax.fori_loop(0, 2 * depth + 5, step, 0)
    for i in range(depth - 1):
        zb_copy(i).wait_recv()
    total = [keep_b[0], keep_b[1]]
    for i in range(depth - 1):
        total = [total[dx] + from_zb[i, dx].astype(jnp.float32) for dx in (0, 1)]
    to_x[...] = total[1].astype(jnp.bfloat16)
    keep_b[0] = total[0]
    total = keep_a[depth - 1]
    for i in range(depth - 1):
        za_copy(i).wait_recv()
        total = total + from_za[i].astype(jnp.float32)
    out_ref[:, :cut] = total.astype(jnp.bfloat16)
    b_copy().start()
    lax.fori_loop(0, chunks, mix_finish, 0)
    lax.fori_loop(0, chunks, mix_sent, 0)
    b_copy().wait_recv()
    out_ref[:, cut:] = (keep_b[0] + came_x[...].astype(jnp.float32)).astype(jnp.bfloat16)
    for n in range(3):
        mix_core_copy(n).wait_send()
    for s in range(steps):
        for side in (0, 1):
            core_copy(s, side).wait_send()
        x_copy(s).wait_send()
    for i in range(depth):
        y_copy(i).wait_send()
        a_copy(i).wait_send()
    b_copy().wait_send()
    for i in range(depth - 1):
        za_copy(i).wait_send()
        zb_copy(i).wait_send()


def mixer_gather_kernel(
    per_group, groups, blocks, depth,
    x_ref, xt_ref, b_ref, bt_ref, c_ref, ct_ref, z_ref, pre_ref, spike_ref, offset_ref, rate_ref, skip_ref, scale_ref,
    exit_ref, marked_ref, x_all, b_all, c_all,
    part_ref, tokens_ref,
    head_rows, lw_of, cum_of, row_of, end_of, skip_of, decay_of, decay_row, xr_ref, br_ref, cr_ref, rim_s,
    rim_r, xbuf, bbuf, cbuf, state, ybuf, nbuf, pair_out, pair_in, line_out, line_in, line_sum, swap_out,
    swap_in, local_sem, z_send, z_recv, xa_s, xa_r, xb_s, xb_r, xf_s, xf_r, ya_s, ya_r, yb_s, yb_r,
    yf_s, yf_r, d_s, d_r, pair_s, pair_r, line_s, line_r, swap_s, swap_r,
):
    step = pl.program_id(0)
    ep, tp = lax.axis_index("ep"), lax.axis_index("tp")
    z, y, x, core = ep // 2, ep % 2, tp // 2, tp % 2
    sibling = {"tp": x * 2 + 1 - core}
    x_next = {"tp": (1 - x) * 2 + core}
    y_next = {"ep": z * 2 + 1 - y}
    mesh_id = pl.DeviceIdType.MESH
    rows = marked_ref.shape[0]
    first_rows = rows * 3 // 8
    inner = state.shape[1]
    wide = inner // 2

    def z_next(k):
        return {"ep": ((z + k) % depth) * 2 + y}

    def remote(source, target, send, recv, device):
        return pltpu.make_async_remote_copy(
            src_ref=source, dst_ref=target, send_sem=send, recv_sem=recv,
            device_id=device, device_id_type=mesh_id,
        )

    def region(dx, dy, k, half, c=core):
        block = (((z + depth - k) % depth) * 2 + (y + dy) % 2) * 4 + ((x + dx) % 2) * 2 + c
        offset, size = ((0, rows), (0, first_rows), (first_rows, rows - first_rows))[
            0 if half is None else 1 + half
        ]
        return tokens_ref.at[pl.ds(pl.multiple_of(block * rows + offset, 16), size)]

    def source(dx, dy, k, half):
        if (dx, dy, k) == (0, 0, 0):
            if half is None:
                return marked_ref
            if half == 0:
                return marked_ref.at[pl.ds(0, first_rows)]
            return marked_ref.at[pl.ds(first_rows, rows - first_rows)]
        return region(dx, dy, k, half)

    def z_copy(k):
        return remote(
            marked_ref, region(0, 0, 0, None), z_send.at[k - 1], z_recv.at[k - 1], z_next(k)
        )

    def z_came(k):
        here = region(0, 0, k, None)
        return remote(here, here, z_send.at[k - 1], z_recv.at[k - 1], z_next(k))

    moves = {
        "xa": ((0, 0, 0), (1, 0, 0), xa_s, xa_r, x_next),
        "xb": ((0, 0, 1), (1, 0, 1), xb_s, xb_r, x_next),
        "xf": ((0, 1, 1), (1, 1, 1), xf_s, xf_r, x_next),
        "yb": ((0, 0, 1), (0, 1, 1), yb_s, yb_r, y_next),
        "ya": ((0, 0, 0), (0, 1, 0), ya_s, ya_r, y_next),
        "yf": ((1, 0, 0), (1, 1, 0), yf_s, yf_r, y_next),
    }

    def sent(name, k):
        (dx, dy, half), _, send, recv, device = moves[name]
        return remote(
            source(dx, dy, k, half), region(dx, dy, k, half), send.at[k], recv.at[k], device
        )

    def came(name, k):
        _, (dx, dy, half), send, recv, device = moves[name]
        here = region(dx, dy, k, half)
        return remote(here, here, send.at[k], recv.at[k], device)

    shared = [(0, 0, None), (1, 0, 0), (1, 0, 1), (0, 1, 1), (0, 1, 0), (1, 1, 0), (1, 1, 1)]

    def d_sent(k, n):
        dx, dy, half = shared[n]
        m = len(shared) * k + n
        return remote(
            source(dx, dy, k, half), region(dx, dy, k, half), d_s.at[m], d_r.at[m], sibling
        )

    def d_came(k, n):
        dx, dy, half = shared[n]
        m = len(shared) * k + n
        here = region(dx, dy, k, half, 1 - core)
        return remote(here, here, d_s.at[m], d_r.at[m], sibling)

    def first_hop(k):
        if k > 0:
            z_came(k).wait_recv()
        for name in ("xa", "yb", "xb", "ya"):
            sent(name, k).start()
        d_sent(k, 0).start()

    def second_hop(k):
        came("xa", k).wait_recv()
        sent("yf", k).start()
        d_sent(k, 1).start()
        came("yb", k).wait_recv()
        sent("xf", k).start()
        d_sent(k, 3).start()

    def last_hop(k, parts=(("xb", 2), ("ya", 4), ("yf", 5), ("xf", 6))):
        for name, n in parts:
            came(name, k).wait_recv()
            d_sent(k, n).start()

    devices = 2 * depth
    after, before = {"ep": (ep + 1) % devices}, {"ep": (ep + devices - 1) % devices}
    last_rows = pl.ds(x_all.shape[0] - 2 * RIM, 2 * RIM)

    def rim_copy(n):
        whole, rim = ((x_all, xr_ref), (b_all, br_ref), (c_all, cr_ref))[n]
        return remote(whole.at[last_rows], rim, rim_s.at[n], rim_r.at[n], after)

    def own_copy():
        return pltpu.make_async_copy(marked_ref, region(0, 0, 0, None), local_sem.at[0])

    @pl.when(step == 0)
    def _():
        barrier = pltpu.get_barrier_semaphore()
        partners = [sibling, x_next, y_next, after, before]
        partners = partners + [z_next(k) for k in range(1, depth)]
        for partner in partners:
            pl.semaphore_signal(barrier, inc=1, device_id=partner, device_id_type=mesh_id)
        pl.semaphore_wait(barrier, len(partners))
        for n in range(3):
            rim_copy(n).start()
        z_copy(1).start()
        first_hop(0)
        for k in range(2, depth - 1):
            z_copy(k).start()
        own_copy().start()
        heads = pre_ref.shape[0]
        head_rows[...] = jnp.zeros_like(head_rows)
        head_rows[0:1, 0:heads] = offset_ref[...]
        head_rows[1:2, 0:heads] = jnp.exp(rate_ref[...])
        skip_of[...] = skip_ref[...]
        by_head = head_rows[...].T[0:heads]

        def stacked(piece):
            return jnp.concatenate([piece(n) for n in range(blocks)], axis=0)

        def tall(column):
            return stacked(lambda n: jnp.broadcast_to(column, (heads, SPAN)))

        raw = stacked(lambda n: pre_ref[:, n * SPAN : (n + 1) * SPAN].astype(jnp.float32))
        raw = raw + tall(by_head[:, 0:1])
        interval = jnp.maximum(raw, 0.0) + jnp.log1p(jnp.exp(-jnp.abs(raw)))
        spikes = stacked(lambda n: spike_ref[:, n * SPAN : (n + 1) * SPAN])
        fading = spikes - tall(by_head[:, 1:2]) * interval
        upto = lax.broadcasted_iota(jnp.int32, (SPAN, SPAN), 0) <= lax.broadcasted_iota(
            jnp.int32, (SPAN, SPAN), 1
        )
        cumulative = jnp.dot(
            fading, jnp.where(upto, 1.0, 0.0), precision=highest, preferred_element_type=jnp.float32
        )
        row_log = jnp.log(interval) - cumulative
        key_log = row_log + cumulative[:, SPAN - 1 :]
        decay = jnp.ones((1, heads), jnp.float32)
        for n in range(blocks):
            rows_n = slice(n * heads, (n + 1) * heads)
            cum = cumulative[rows_n].T
            end = jnp.exp(cum[SPAN - 1 :])
            row_of[n] = row_log[rows_n]
            lw_of[n] = key_log[rows_n].T
            cum_of[n] = cum
            end_of[n] = end
            decay = decay * end
        decay_of[...] = decay
        for n in range(3):
            rim_copy(n).wait_recv()

    def per_head(row, h):
        first_head = jnp.broadcast_to(row[:, h : h + 1], (1, 2 * HEAD))
        second_head = jnp.broadcast_to(row[:, h + 1 : h + 2], (1, 2 * HEAD))
        return jnp.where(low[0:1], first_head, second_head)

    has_rim = ep > 0
    low = lax.broadcasted_iota(jnp.int32, (SPAN, 2 * HEAD), 1) < HEAD
    state_pass = step < blocks
    output_pass = step > blocks

    @pl.when(state_pass)
    def _():
        first = step == 0
        xv = conv_after(xbuf, first, x_ref, xr_ref, has_rim, xt_ref)
        bv = conv_after(bbuf, first, b_ref, br_ref, has_rim, bt_ref)

        @pl.when(first)
        def _():
            state[...] = jnp.zeros_like(state)

        lw = lw_of[step]
        end = end_of[step]
        for g in range(groups):
            bt = bv[:, g * STATE : (g + 1) * STATE].T.astype(jnp.bfloat16)
            for pair in range(per_group // 2):
                h = g * per_group + 2 * pair
                cols = slice(h * HEAD, (h + 2) * HEAD)
                factor = jnp.exp(
                    jnp.where(low, spread(lw, h, 2 * HEAD), spread(lw, h + 1, 2 * HEAD))
                )
                xw = (xv[:, cols] * factor).astype(jnp.bfloat16)
                added = jnp.dot(bt, xw, preferred_element_type=jnp.float32)
                state[:, cols] = state[:, cols] * per_head(end, h) + added

    @pl.when(step == blocks // 2)
    def _():
        second_hop(0)

    @pl.when(step == blocks)
    def _():
        pair = remote(pair_out, pair_in, pair_s.at[0], pair_r.at[0], y_next)
        swap = remote(swap_out, swap_in, swap_s.at[0], swap_r.at[0], y_next)

        def line(k):
            return remote(
                line_out, line_in.at[k - 1], line_s.at[k - 1], line_r.at[k - 1], z_next(k)
            )

        for h in range(0, groups * per_group, 2):
            decay_row[:, h * HEAD : (h + 2) * HEAD] = per_head(decay_of[...], h)
        decay = decay_row[...]
        pair_out[:STATE, :] = state[...].astype(jnp.bfloat16)
        pair_out[STATE:, :] = jnp.broadcast_to(decay, (2 * RIM, inner)).astype(jnp.bfloat16)
        last_hop(0, (("xb", 2), ("ya", 4)))
        pair.start()
        first_hop(1)
        last_hop(0, (("yf", 5), ("xf", 6)))
        pair.wait_recv()
        mine = pl.ds(pl.multiple_of(y * wide, wide), wide)
        theirs = pl.ds(pl.multiple_of((1 - y) * wide, wide), wide)
        own_state, own_decay = state[:, mine], decay_row[:, mine]
        other_state = pair_in[:STATE, mine].astype(jnp.float32)
        other_decay = pair_in[STATE : STATE + 1, mine].astype(jnp.float32)
        later = y == 1
        both = jnp.where(
            later, other_state * own_decay + own_state, own_state * other_decay + other_state
        )
        line_out[:STATE, :] = both.astype(jnp.bfloat16)
        line_out[STATE:, :] = jnp.broadcast_to(own_decay * other_decay, (2 * RIM, wide)).astype(
            jnp.bfloat16
        )
        line_sum[...] = jnp.zeros_like(line_sum)
        for k in range(1, depth):
            @pl.when(z + k < depth)
            def _():
                line(k).start()

        z_copy(depth - 1).start()
        for k in range(depth - 1, 0, -1):
            @pl.when(z >= k)
            def _():
                line(k).wait_recv()
                line_sum[...] = line_sum[...] * line_in[k - 1, STATE : STATE + 1, :].astype(
                    jnp.float32
                ) + line_in[k - 1, :STATE, :].astype(jnp.float32)

        swap_out[...] = line_sum[...].astype(jnp.bfloat16)
        state[:, mine] = line_sum[...]
        second_hop(1)
        swap.start()
        swap.wait_recv()
        state[:, theirs] = swap_in[...].astype(jnp.float32)

        @pl.when(later)
        def _():
            state[...] = state[...] * pair_in[STATE : STATE + 1, :].astype(jnp.float32) + pair_in[
                :STATE, :
            ].astype(jnp.float32)

        pair.wait_send()
        swap.wait_send()
        for k in range(1, depth):
            @pl.when(z + k < depth)
            def _():
                line(k).wait_send()

    @pl.when(output_pass)
    def _():
        first = step == blocks + 1
        xv = conv_after(xbuf, first, x_ref, xr_ref, has_rim, xt_ref)
        bv = conv_after(bbuf, first, b_ref, br_ref, has_rim, bt_ref)
        cv = conv_after(cbuf, first, c_ref, cr_ref, has_rim, ct_ref)
        at = step - blocks - 1
        lw = lw_of[at]
        cum = cum_of[at]
        end = end_of[at]
        causal = lax.broadcasted_iota(jnp.int32, (SPAN, SPAN), 0) >= lax.broadcasted_iota(
            jnp.int32, (SPAN, SPAN), 1
        )
        group_cols = per_group * HEAD
        for g in range(groups):
            bt = bv[:, g * STATE : (g + 1) * STATE].T.astype(jnp.bfloat16)
            cg = cv[:, g * STATE : (g + 1) * STATE].astype(jnp.bfloat16)
            scores = jnp.dot(cg, bt, preferred_element_type=jnp.float32)
            squares = jnp.zeros((SPAN, 2 * HEAD), jnp.float32)
            for pair in range(per_group // 2):
                h = g * per_group + 2 * pair
                cols = slice(h * HEAD, (h + 2) * HEAD)
                xp = xv[:, cols]
                cum_0, cum_1 = spread(cum, h, SPAN), spread(cum, h + 1, SPAN)
                row_0, row_1 = row_of[at, h : h + 1, :], row_of[at, h + 1 : h + 2, :]
                m_0 = scores * jnp.exp(jnp.where(causal, cum_0 + row_0, -jnp.inf))
                m_1 = scores * jnp.exp(jnp.where(causal, cum_1 + row_1, -jnp.inf))
                mixing = jnp.concatenate([m_0.astype(jnp.bfloat16), m_1.astype(jnp.bfloat16)], axis=1)
                x_0 = jnp.where(low, xp, 0.0).astype(jnp.bfloat16)
                x_1 = jnp.where(low, 0.0, xp).astype(jnp.bfloat16)
                value = jnp.dot(
                    mixing, jnp.concatenate([x_0, x_1], axis=0), preferred_element_type=jnp.float32
                )
                before = state[:, cols]
                carried = jnp.dot(cg, before.astype(jnp.bfloat16), preferred_element_type=jnp.float32)
                value = value + carried * jnp.exp(jnp.where(low, cum_0, cum_1)) + xp * per_head(skip_of[...], h)
                factor = jnp.exp(
                    jnp.where(low, spread(lw, h, 2 * HEAD), spread(lw, h + 1, 2 * HEAD))
                )
                xw = (xp * factor).astype(jnp.bfloat16)
                added = jnp.dot(bt, xw, preferred_element_type=jnp.float32)
                state[:, cols] = before * per_head(end, h) + added
                gate = z_ref[:, cols].astype(jnp.float32)
                gated = value * (gate * jax.nn.sigmoid(gate))
                squares = squares + gated * gated
                ybuf[:, cols] = gated
            mean = jnp.sum(squares, axis=1, keepdims=True) / group_cols
            inverse = lax.rsqrt(mean + norm_eps)
            cols = slice(g * group_cols, (g + 1) * group_cols)
            nbuf[:, cols] = (ybuf[:, cols] * inverse * scale_ref[:, cols]).astype(jnp.bfloat16)
        part_ref[...] = jnp.dot(
            nbuf[...], exit_ref[...], preferred_element_type=jnp.float32
        ).astype(jnp.bfloat16)

    pace = blocks // (2 * depth - 2)
    for k in range(2, depth):
        at = blocks + 1 + (2 * k - 4) * pace

        @pl.when(step == at - (1 if k == 2 else 0))
        def _():
            first_hop(k)

        @pl.when(step == at + pace)
        def _():
            second_hop(k)
            last_hop(k - 1)

    @pl.when(step == 2 * blocks)
    def _():
        last_hop(depth - 1)
        for k in range(depth):
            for n in range(len(shared)):
                d_came(k, n).wait_recv()
        own_copy().wait()
        for n in range(3):
            rim_copy(n).wait_send()
        for k in range(1, depth):
            z_copy(k).wait_send()
        for k in range(depth):
            for name in moves:
                sent(name, k).wait_send()
            for n in range(len(shared)):
                d_sent(k, n).wait_send()


def dense_experts_fit(tok_rows, top_count, capacity, mix_rows):
    experts = lax.axis_size("ep")
    fits = experts % 2 == 0 and experts >= 4 and 3 * experts <= LANES and lax.axis_size("tp") == 4
    return fits and 2 * top_count >= experts and mix_rows % (4 * MIX_ROWS) == 0 and tok_rows == LANES and capacity % 16 == 0 and top_count <= 8


def marked_tokens(
    specialist_sample_slice, specialist_scaling_vector, chosen_specialists, dispatcher_affinity_matrix
):
    rows, features = specialist_sample_slice.shape
    return pl.pallas_call(
        functools.partial(routing_kernel, lax.axis_size("ep")),
        out_shape=jax.ShapeDtypeStruct((rows, features + LANES), jnp.bfloat16),
        scratch_shapes=[pltpu.VMEM((LANES, rows), jnp.float32)],
        name="routing",
    )(
        specialist_sample_slice, specialist_scaling_vector[None], chosen_specialists.T,
        dispatcher_affinity_matrix.T,
    )


def experts_dense(
    tokens, mix_part, rows, capacity, gating_projection, expand_projection, shrink_projection
):
    experts = lax.axis_size("ep")
    features = gating_projection.shape[1]
    depth, steps = experts // 2, experts
    cut = features * CUT_EIGHTHS // 8 // LANES * LANES
    rest = features - cut
    hidden = gating_projection.shape[2]
    narrow = jnp.bfloat16
    dma = pltpu.SemaphoreType.DMA
    share = mix_part.shape[0] // 4
    pieces = share // MIX_ROWS
    work = 2 * experts * 4 * capacity * features * hidden * 3
    return pl.pallas_call(
        functools.partial(experts_kernel, experts, capacity),
        in_specs=[pl.BlockSpec(memory_space=pl.ANY)] * 2
        + [pl.BlockSpec(memory_space=pltpu.VMEM)] * 3,
        out_specs=[pl.BlockSpec(memory_space=pltpu.VMEM)] * 2,
        out_shape=[
            jax.ShapeDtypeStruct((rows, features), narrow),
            jax.ShapeDtypeStruct((share, features), narrow),
        ],
        scratch_shapes=[
            pltpu.VMEM((2, 4 * rows, features + LANES), narrow),
            pltpu.VMEM((4 * capacity, features), narrow),
            pltpu.VMEM((steps, 2, capacity, cut), narrow),
            pltpu.VMEM((steps, 2, capacity, rest), narrow),
            pltpu.VMEM((steps, 2, capacity, cut), narrow),
            pltpu.VMEM((steps, 2, capacity, rest), narrow),
            pltpu.VMEM((steps, 2, capacity, cut), narrow),
            pltpu.VMEM((steps, 2, capacity, rest), narrow),
            pltpu.VMEM((steps, 2, rows, LANES), narrow),
            pltpu.VMEM((steps, 2, rows, LANES), narrow),
            pltpu.VMEM((steps, capacity, cut), narrow),
            pltpu.VMEM((depth, 2, capacity, rest), narrow),
            pltpu.VMEM((depth, rows, cut), narrow),
            pltpu.VMEM((depth, rows, cut), narrow),
            pltpu.VMEM((rows, rest), narrow),
            pltpu.VMEM((rows, rest), narrow),
            pltpu.VMEM((depth, rows, cut), jnp.float32),
            pltpu.VMEM((2, rows, rest), jnp.float32),
            pltpu.VMEM((depth - 1, rows, cut), narrow),
            pltpu.VMEM((depth - 1, rows, cut), narrow),
            pltpu.VMEM((depth - 1, 2, rows, rest), narrow),
            pltpu.VMEM((depth - 1, 2, rows, rest), narrow),
            pltpu.VMEM((2, share, features), narrow),
            pltpu.VMEM((2, share, features), narrow),
            pltpu.VMEM((share, features), narrow),
            pltpu.VMEM((share, features), narrow),
            dma((3,)), dma((3,)), dma((3,)), dma((pieces,)), dma((pieces,)),
            dma((2,)), dma((2 * steps,)), dma((2 * steps,)), dma((steps,)), dma((steps,)),
            dma((depth,)), dma((depth,)), dma((depth,)), dma((depth,)), dma((1,)), dma((1,)),
            dma((depth - 1,)), dma((depth - 1,)), dma((depth - 1,)), dma((depth - 1,)),
        ],
        compiler_params=pltpu.CompilerParams(
            collective_id=0, has_side_effects=True, vmem_limit_bytes=63 * 1024 * 1024
        ),
        cost_estimate=pl.CostEstimate(
            flops=8 * work, bytes_accessed=4 * tokens.size, transcendentals=0
        ),
        name="experts",
    )(tokens, mix_part, gating_projection[0], expand_projection[0], shrink_projection[0])


def body(
    sequence_entry_features,
    sequence_exit_gating,
    memory_insert_clusters,
    memory_query_clusters,
    interval_presoftplus,
    entry_filter_taps,
    insert_filter_taps,
    query_filter_taps,
    interval_offset,
    head_fading_exponent,
    skip_connection_factor,
    spike_fading_exponent,
    cluster_scaling_vector,
    sequence_exit_projection,
    specialist_sample_slice,
    specialist_scaling_vector,
    chosen_specialists,
    dispatcher_affinity_matrix,
    gating_projection,
    expand_projection,
    shrink_projection,
):
    tok_rows, top_count = chosen_specialists.shape
    capacity = tok_rows * top_count * 5 // (4 * lax.axis_size("ep"))
    dense = dense_experts_fit(tok_rows, top_count, capacity, sequence_entry_features.shape[0])
    marked = None
    if dense:
        marked = marked_tokens(
            specialist_sample_slice,
            specialist_scaling_vector,
            chosen_specialists,
            dispatcher_affinity_matrix,
        )
    mix_part = mixer_half(
        sequence_entry_features,
        sequence_exit_gating,
        memory_insert_clusters,
        memory_query_clusters,
        interval_presoftplus,
        entry_filter_taps,
        insert_filter_taps,
        query_filter_taps,
        interval_offset,
        head_fading_exponent,
        skip_connection_factor,
        spike_fading_exponent,
        cluster_scaling_vector,
        sequence_exit_projection,
        marked,
    )
    if dense:
        mix_part, tokens = mix_part
        moe_out, mixed = experts_dense(
            tokens, mix_part, tok_rows, capacity, gating_projection, expand_projection, shrink_projection
        )
        return (mixed, moe_out)
    mixed = lax.psum_scatter(mix_part, "tp", scatter_dimension=0, tiled=True)
    moe_out = experts_half(
        specialist_sample_slice,
        specialist_scaling_vector,
        chosen_specialists,
        dispatcher_affinity_matrix,
        gating_projection,
        expand_projection,
        shrink_projection,
    )
    return (mixed, moe_out)


def solution(mesh):
    in_specs = (
        P("ep", "tp"),
        P("ep", "tp"),
        P("ep", "tp"),
        P("ep", "tp"),
        P("ep", "tp"),
        P(None, "tp"),
        P(None, "tp"),
        P(None, "tp"),
        P("tp"),
        P("tp"),
        P("tp"),
        P("ep", "tp"),
        P("tp"),
        P("tp", None),
        P(("ep", "tp"), None),
        P(),
        P(("ep", "tp"), None),
        P(("ep", "tp"), None),
        P("ep", None, "tp"),
        P("ep", None, "tp"),
        P("ep", "tp", None),
    )
    out_specs = (P(("ep", "tp"), None), P(("ep", "tp"), None))
    return jax.shard_map(body, mesh=mesh, in_specs=in_specs, out_specs=out_specs, check_vma=False)
```
